32 devices in a mesh: grp: 2 (over y), sp: 4 (over z), tp: 4 (over x, core).
Axes of the slice: x: 2, y: 2, z: 4, core: 2. Of those that a mesh axis runs over, the one named last changes fastest.
Arguments:
- hidden: bfloat16 [3072, 2048], P(('grp', 'sp'), 'tp'), parts along dimension 0, may hold values from -45 to 45
- norm_gain: bfloat16 [2048], replicated, may hold values from 0.099609375 to 1.8984375
- w_query: bfloat16 [2048, 1024], P(None, 'tp'), may hold values from -0.125 to 0.125
- w_key: bfloat16 [2048, 1024], P(None, 'tp'), may hold values from -0.125 to 0.125
- w_value: bfloat16 [2048, 1024], P(None, 'tp'), may hold values from -0.125 to 0.125
- query_gain: float32 [8, 128], P('tp'), may hold values from 0.3 to 16
- key_gain: float32 [8, 128], P('tp'), may hold values from 0.3 to 16
- w_out: bfloat16 [1024, 2048], P('tp'), may hold values from -1.5 to 1.5
Outputs:
- mixed: bfloat16 [3072, 2048], P(('grp', 'sp'), 'tp'), parts along dimension 0
- log_total: float32 [3072, 8], P(('grp', 'sp'), 'tp'), parts along dimension 0
The draws below stay inside these ranges and needn't reach their ends.
There are 2 independent parts, one for each index of `grp`. The reference program is written for one: setup_inputs(seed, part) draws one part's arguments, and reference() takes and returns one part's arrays. A program takes and returns all parts, laid end to end along the dimension named above; an argument that names none is the same for every part. Nothing has to cross between parts.
All inputs are finite; a program needn't handle non-finite values.
Results may differ from the reference program's by a relative error of at most 0.015.
The reference program's roundings to bfloat16 on the way count: a program that leaves them out, or rounds other values in their place, can miss the bound.
Values may be sent and summed in bfloat16 or wider, within the bound.
A program may use at most 64 MiB of HBM per device.

```python
import jax
import jax.numpy as jnp
from jax import lax

D = 2048
HEADS = 8
HEAD_DIM = 128
KEYS_BEHIND = 128
MIDDLE_DILATION = 4
WIDEST_DILATION = 16
TOKENS = 1536


def draw_hidden(key, part):
    row_key, col_key, base_key = jax.random.split(jax.random.fold_in(key, 17), 3)
    row_factor = jnp.exp(jax.random.uniform(row_key, (TOKENS, 1), jnp.float32, -1.2, 1.1))
    rising = 1.0 + 2.0 * jnp.arange(D, dtype=jnp.float32) / D
    col_factor = jnp.exp(jax.random.uniform(col_key, (1, D), jnp.float32, 0.0, 2.3)) * rising * 0.125
    base = jnp.clip(jax.random.normal(base_key, (TOKENS, D), jnp.float32), -4.0, 4.0)
    return (base * row_factor * col_factor).astype(jnp.bfloat16)


def head_gains(key, salt):
    channel_key = jax.random.fold_in(jax.random.fold_in(key, salt), 1)
    noise = jnp.clip(jax.random.normal(channel_key, (HEADS, HEAD_DIM), jnp.float32), -3.5, 3.5)
    return (1.0 + 0.18 * noise).astype(jnp.float32)


def draw_query_gain(key, part):
    return head_gains(key, 31)


def draw_key_gain(key, part):
    return head_gains(key, 47)


def block_levels(stream_key, shape, pieces, low, high):
    factor_of = 1.0
    for dim, parts in pieces:
        draws = jax.random.uniform(jax.random.fold_in(jax.random.fold_in(stream_key, 6), dim), (parts,), jnp.float32, low / len(pieces), high / len(pieces))
        factor_of = factor_of * jnp.repeat(jnp.exp(draws), shape[dim] // parts).reshape((-1,) + (1,) * (len(shape) - 1 - dim))
    return factor_of


def centred(key, dims, scale, bound, cuts=(), held_as=jnp.bfloat16):
    drawn = jax.random.normal(key, dims, jnp.float32) * scale
    if len(cuts) > 0:
        drawn = block_levels(key, dims, cuts, -0.22, 0.18) * drawn
    return jnp.clip(drawn, min=-bound, max=bound).astype(held_as)


def setup_inputs(seed: int = 0, part: int = 0) -> dict:
    seeds = jax.random.split(jax.random.key(seed), 9)
    part_splits = jax.random.split(jax.random.fold_in(seeds[8], part), 9)
    return {
        "hidden": draw_hidden(jax.random.fold_in(jax.random.fold_in(seeds[8], part), 71), part),
        "norm_gain": jnp.clip(1.0 + 0.18 * jax.random.normal(seeds[1], (D,), jnp.float32), 0.099609375, 1.8984375).astype(jnp.bfloat16),
        "w_query": centred(seeds[2], (D, HEADS * HEAD_DIM), D ** -0.5, 0.125, ((1, 4),)),
        "w_key": centred(seeds[3], (D, HEADS * HEAD_DIM), D ** -0.5, 0.125, ((1, 4),)),
        "w_value": centred(seeds[4], (D, HEADS * HEAD_DIM), D ** -0.5, 0.125, ((1, 4),)),
        "query_gain": draw_query_gain(jax.random.fold_in(seeds[8], 71), part),
        "key_gain": draw_key_gain(jax.random.fold_in(seeds[8], 71), part),
        "w_out": centred(seeds[7], (HEADS * HEAD_DIM, D), 16 ** -0.5, 1.5, ((0, 4),)),
    }


EPSILON = 1e-06
ROTARY_BASE = 500000.0

def rotate(values, positions):
    head_width = values.shape[-1]
    inverse = ROTARY_BASE ** (-jnp.arange(0, head_width, 2, dtype=jnp.float32) / head_width)
    angles = positions[:, None] * inverse[None, :]
    cosine = jnp.cos(angles)[:, None, :]
    sine = jnp.sin(angles)[:, None, :]
    half_width = head_width // 2
    first_half = values[..., :half_width]
    second_half = values[..., half_width:]
    return jnp.concatenate([first_half * cosine - second_half * sine, second_half * cosine + first_half * sine], axis=-1)

def head_norm(values, gains):
    normed = values * lax.rsqrt(lax.optimization_barrier(jnp.mean(values * values, axis=-1, keepdims=True)) + EPSILON)
    return normed * gains[None, :, :]

def dilated_branch(query, key_all, value_all, dilation_step):
    sequence_rows, head_count, head_width = query.shape
    class_rows = sequence_rows // dilation_step
    block_count = -(-class_rows // KEYS_BEHIND)
    padded_rows = block_count * KEYS_BEHIND

    def by_class(values):
        return values.reshape(class_rows, dilation_step, head_count, head_width).transpose(1, 0, 2, 3).astype(jnp.float32)
    query_blocks = jnp.pad(by_class(query), ((0, 0), (0, padded_rows - class_rows), (0, 0), (0, 0)))
    query_blocks = query_blocks.reshape(dilation_step, block_count, KEYS_BEHIND, head_count, head_width)

    def windows(values):
        padded = jnp.pad(by_class(values), ((0, 0), (KEYS_BEHIND, padded_rows - class_rows), (0, 0), (0, 0)))
        padded = padded.reshape(dilation_step, block_count + 1, KEYS_BEHIND, head_count, head_width)
        return jnp.concatenate([padded[:, :-1], padded[:, 1:]], axis=2)
    key_windows = windows(key_all)
    value_windows = windows(value_all)
    scores = jnp.einsum('rnqhd,rnkhd->rnhqk', query_blocks, key_windows) * head_width ** (-0.5)
    row_index = jnp.arange(KEYS_BEHIND, dtype=jnp.int32)[:, None]
    col_index = jnp.arange(2 * KEYS_BEHIND, dtype=jnp.int32)[None, :]
    distance = row_index + KEYS_BEHIND - col_index
    in_band = (distance >= 0) & (distance <= KEYS_BEHIND)
    class_index = jnp.arange(block_count, dtype=jnp.int32)[:, None] * KEYS_BEHIND + col_index - KEYS_BEHIND
    allowed = in_band[None, :, :] & (class_index >= 0)[:, None, :]
    scores = jnp.where(allowed[None, :, None, :, :], scores, -jnp.inf)
    row_max = lax.optimization_barrier(jnp.max(scores, axis=-1, keepdims=True))
    weights = jnp.exp(scores - row_max)
    weight_sum = lax.optimization_barrier(jnp.sum(weights, axis=-1))
    rounded = lax.optimization_barrier(weights.astype(jnp.bfloat16)).astype(jnp.float32)
    weighted = jnp.einsum('rnhqk,rnkhd->rnqhd', rounded, value_windows)
    branch_out = weighted / jnp.transpose(weight_sum, (0, 1, 3, 2))[..., None]
    branch_out = branch_out.reshape(dilation_step, padded_rows, head_count, head_width)[:, :class_rows]
    branch_out = branch_out.transpose(1, 0, 2, 3).reshape(sequence_rows, head_count, head_width)
    log_sum = jnp.transpose(row_max[..., 0] + jnp.log(weight_sum), (0, 1, 3, 2))
    log_sum = log_sum.reshape(dilation_step, padded_rows, head_count)[:, :class_rows]
    log_sum = log_sum.transpose(1, 0, 2).reshape(sequence_rows, head_count)
    return (branch_out, log_sum)

def reference(hidden, norm_gain, w_query, w_key, w_value, query_gain, key_gain, w_out):
    sequence_rows = hidden.shape[0]
    hidden_float = hidden.astype(jnp.float32)
    row_scale = lax.rsqrt(lax.optimization_barrier(jnp.mean(hidden_float * hidden_float, axis=1, keepdims=True)) + EPSILON)
    scaled = (hidden_float * norm_gain.astype(jnp.float32)[None, :]).astype(jnp.bfloat16)
    query_raw = jnp.dot(scaled, w_query, preferred_element_type=jnp.float32) * row_scale
    key_raw = jnp.dot(scaled, w_key, preferred_element_type=jnp.float32) * row_scale
    value_raw = jnp.dot(scaled, w_value, preferred_element_type=jnp.float32) * row_scale
    positions = jnp.arange(sequence_rows, dtype=jnp.int32).astype(jnp.float32)
    query = rotate(head_norm(query_raw.reshape(sequence_rows, HEADS, HEAD_DIM), query_gain), positions).astype(jnp.bfloat16)
    key_all = rotate(head_norm(key_raw.reshape(sequence_rows, HEADS, HEAD_DIM), key_gain), positions).astype(jnp.bfloat16)
    value_all = value_raw.astype(jnp.bfloat16).reshape(sequence_rows, HEADS, HEAD_DIM)
    branch_outs = []
    branch_logs = []
    for dilation_step in (1, MIDDLE_DILATION, WIDEST_DILATION):
        branch_out, log_sum = dilated_branch(query, key_all, value_all, dilation_step)
        branch_outs.append(branch_out)
        branch_logs.append(log_sum)
    stacked_logs = jnp.stack(branch_logs, axis=0)
    peak = lax.optimization_barrier(jnp.max(stacked_logs, axis=0))
    log_total = peak + jnp.log(lax.optimization_barrier(jnp.sum(jnp.exp(stacked_logs - peak[None]), axis=0)))
    shares = jnp.exp(stacked_logs - log_total[None])
    attended = lax.optimization_barrier(jnp.sum(shares[..., None] * jnp.stack(branch_outs, axis=0), axis=0))
    attended = attended.astype(jnp.bfloat16).reshape(sequence_rows, HEADS * HEAD_DIM)
    mixed = jnp.dot(attended, w_out, preferred_element_type=jnp.float32).astype(jnp.bfloat16)
    return (mixed, log_total)
```

```python
import functools
import math

import jax
import jax.numpy as jnp
import numpy as np
from jax import lax
from jax.experimental import pallas as pl
from jax.experimental.pallas import tpu as pltpu
from jax.sharding import PartitionSpec as P

D = 2048
KEYS_BEHIND = 128
MIDDLE_DILATION = 4
WIDEST_DILATION = 16


EPSILON = 1e-06
ROTARY_BASE = 500000.0


def from_behind(value, axis, steps):
    count = lax.axis_size(axis)
    initial, last = (max(0, -steps), min(count, count - steps))
    return lax.ppermute(value, axis, [(source, source + steps) for source in range(initial, last)])


def rotate(values, positions):
    head_width = values.shape[-1]
    inverse = ROTARY_BASE ** (-jnp.arange(0, head_width, 2, dtype=jnp.float32) / head_width)
    angles = positions[:, None] * inverse[None, :]
    cosine = jnp.cos(angles)[:, None, :]
    sine = jnp.sin(angles)[:, None, :]
    half_width = head_width // 2
    first_half = values[..., :half_width]
    second_half = values[..., half_width:]
    return jnp.concatenate(
        [first_half * cosine - second_half * sine, second_half * cosine + first_half * sine],
        axis=-1,
    )


def head_norm(values, gains):
    normed = values * lax.rsqrt(jnp.mean(values * values, axis=-1, keepdims=True) + EPSILON)
    return normed * gains[None, :, :]


def earlier_pairs(own_pair, token_rows):
    distant_shards = (KEYS_BEHIND * WIDEST_DILATION + token_rows - 1) // token_rows
    pieces = [own_pair]
    for distance in range(1, distant_shards + 1):
        pieces.insert(0, from_behind(own_pair, "sp", distance))
    buffer = jnp.concatenate(pieces, axis=1)
    return buffer


def local_branch(query, key_rows, value_rows, dilation_step, first_pos):
    token_rows, head_count, head_width = query.shape
    reach_rows = KEYS_BEHIND * dilation_step
    buffer_rows = key_rows.shape[0]
    class_rows = token_rows // dilation_step
    class_keys = class_rows + KEYS_BEHIND
    window_start = buffer_rows - token_rows - reach_rows
    key_window = key_rows[window_start:]
    value_window = value_rows[window_start:]
    query_class = query.reshape(class_rows, dilation_step, head_count, head_width).transpose(
        1, 0, 2, 3
    )
    key_class = key_window.reshape(class_keys, dilation_step, head_count, head_width).transpose(
        1, 0, 2, 3
    )
    value_class = value_window.reshape(class_keys, dilation_step, head_count, head_width).transpose(
        1, 0, 2, 3
    )
    block_rows = math.gcd(class_rows, KEYS_BEHIND) if class_rows > KEYS_BEHIND else class_rows
    block_count = class_rows // block_rows
    query_blocks = query_class.reshape(
        dilation_step, block_count, block_rows, head_count, head_width
    )
    key_blocks = jnp.stack(
        [
            key_class[:, number * block_rows : number * block_rows + block_rows + KEYS_BEHIND]
            for number in range(block_count)
        ],
        axis=1,
    )
    value_blocks = jnp.stack(
        [
            value_class[:, number * block_rows : number * block_rows + block_rows + KEYS_BEHIND]
            for number in range(block_count)
        ],
        axis=1,
    )
    scores = jnp.einsum(
        "rnqhd,rnkhd->rnhqk", query_blocks, key_blocks, preferred_element_type=jnp.float32
    ) * head_width ** (-0.5)
    row_index = jnp.arange(block_rows, dtype=jnp.int32)[:, None]
    col_index = jnp.arange(block_rows + KEYS_BEHIND, dtype=jnp.int32)[None, :]
    distance = KEYS_BEHIND + row_index - col_index
    in_band = (distance >= 0) & (distance <= KEYS_BEHIND)
    class_index = jnp.arange(block_count, dtype=jnp.int32)[:, None] * block_rows + col_index
    residue = jnp.arange(dilation_step, dtype=jnp.int32)[:, None, None]
    key_position = first_pos - reach_rows + class_index[None] * dilation_step + residue
    allowed = in_band[None, None, None, :, :] & (key_position >= 0)[:, :, None, None, :]
    scores = jnp.where(allowed, scores, -jnp.inf)
    row_max = jnp.max(scores, axis=-1, keepdims=True)
    weights = jnp.exp(scores - row_max)
    weight_sum = jnp.sum(weights, axis=-1)
    weighted = jnp.einsum(
        "rnhqk,rnkhd->rnqhd",
        weights.astype(jnp.bfloat16),
        value_blocks,
        preferred_element_type=jnp.float32,
    )
    branch_out = weighted / jnp.transpose(weight_sum, (0, 1, 3, 2))[..., None]
    branch_out = branch_out.reshape(dilation_step, class_rows, head_count, head_width).transpose(
        1, 0, 2, 3
    )
    branch_out = branch_out.reshape(token_rows, head_count, head_width)
    log_sum = jnp.transpose(row_max[..., 0] + jnp.log(weight_sum), (0, 1, 3, 2))
    log_sum = (
        log_sum.reshape(dilation_step, class_rows, head_count)
        .transpose(1, 0, 2)
        .reshape(token_rows, head_count)
    )
    return (branch_out, log_sum)


def local(hidden, norm_gain, w_query, w_key, w_value, query_gain, key_gain, w_out):
    token_rows = hidden.shape[0]
    local_width = w_query.shape[1]
    head_count = query_gain.shape[0]
    head_width = query_gain.shape[1]
    gain_full = norm_gain.astype(jnp.float32)
    raw_piece = lax.all_gather(hidden, "tp", axis=1, tiled=True).astype(jnp.float32)
    scaled = (raw_piece * gain_full[None, :]).astype(jnp.bfloat16)

    def add_product(weight):
        return jnp.dot(scaled, weight, preferred_element_type=jnp.float32)

    query_raw = add_product(w_query)
    key_raw = add_product(w_key)
    value_raw = add_product(w_value)
    squares = jnp.sum(raw_piece * raw_piece, axis=1)
    row_scale = lax.rsqrt(squares / D + EPSILON)[:, None]
    first_pos = lax.axis_index("sp") * token_rows
    positions = (jnp.arange(token_rows, dtype=jnp.int32) + first_pos).astype(jnp.float32)
    query = rotate(
        head_norm((query_raw * row_scale).reshape(token_rows, head_count, head_width), query_gain),
        positions,
    ).astype(jnp.bfloat16)
    key_now = rotate(
        head_norm((key_raw * row_scale).reshape(token_rows, head_count, head_width), key_gain),
        positions,
    ).astype(jnp.bfloat16)
    value_now = (value_raw * row_scale).astype(jnp.bfloat16)
    own_pair = jnp.stack([key_now.reshape(token_rows, local_width), value_now], axis=0)
    buffer = earlier_pairs(own_pair, token_rows)
    key_rows = buffer[0].reshape(-1, head_count, head_width)
    value_rows = buffer[1].reshape(-1, head_count, head_width)
    branch_outs = []
    branch_logs = []
    for dilation_step in (1, MIDDLE_DILATION, WIDEST_DILATION):
        branch_out, log_sum = local_branch(query, key_rows, value_rows, dilation_step, first_pos)
        branch_outs.append(branch_out)
        branch_logs.append(log_sum)
    stacked_logs = jnp.stack(branch_logs, axis=0)
    peak = jnp.max(stacked_logs, axis=0)
    log_total = peak + jnp.log(jnp.sum(jnp.exp(stacked_logs - peak[None]), axis=0))
    shares = jnp.exp(stacked_logs - log_total[None])
    attended = jnp.sum(shares[..., None] * jnp.stack(branch_outs, axis=0), axis=0)
    attended = attended.astype(jnp.bfloat16).reshape(token_rows, local_width)
    column_block = lax.all_to_all(w_out, "tp", split_axis=1, concat_axis=0, tiled=True)
    mixed = jnp.dot(
        lax.all_gather(attended, "tp", axis=1, tiled=True),
        column_block,
        preferred_element_type=jnp.float32,
    )
    return (mixed.astype(jnp.bfloat16), log_total)


MESH = pl.DeviceIdType.MESH
LANES = 128


def rotary_table(classes, rows, head_width):
    inverse = (ROTARY_BASE ** (-np.arange(0, head_width, 2, dtype=np.float64) / head_width)).astype(np.float32)
    positions = np.arange(classes * classes * rows, dtype=np.float32)
    angles = (positions[:, None] * inverse[None, :]).astype(np.float64)
    cosine, sine = np.cos(angles), np.sin(angles)
    table = np.concatenate([cosine, cosine, -sine, sine], axis=1).astype(np.float32)
    return table.reshape(classes, rows, classes, 2 * head_width).transpose(0, 2, 1, 3)


def class_kernel(
    hid_ref, gain_ref, qgain_ref, kgain_ref, wq_ref, wk_ref, wv_ref, wo_ref, table_ref,
    mixed_ref, total_ref,
    hid, gain_in, qgain, kgain, hb, hm, wall, wo, tb, tm, acc, acc_m, sq, qkv_b, qkv_c,
    halo, oc, lsend, ro, rl, near_out, near_log, all_log, at, gain, drain,
    loc, sent, zr, axr, acr, afr, cxr, ccr, cfr, wor, wfr, qr, hs, hr, rr, lr, gxr, gcr, gfr,
):
    f32, bf16 = jnp.float32, jnp.bfloat16
    g, s, p = lax.axis_index("grp"), lax.axis_index("sp"), lax.axis_index("tp")
    n = MIDDLE_DILATION
    rows, width = hid_ref.shape
    sub = rows // n
    heads, hd = qgain_ref.shape
    lw = heads * hd
    halo_sub = halo.shape[2]
    halo_rows = n * halo_sub
    core = p + 1 - 2 * lax.rem(p, 2)
    xp = lax.rem(p + 2, 4)
    diag = lax.rem(core + 2, 4)
    pair, two, mirror = s + 1 - 2 * lax.rem(s, 2), lax.rem(s + 2, n), n - 1 - s
    peer = (s, pair, two, mirror)
    chunk_order = (two, pair, s, mirror)

    def copy_to(axis, src, dst, ss, sr, q):
        return pltpu.make_async_remote_copy(
            src_ref=src, dst_ref=dst, send_sem=ss, recv_sem=sr, device_id={axis: q}, device_id_type=MESH
        )

    tp_copy = functools.partial(copy_to, "tp")
    sp_copy = functools.partial(copy_to, "sp")

    def same(copy, ref, sr, q):
        return copy(ref, ref, sent, sr, q)

    load_hid = pltpu.make_async_copy(hid_ref, hid, loc.at[1])
    load_hid.start()
    barrier = pltpu.get_barrier_semaphore()
    for k in (3, 2, 1):
        pl.semaphore_signal(barrier, inc=1, device_id={"sp": peer[k]}, device_id_type=MESH)
    for q in (xp, diag, core):
        pl.semaphore_signal(barrier, inc=1, device_id={"tp": q}, device_id_type=MESH)
    pl.semaphore_signal(barrier, inc=1, device_id={"grp": 1 - g}, device_id_type=MESH)
    loads = [
        pltpu.make_async_copy(gain_ref, gain_in, loc.at[0]),
        pltpu.make_async_copy(qgain_ref, qgain, loc.at[2]),
        pltpu.make_async_copy(kgain_ref, kgain, loc.at[3]),
        pltpu.make_async_copy(wq_ref, wall.at[:, pl.ds(0, lw)], loc.at[4]),
        pltpu.make_async_copy(wk_ref, wall.at[:, pl.ds(lw, lw)], loc.at[5]),
        pltpu.make_async_copy(wv_ref, wall.at[:, pl.ds(2 * lw, lw)], loc.at[6]),
        pltpu.make_async_copy(table_ref.at[s], tb, loc.at[7]),
        pltpu.make_async_copy(table_ref.at[mirror, s], tm, loc.at[8]),
        pltpu.make_async_copy(
            wo_ref.at[:, pl.ds(pl.multiple_of(p * width, LANES), width)], wo.at[p], loc.at[9]
        ),
    ]
    for load in loads:
        load.start()

    def iota(shape, dim):
        return lax.broadcasted_iota(jnp.int32, shape, dim)

    def row_of(r, part):
        return n * lax.rem(r, part) + r // part

    square = (rows, rows)
    to_class = (row_of(iota(square, 0), sub) == iota(square, 1)).astype(f32).astype(bf16)
    load_hid.wait()
    permuted = jnp.dot(to_class, hid[...], preferred_element_type=f32).astype(bf16)
    hb[p] = permuted.reshape(n, sub, width)
    pl.semaphore_wait(barrier, 3 + n)

    sends = []

    def go(copy):
        copy.start()
        sends.append(math.prod(copy.src_ref.shape) * copy.src_ref.dtype.itemsize)
        return copy

    part = sub // 2
    zs = [
        go(sp_copy(hb.at[p, mirror, pl.ds(a * part, part), :], hm.at[p, a], sent, zr.at[a], mirror))
        for a in range(2)
    ]
    ax = [same(tp_copy, hb.at[p, c], axr.at[j], xp) for j, c in enumerate(chunk_order)]
    for copy in ax[:3]:
        go(copy)
    ac = go(same(tp_copy, hb.at[p], acr, core))
    w_sends = [
        go(tp_copy(wo_ref.at[:, pl.ds(pl.multiple_of(core * width, LANES), width)], wo.at[p], sent, wor.at[0], core))
    ]

    for load in loads:
        load.wait()
    flat_gain = gain_in[...].astype(f32)
    for j in range(flat_gain.shape[0]):
        each = width // LANES
        gain[j // each, :, (j % each) * LANES : (j % each + 1) * LANES] = flat_gain[j : j + 1]

    def chunk(raw, q):
        raw = raw.astype(f32)
        scaled = (raw * gain[q]).astype(bf16)
        w = wall[pl.ds(pl.multiple_of(q * width, LANES), width), :]
        return jnp.dot(scaled, w, preferred_element_type=f32), jnp.sum(raw * raw, axis=1, keepdims=True)

    def add_all(q, first):
        prod, more = chunk(hb[q].reshape(rows, width), q)
        prod, more = prod.reshape(n, sub, 3 * lw), more.reshape(n, sub, 1)
        acc[...] = prod if first else acc[...] + prod
        sq[...] = more if first else sq[...] + more

    add_all(p, True)
    ac.wait_recv()
    add_all(core, False)

    def finish(acc, sq, table, places):
        raw = acc * lax.rsqrt(sq / (width * 4) + EPSILON)
        cosine, sine = table[:, :hd], table[:, hd:]
        for h in range(heads):
            for j, gains in enumerate((qgain, kgain, None)):
                x = raw[:, j * lw + h * hd : j * lw + (h + 1) * hd]
                if gains is not None:
                    x = x * lax.rsqrt(jnp.mean(x * x, axis=-1, keepdims=True) + EPSILON)
                    x = x * gains[pl.ds(h, 1), :]
                    x = x * cosine + pltpu.roll(x, hd // 2, 1) * sine
                for ref, c in places:
                    ref[c, h, :, j * hd : (j + 1) * hd] = x.astype(bf16)

    def take(j):
        ax[j].wait_recv()
        go(same(tp_copy, hb.at[xp, chunk_order[j]], afr.at[j], core))

    def close(j, places, between):
        c = chunk_order[j]
        prod, more = chunk(hb[xp, c], xp)
        between()
        same(tp_copy, hb.at[diag, c], afr.at[j], core).wait_recv()
        last, most = chunk(hb[diag, c], diag)
        finish(acc[c] + prod + last, sq[c] + more + most, tb[c], places)

    cx, cc = {}, {}

    def spread(a):
        zs[a].wait_recv()
        cx[a] = go(same(tp_copy, hm.at[p, a], cxr.at[a], xp))
        cc[a] = go(same(tp_copy, hm.at[p, a], ccr, core))

    def cross(a):
        cx[a].wait_recv()
        go(same(tp_copy, hm.at[xp, a], cfr, core))

    def give(k):
        for h in range(heads):
            go(sp_copy(qkv_b.at[peer[k], h], qkv_c.at[s, h], sent, qr.at[k - 1, h], peer[k]))

    half = lw // 2
    mine = pl.ds(pl.multiple_of(g * half, 8), half)

    def spread_last():
        spread(1)
        go(ax[3])
        for j, q in ((1, xp), (2, diag)):
            w_sends.append(go(tp_copy(
                wo_ref.at[mine, pl.ds(pl.multiple_of(q * width, LANES), width)], wo.at[p, mine], sent, wor.at[j], q
            )))

    def add_mirror(q):
        prod, more = chunk(hm[q].reshape(sub, width), q)
        return prod, more

    squares = []

    def start_mirror():
        same(tp_copy, hm.at[core], ccr, core).wait_recv()
        first, one = add_mirror(p)
        prod, more = add_mirror(core)
        acc_m[...] = first + prod
        squares.append(one + more)
        cross(0)

    take(0)
    close(0, ((qkv_b, two),), functools.partial(spread, 0))
    give(2)
    take(1)
    close(1, ((qkv_b, pair),), spread_last)
    give(1)
    take(2)
    close(2, ((qkv_b, s), (qkv_c, s)), start_mirror)

    above = lax.rem(s + 1, n)

    def send_halo(cs):
        @pl.when(s < n - 1)
        def _():
            for c in cs:
                sp_copy(
                    qkv_b.at[c, :, pl.ds(sub - halo_sub, halo_sub), pl.ds(hd, 2 * hd)], halo.at[c], hs, hr, above
                ).start()

    whole_halo = sp_copy(halo, halo, hs, hr, above)
    send_halo(chunk_order[:3])

    @pl.when(s == 0)
    def _():
        halo[...] = jnp.zeros_like(halo)

    cross(1)
    prod, more = add_mirror(xp)
    same(tp_copy, hm.at[diag], cfr, core).wait_recv()
    last, most = add_mirror(diag)
    finish(acc_m[...] + prod + last, squares[0] + more + most, tm[...], ((qkv_c, mirror),))

    def attend(q, k, v, bias):
        score = lax.dot_general(q, k, (((1,), (1,)), ((), ())), preferred_element_type=f32)
        score = score * hd ** (-0.5) + bias
        top = jnp.max(score, axis=-1, keepdims=True)
        weight = jnp.exp(score - top)
        total = jnp.sum(weight, axis=-1, keepdims=True)
        out = jnp.dot(weight.astype(bf16), v, preferred_element_type=f32) / total
        return out, top + jnp.log(total)

    behind = iota(square, 0) - iota(square, 1)
    stride = WIDEST_DILATION // n
    near = (behind >= 0) & (behind <= KEYS_BEHIND)
    far = (behind >= 0) & (behind <= KEYS_BEHIND * stride) & ((behind + rows * stride) % stride == 0)
    bias_c = jnp.where(
        near & far, math.log(2.0), jnp.where(near | far, 0.0, -jnp.inf)
    ).astype(f32)
    lane = iota((rows, LANES), 1)
    pad = LANES - sub

    def three(ref, h, count):
        return [ref[:, h, :, j * hd : (j + 1) * hd].reshape(rows, hd) for j in range(count)]

    def far_head(h):
        for k in (2, 1):
            same(sp_copy, qkv_c.at[peer[k], h], qr.at[k - 1, h], peer[k]).wait_recv()
        out, lse = attend(*three(qkv_c, h, 3), bias_c)
        oc[h] = out.astype(bf16).reshape(n, sub, hd)
        for k in (3, 2, 1):
            go(sp_copy(oc.at[h, peer[k]], ro.at[s, h], sent, rr.at[k - 1, h], peer[k]))
        for b in range(n):
            column = jnp.broadcast_to(lse[b * sub : (b + 1) * sub], (sub, LANES))
            lsend[h, b] = jnp.transpose(jnp.concatenate([column, jnp.zeros((pad, LANES), f32)], axis=0))[:8]
        for k in (3, 2, 1):
            go(sp_copy(lsend.at[h, peer[k]], rl.at[s, h], sent, lr.at[k - 1, h], peer[k]))

    take(3)
    far_head(0)
    close(3, ((qkv_b, mirror),), lambda: None)
    send_halo(chunk_order[3:])
    for h in range(1, heads):
        far_head(h)

    wf = []

    def pass_on(j):
        q = (xp, diag)[j]
        w_sends[j + 1].wait_recv()
        wf.append(go(copy_to("grp", wo.at[q, mine], wo.at[q, mine], sent, wfr.at[j], 1 - g)))

    pass_on(0)

    @pl.when(s > 0)
    def _():
        whole_halo.wait_recv()

    total_keys = rows + halo_rows
    wide = (rows, total_keys)
    key = iota(wide, 1)
    key_row = jnp.where(key < rows, row_of(key, sub), row_of(key - rows, halo_sub) - halo_rows)
    behind = row_of(iota(wide, 0), sub) - key_row
    ok = (behind >= 0) & (behind <= KEYS_BEHIND) & (key_row + s * rows >= 0)
    bias_b = jnp.where(ok, 0.0, -jnp.inf).astype(f32)
    logs = jnp.zeros((rows, LANES), f32)
    for h in range(heads):
        q, k, v = three(qkv_b, h, 3)
        out, lse = attend(
            q,
            jnp.concatenate([k, halo[:, h, :, :hd].reshape(halo_rows, hd)], axis=0),
            jnp.concatenate([v, halo[:, h, :, hd:].reshape(halo_rows, hd)], axis=0),
            bias_b,
        )
        near_out[h] = out.reshape(n, sub, hd)
        logs = jnp.where(lane == h, lse, logs)
    near_log[...] = logs.reshape(n, sub, LANES)

    gx = {}

    def merge(k, h):
        b = peer[k]
        received = lsend[h, s] if k == 0 else rl[b, h]
        far_lse = jnp.transpose(
            jnp.concatenate([received, jnp.zeros((LANES - 8, LANES), f32)], axis=0)
        )[:sub, :1]
        lse = near_log[b][:, h : h + 1]
        far_out = (oc[h, s] if k == 0 else ro[b, h]).astype(f32)
        top = jnp.maximum(lse, far_lse)
        e_near, e_far = jnp.exp(lse - top), jnp.exp(far_lse - top)
        both = e_near + e_far
        before = jnp.zeros((sub, LANES), f32) if h == 0 else all_log[b]
        at[p, b, h] = ((e_near * near_out[h, b] + e_far * far_out) / both).astype(bf16)
        all_log[b] = jnp.where(lane[:sub] == h, top + jnp.log(both), before)

    def share(k, h, piece):
        gx[k, h] = go(same(tp_copy, piece, gxr.at[k, h], xp))
        go(same(tp_copy, piece, gcr, core))

    def forward(k, h):
        gx[k, h].wait_recv()
        piece = at.at[xp, peer[k]]
        go(same(tp_copy, piece if k == 0 else piece.at[h], gfr, core))

    for h in range(heads):
        merge(0, h)
    share(0, 0, at.at[p, s])
    pass_on(1)
    for h in range(heads):
        for k in (1, 2, 3):
            same(sp_copy, ro.at[peer[k], h], rr.at[k - 1, h], peer[k]).wait_recv()
            same(sp_copy, rl.at[peer[k], h], lr.at[k - 1, h], peer[k]).wait_recv()
            merge(k, h)
            share(k, h, at.at[p, peer[k], h])
    from_class = (iota(square, 0) == row_of(iota(square, 1), sub)).astype(f32).astype(bf16)
    logs = all_log[...].reshape(rows, LANES)
    high = logs.astype(bf16)
    rest = logs - high.astype(f32)
    middle = rest.astype(bf16)
    low = (rest - middle.astype(f32)).astype(bf16)
    ordered = sum(jnp.dot(from_class, x, preferred_element_type=f32) for x in (high, middle, low))
    for j in range(rows // LANES):
        block = slice(j * LANES, (j + 1) * LANES)
        total_ref[:, block] = jnp.transpose(ordered[block])[:heads]

    def product(q):
        x = jnp.concatenate([at[q, :, h].reshape(rows, hd) for h in range(heads)], axis=1)
        return jnp.dot(x, wo[q], preferred_element_type=f32)

    result = product(p)
    forward(0, 0)
    w_sends[0].wait_recv()
    same(tp_copy, at.at[core], gcr, core).wait_recv()
    result += product(core)
    for h in range(heads):
        for k in (1, 2, 3):
            forward(k, h)
    for copy in wf:
        copy.wait_recv()
    result += product(xp)
    same(tp_copy, at.at[diag], gfr, core).wait_recv()
    result += product(diag)
    mixed_ref[...] = jnp.dot(from_class, result.astype(bf16), preferred_element_type=f32).astype(bf16)
    assert sum(sends) == drain.shape[0] * LANES * 4
    same(tp_copy, drain, acr, core).wait_send()

    @pl.when(s < n - 1)
    def _():
        whole_halo.wait_send()


def local_by_class(hidden, norm_gain, w_query, w_key, w_value, query_gain, key_gain, w_out):
    n = MIDDLE_DILATION
    rows, width = hidden.shape
    heads, hd = query_gain.shape
    lw = heads * hd
    sub = rows // n
    halo_sub = KEYS_BEHIND // n
    bf16, f32 = jnp.bfloat16, jnp.float32
    table = jnp.asarray(rotary_table(n, sub, hd))
    sent_bytes = 2 * (16 * sub * width + 3 * lw * width + 21 * sub * lw) + 3 * heads * 8 * LANES * 4
    vmem = pl.BlockSpec(memory_space=pltpu.VMEM)
    anyspace = pl.BlockSpec(memory_space=pl.ANY)
    dma = pltpu.SemaphoreType.DMA
    mixed, total = pl.pallas_call(
        class_kernel,
        out_shape=(
            pltpu.VMEM((rows, w_out.shape[1] // 4), bf16),
            pltpu.VMEM((heads, rows), f32),
        ),
        in_specs=[anyspace] * 9,
        out_specs=(vmem, vmem),
        scratch_shapes=[
            pltpu.VMEM((rows, width), bf16),
            pltpu.VMEM((4 * width // LANES, LANES), bf16),
            pltpu.VMEM((heads, hd), f32),
            pltpu.VMEM((heads, hd), f32),
            pltpu.VMEM((4, n, sub, width), bf16),
            pltpu.VMEM((4, 2, sub // 2, width), bf16),
            pltpu.VMEM((4 * width, 3 * lw), bf16),
            pltpu.VMEM((4, lw, width), bf16),
            pltpu.VMEM((n, sub, 2 * hd), f32),
            pltpu.VMEM((sub, 2 * hd), f32),
            pltpu.VMEM((n, sub, 3 * lw), f32),
            pltpu.VMEM((sub, 3 * lw), f32),
            pltpu.VMEM((n, sub, 1), f32),
            pltpu.VMEM((n, heads, sub, 3 * hd), bf16),
            pltpu.VMEM((n, heads, sub, 3 * hd), bf16),
            pltpu.VMEM((n, heads, halo_sub, 2 * hd), bf16),
            pltpu.VMEM((heads, n, sub, hd), bf16),
            pltpu.VMEM((heads, n, 8, LANES), f32),
            pltpu.VMEM((n, heads, sub, hd), bf16),
            pltpu.VMEM((n, heads, 8, LANES), f32),
            pltpu.VMEM((heads, n, sub, hd), f32),
            pltpu.VMEM((n, sub, LANES), f32),
            pltpu.VMEM((n, sub, LANES), f32),
            pltpu.VMEM((4, n, heads, sub, hd), bf16),
            pltpu.VMEM((4, 1, width), f32),
            pltpu.VMEM((sent_bytes // (4 * LANES), LANES), f32),
            dma((10,)), dma, dma((2,)), dma((n,)), dma, dma((n,)), dma((2,)), dma, dma,
            dma((3,)), dma((2,)), dma((2, heads)), dma, dma, dma((3, heads)), dma((3, heads)),
            dma((n, heads)), dma, dma,
        ],
        compiler_params=pltpu.CompilerParams(
            collective_id=0, has_side_effects=True, vmem_limit_bytes=60 * 1024 * 1024
        ),
    )(
        hidden, norm_gain.reshape(-1, LANES), query_gain, key_gain,
        w_query, w_key, w_value, w_out, table,
    )
    return mixed, total.T


def solution(mesh):
    split = (mesh.shape["grp"], mesh.shape["sp"], mesh.shape["tp"]) == (2, MIDDLE_DILATION, 4)
    chosen = local_by_class if split else local
    placed = (
        P(("grp", "sp"), "tp"),
        P(),
        P(None, "tp"),
        P(None, "tp"),
        P(None, "tp"),
        P("tp", None),
        P("tp", None),
        P("tp", None),
    )
    return jax.shard_map(
        chosen,
        mesh=mesh,
        in_specs=placed,
        out_specs=(P(("grp", "sp"), "tp"), P(("grp", "sp"), "tp")),
        check_vma=False,
    )
```

```python
import functools
import math

import jax
import jax.numpy as jnp
import numpy as np
from jax import lax
from jax.experimental import pallas as pl
from jax.experimental.pallas import tpu as pltpu
from jax.sharding import PartitionSpec as P

D = 2048
KEYS_BEHIND = 128
MIDDLE_DILATION = 4
WIDEST_DILATION = 16


EPSILON = 1e-06
ROTARY_BASE = 500000.0


def from_behind(value, axis, steps):
    count = lax.axis_size(axis)
    initial, last = (max(0, -steps), min(count, count - steps))
    return lax.ppermute(value, axis, [(source, source + steps) for source in range(initial, last)])


def rotate(values, positions):
    head_width = values.shape[-1]
    inverse = ROTARY_BASE ** (-jnp.arange(0, head_width, 2, dtype=jnp.float32) / head_width)
    angles = positions[:, None] * inverse[None, :]
    cosine = jnp.cos(angles)[:, None, :]
    sine = jnp.sin(angles)[:, None, :]
    half_width = head_width // 2
    first_half = values[..., :half_width]
    second_half = values[..., half_width:]
    return jnp.concatenate(
        [first_half * cosine - second_half * sine, second_half * cosine + first_half * sine],
        axis=-1,
    )


def head_norm(values, gains):
    normed = values * lax.rsqrt(jnp.mean(values * values, axis=-1, keepdims=True) + EPSILON)
    return normed * gains[None, :, :]


def earlier_pairs(own_pair, token_rows):
    distant_shards = (KEYS_BEHIND * WIDEST_DILATION + token_rows - 1) // token_rows
    pieces = [own_pair]
    for distance in range(1, distant_shards + 1):
        pieces.insert(0, from_behind(own_pair, "sp", distance))
    buffer = jnp.concatenate(pieces, axis=1)
    return buffer


def local_branch(query, key_rows, value_rows, dilation_step, first_pos):
    token_rows, head_count, head_width = query.shape
    reach_rows = KEYS_BEHIND * dilation_step
    buffer_rows = key_rows.shape[0]
    class_rows = token_rows // dilation_step
    class_keys = class_rows + KEYS_BEHIND
    window_start = buffer_rows - token_rows - reach_rows
    key_window = key_rows[window_start:]
    value_window = value_rows[window_start:]
    query_class = query.reshape(class_rows, dilation_step, head_count, head_width).transpose(
        1, 0, 2, 3
    )
    key_class = key_window.reshape(class_keys, dilation_step, head_count, head_width).transpose(
        1, 0, 2, 3
    )
    value_class = value_window.reshape(class_keys, dilation_step, head_count, head_width).transpose(
        1, 0, 2, 3
    )
    block_rows = math.gcd(class_rows, KEYS_BEHIND) if class_rows > KEYS_BEHIND else class_rows
    block_count = class_rows // block_rows
    query_blocks = query_class.reshape(
        dilation_step, block_count, block_rows, head_count, head_width
    )
    key_blocks = jnp.stack(
        [
            key_class[:, number * block_rows : number * block_rows + block_rows + KEYS_BEHIND]
            for number in range(block_count)
        ],
        axis=1,
    )
    value_blocks = jnp.stack(
        [
            value_class[:, number * block_rows : number * block_rows + block_rows + KEYS_BEHIND]
            for number in range(block_count)
        ],
        axis=1,
    )
    scores = jnp.einsum(
        "rnqhd,rnkhd->rnhqk", query_blocks, key_blocks, preferred_element_type=jnp.float32
    ) * head_width ** (-0.5)
    row_index = jnp.arange(block_rows, dtype=jnp.int32)[:, None]
    col_index = jnp.arange(block_rows + KEYS_BEHIND, dtype=jnp.int32)[None, :]
    distance = KEYS_BEHIND + row_index - col_index
    in_band = (distance >= 0) & (distance <= KEYS_BEHIND)
    class_index = jnp.arange(block_count, dtype=jnp.int32)[:, None] * block_rows + col_index
    residue = jnp.arange(dilation_step, dtype=jnp.int32)[:, None, None]
    key_position = first_pos - reach_rows + class_index[None] * dilation_step + residue
    allowed = in_band[None, None, None, :, :] & (key_position >= 0)[:, :, None, None, :]
    scores = jnp.where(allowed, scores, -jnp.inf)
    row_max = jnp.max(scores, axis=-1, keepdims=True)
    weights = jnp.exp(scores - row_max)
    weight_sum = jnp.sum(weights, axis=-1)
    weighted = jnp.einsum(
        "rnhqk,rnkhd->rnqhd",
        weights.astype(jnp.bfloat16),
        value_blocks,
        preferred_element_type=jnp.float32,
    )
    branch_out = weighted / jnp.transpose(weight_sum, (0, 1, 3, 2))[..., None]
    branch_out = branch_out.reshape(dilation_step, class_rows, head_count, head_width).transpose(
        1, 0, 2, 3
    )
    branch_out = branch_out.reshape(token_rows, head_count, head_width)
    log_sum = jnp.transpose(row_max[..., 0] + jnp.log(weight_sum), (0, 1, 3, 2))
    log_sum = (
        log_sum.reshape(dilation_step, class_rows, head_count)
        .transpose(1, 0, 2)
        .reshape(token_rows, head_count)
    )
    return (branch_out, log_sum)


def local(hidden, norm_gain, w_query, w_key, w_value, query_gain, key_gain, w_out):
    token_rows = hidden.shape[0]
    local_width = w_query.shape[1]
    head_count = query_gain.shape[0]
    head_width = query_gain.shape[1]
    gain_full = norm_gain.astype(jnp.float32)
    raw_piece = lax.all_gather(hidden, "tp", axis=1, tiled=True).astype(jnp.float32)
    scaled = (raw_piece * gain_full[None, :]).astype(jnp.bfloat16)

    def add_product(weight):
        return jnp.dot(scaled, weight, preferred_element_type=jnp.float32)

    query_raw = add_product(w_query)
    key_raw = add_product(w_key)
    value_raw = add_product(w_value)
    squares = jnp.sum(raw_piece * raw_piece, axis=1)
    row_scale = lax.rsqrt(squares / D + EPSILON)[:, None]
    first_pos = lax.axis_index("sp") * token_rows
    positions = (jnp.arange(token_rows, dtype=jnp.int32) + first_pos).astype(jnp.float32)
    query = rotate(
        head_norm((query_raw * row_scale).reshape(token_rows, head_count, head_width), query_gain),
        positions,
    ).astype(jnp.bfloat16)
    key_now = rotate(
        head_norm((key_raw * row_scale).reshape(token_rows, head_count, head_width), key_gain),
        positions,
    ).astype(jnp.bfloat16)
    value_now = (value_raw * row_scale).astype(jnp.bfloat16)
    own_pair = jnp.stack([key_now.reshape(token_rows, local_width), value_now], axis=0)
    buffer = earlier_pairs(own_pair, token_rows)
    key_rows = buffer[0].reshape(-1, head_count, head_width)
    value_rows = buffer[1].reshape(-1, head_count, head_width)
    branch_outs = []
    branch_logs = []
    for dilation_step in (1, MIDDLE_DILATION, WIDEST_DILATION):
        branch_out, log_sum = local_branch(query, key_rows, value_rows, dilation_step, first_pos)
        branch_outs.append(branch_out)
        branch_logs.append(log_sum)
    stacked_logs = jnp.stack(branch_logs, axis=0)
    peak = jnp.max(stacked_logs, axis=0)
    log_total = peak + jnp.log(jnp.sum(jnp.exp(stacked_logs - peak[None]), axis=0))
    shares = jnp.exp(stacked_logs - log_total[None])
    attended = jnp.sum(shares[..., None] * jnp.stack(branch_outs, axis=0), axis=0)
    attended = attended.astype(jnp.bfloat16).reshape(token_rows, local_width)
    column_block = lax.all_to_all(w_out, "tp", split_axis=1, concat_axis=0, tiled=True)
    mixed = jnp.dot(
        lax.all_gather(attended, "tp", axis=1, tiled=True),
        column_block,
        preferred_element_type=jnp.float32,
    )
    return (mixed.astype(jnp.bfloat16), log_total)


MESH = pl.DeviceIdType.MESH
LANES = 128


def rotary_table(classes, rows, head_width):
    inverse = (ROTARY_BASE ** (-np.arange(0, head_width, 2, dtype=np.float64) / head_width)).astype(np.float32)
    positions = np.arange(classes * classes * rows, dtype=np.float32)
    angles = (positions[:, None] * inverse[None, :]).astype(np.float64)
    cosine, sine = np.cos(angles), np.sin(angles)
    table = np.concatenate([cosine, cosine, -sine, sine], axis=1).astype(np.float32)
    return table.reshape(classes, rows, classes, 2 * head_width).transpose(0, 2, 1, 3)


def class_kernel(
    hid_ref, gain_ref, qgain_ref, kgain_ref, wq_ref, wk_ref, wv_ref, wo_ref, table_ref,
    mixed_ref, total_ref,
    hid, gain_in, qgain, kgain, hb, hm, wall, wo, tb, tm, acc, acc_m, sq, q_b, kv_b, q_c, kv_c,
    halo, oc, lsend, ro, rl, near_out, near_row, halo_out, halo_row, all_log, at, gain, drain,
    loc, sent, zr, axr, acr, afr, cxr, ccr, cfr, wor, wfr, qr, kr, hr, rr, lr, gxr, gcr, gfr,
):
    f32, bf16 = jnp.float32, jnp.bfloat16
    g, s, p = lax.axis_index("grp"), lax.axis_index("sp"), lax.axis_index("tp")
    n = MIDDLE_DILATION
    rows, width = hid_ref.shape
    sub = rows // n
    heads, hd = qgain_ref.shape
    lw = heads * hd
    halo_sub = halo.shape[2]
    halo_rows = n * halo_sub
    core = p + 1 - 2 * lax.rem(p, 2)
    xp = lax.rem(p + 2, 4)
    diag = lax.rem(core + 2, 4)
    pair, two, mirror = s + 1 - 2 * lax.rem(s, 2), lax.rem(s + 2, n), n - 1 - s
    peer = (s, pair, two, mirror)
    part = sub // 2
    pieces = ((two, 0, part), (two, part, part), (pair, 0, sub), (s, 0, sub), (mirror, 0, sub))

    def copy_to(axis, src, dst, ss, sr, q):
        return pltpu.make_async_remote_copy(
            src_ref=src, dst_ref=dst, send_sem=ss, recv_sem=sr, device_id={axis: q}, device_id_type=MESH
        )

    tp_copy = functools.partial(copy_to, "tp")
    sp_copy = functools.partial(copy_to, "sp")

    def same(copy, ref, sr, q):
        return copy(ref, ref, sent, sr, q)

    load_hid = pltpu.make_async_copy(hid_ref, hid, loc.at[1])
    load_hid.start()
    barrier = pltpu.get_barrier_semaphore()
    for k in (3, 2, 1):
        pl.semaphore_signal(barrier, inc=1, device_id={"sp": peer[k]}, device_id_type=MESH)
    for q in (xp, diag, core):
        pl.semaphore_signal(barrier, inc=1, device_id={"tp": q}, device_id_type=MESH)
    pl.semaphore_signal(barrier, inc=1, device_id={"grp": 1 - g}, device_id_type=MESH)
    loads = [
        pltpu.make_async_copy(gain_ref, gain_in, loc.at[0]),
        pltpu.make_async_copy(qgain_ref, qgain, loc.at[2]),
        pltpu.make_async_copy(kgain_ref, kgain, loc.at[3]),
        pltpu.make_async_copy(wq_ref, wall.at[:, pl.ds(0, lw)], loc.at[4]),
        pltpu.make_async_copy(wk_ref, wall.at[:, pl.ds(lw, lw)], loc.at[5]),
        pltpu.make_async_copy(wv_ref, wall.at[:, pl.ds(2 * lw, lw)], loc.at[6]),
        pltpu.make_async_copy(table_ref.at[s], tb, loc.at[7]),
        pltpu.make_async_copy(table_ref.at[mirror, s], tm, loc.at[8]),
        pltpu.make_async_copy(
            wo_ref.at[:, pl.ds(pl.multiple_of(p * width, LANES), width)], wo.at[p], loc.at[9]
        ),
    ]
    for load in loads:
        load.start()

    def iota(shape, dim):
        return lax.broadcasted_iota(jnp.int32, shape, dim)

    def row_of(r, part):
        return n * lax.rem(r, part) + r // part

    square = (rows, rows)
    to_class = (row_of(iota(square, 0), sub) == iota(square, 1)).astype(f32).astype(bf16)
    load_hid.wait()
    permuted = jnp.dot(to_class, hid[...], preferred_element_type=f32).astype(bf16)
    hb[p] = permuted.reshape(n, sub, width)
    pl.semaphore_wait(barrier, 3 + n)

    sends = []

    def go(copy):
        copy.start()
        sends.append(math.prod(copy.src_ref.shape) * copy.src_ref.dtype.itemsize)
        return copy

    zs = [
        go(sp_copy(hb.at[p, mirror, pl.ds(a * part, part), :], hm.at[p, a], sent, zr.at[a], mirror))
        for a in range(2)
    ]
    ax = [same(tp_copy, hb.at[p, c, pl.ds(i, m), :], axr.at[j], xp) for j, (c, i, m) in enumerate(pieces)]
    for copy in ax[:4]:
        go(copy)
    ac = go(same(tp_copy, hb.at[p], acr, core))
    w_sends = [
        go(tp_copy(wo_ref.at[:, pl.ds(pl.multiple_of(core * width, LANES), width)], wo.at[p], sent, wor.at[0], core))
    ]

    for load in loads:
        load.wait()
    flat_gain = gain_in[...].astype(f32)
    for j in range(flat_gain.shape[0]):
        each = width // LANES
        gain[j // each, :, (j % each) * LANES : (j % each + 1) * LANES] = flat_gain[j : j + 1]

    def chunk(raw, q):
        raw = raw.astype(f32)
        scaled = (raw * gain[q]).astype(bf16)
        w = wall[pl.ds(pl.multiple_of(q * width, LANES), width), :]
        return jnp.dot(scaled, w, preferred_element_type=f32), jnp.sum(raw * raw, axis=1, keepdims=True)

    def add_all(q, first):
        prod, more = chunk(hb[q].reshape(rows, width), q)
        prod, more = prod.reshape(n, sub, 3 * lw), more.reshape(n, sub, 1)
        acc[...] = prod if first else acc[...] + prod
        sq[...] = more if first else sq[...] + more

    add_all(p, True)
    ac.wait_recv()
    add_all(core, False)

    def finish(acc, sq, table, places, span):
        raw = acc * lax.rsqrt(sq / (width * 4) + EPSILON)
        cosine, sine = table[:, :hd], table[:, hd:]
        for h in range(heads):
            for j, gains in enumerate((qgain, kgain, None)):
                x = raw[:, j * lw + h * hd : j * lw + (h + 1) * hd]
                if gains is not None:
                    x = x * lax.rsqrt(jnp.mean(x * x, axis=-1, keepdims=True) + EPSILON)
                    x = x * gains[pl.ds(h, 1), :]
                    x = x * cosine + pltpu.roll(x, hd // 2, 1) * sine
                for q_ref, kv_ref, c in places:
                    if j == 0:
                        q_ref[c, h, span] = x.astype(bf16)
                    else:
                        kv_ref[c, h, span, (j - 1) * hd : j * hd] = x.astype(bf16)

    def take(j):
        c, i, m = pieces[j]
        ax[j].wait_recv()
        go(same(tp_copy, hb.at[xp, c, pl.ds(i, m), :], afr.at[j], core))

    def close(j, places, between):
        c, i, m = pieces[j]
        span = slice(i, i + m)
        prod, more = chunk(hb[xp, c, span], xp)
        between()
        same(tp_copy, hb.at[diag, c, pl.ds(i, m), :], afr.at[j], core).wait_recv()
        last, most = chunk(hb[diag, c, span], diag)
        finish(acc[c, span] + prod + last, sq[c, span] + more + most, tb[c, span], places, span)

    cx, cc = {}, {}

    def spread(a):
        zs[a].wait_recv()
        cx[a] = go(same(tp_copy, hm.at[p, a], cxr.at[a], xp))
        cc[a] = go(same(tp_copy, hm.at[p, a], ccr, core))

    def cross(a):
        cx[a].wait_recv()
        go(same(tp_copy, hm.at[xp, a], cfr, core))

    parts_of = {1: pieces[2:3], 2: pieces[:2]}

    def class_copy(own, other, sems, k, h, j, arriving):
        _, i, m = parts_of[k][j]
        q = peer[k]
        mine = other.at[q, h, pl.ds(i, m), :]
        if arriving:
            return same(sp_copy, mine, sems.at[k - 1, h, j], q)
        return sp_copy(own.at[q, h, pl.ds(i, m), :], other.at[s, h, pl.ds(i, m), :], sent, sems.at[k - 1, h, j], q)

    kv_copy = functools.partial(class_copy, kv_b, kv_c, kr)
    q_copy = functools.partial(class_copy, q_b, q_c, qr)

    def give(k, j):
        for h in range(heads):
            @pl.when(s < n - 1)
            def _():
                kv_copy(k, h, j, False).start()

            @pl.when(s > 0)
            def _():
                q_copy(k, h, j, False).start()

    def receive(k, h):
        @pl.when(peer[k] < n - 1)
        def _():
            for j in range(len(parts_of[k])):
                kv_copy(k, h, j, True).wait_recv()

        @pl.when(peer[k] > 0)
        def _():
            for j in range(len(parts_of[k])):
                q_copy(k, h, j, True).wait_recv()

    half = lw // 2
    mine = pl.ds(pl.multiple_of(g * half, 8), half)

    def spread_last():
        spread(1)
        go(ax[4])
        for j, q in ((1, xp), (2, diag)):
            w_sends.append(go(tp_copy(
                wo_ref.at[mine, pl.ds(pl.multiple_of(q * width, LANES), width)], wo.at[p, mine], sent, wor.at[j], q
            )))

    def add_mirror(q):
        prod, more = chunk(hm[q].reshape(sub, width), q)
        return prod, more

    squares = []

    def start_mirror():
        same(tp_copy, hm.at[core], ccr, core).wait_recv()
        first, one = add_mirror(p)
        prod, more = add_mirror(core)
        acc_m[...] = first + prod
        squares.append(one + more)
        cross(0)

    take(0)
    close(0, ((q_b, kv_b, two),), lambda: None)
    give(2, 0)
    take(1)
    close(1, ((q_b, kv_b, two),), functools.partial(spread, 0))
    give(2, 1)
    take(2)
    close(2, ((q_b, kv_b, pair),), spread_last)
    give(1, 0)
    take(3)
    close(3, ((q_b, kv_b, s), (q_c, kv_c, s)), start_mirror)

    above = lax.rem(s + 1, n)

    def send_halo(c):
        sp_copy(kv_b.at[c, :, pl.ds(sub - halo_sub, halo_sub), :], halo.at[c], sent, hr, above).start()

    @pl.when(s < n - 1)
    def _():
        send_halo(two)
        send_halo(s)

    @pl.when(s == 1)
    def _():
        send_halo(pair)

    cross(1)
    prod, more = add_mirror(xp)
    same(tp_copy, hm.at[diag], cfr, core).wait_recv()
    last, most = add_mirror(diag)
    finish(acc_m[...] + prod + last, squares[0] + more + most, tm[...], ((q_c, kv_c, mirror),), slice(0, sub))

    def attend(q, k, v, bias):
        score = lax.dot_general(q, k, (((1,), (1,)), ((), ())), preferred_element_type=f32)
        score = score * hd ** (-0.5) + bias
        top = jnp.max(score, axis=-1, keepdims=True)
        weight = jnp.exp(score - top)
        total = jnp.sum(weight, axis=-1, keepdims=True)
        out = jnp.dot(weight.astype(bf16), v, preferred_element_type=f32) / total
        return out, top + jnp.log(total)

    def log_count(*read):
        count = sum(each.astype(f32) for each in read)
        bias = jnp.where(count == 2, math.log(2.0), jnp.where(count == 3, math.log(3.0), 0.0))
        return jnp.where(count == 0, -jnp.inf, bias)

    def strided(behind, step):
        return (behind >= 0) & (behind <= KEYS_BEHIND * step) & ((behind + rows * step) % step == 0)

    later = (rows - sub, rows - sub)
    late, early = iota(later, 0) + sub, iota(later, 1)
    stride = WIDEST_DILATION // n
    crosses = late // sub > early // sub
    bias_c = log_count(strided(late - early, 1) & crosses, strided(late - early, stride) & crosses)
    lane = iota((rows, LANES), 1)

    def as_rows(columns):
        spread_out = jnp.full((sub, LANES), -jnp.inf, f32)
        for c, column in enumerate(columns):
            if column is not None:
                spread_out = jnp.where(lane[:sub] == c, column, spread_out)
        pad = jnp.zeros((LANES - sub, LANES), f32)
        return jnp.transpose(jnp.concatenate([spread_out, pad], axis=0))[:8]

    def flat(x):
        return x.reshape(x.shape[0] * x.shape[1], x.shape[2])

    def far_head(h):
        receive(2, h)
        receive(1, h)
        out, lse = attend(
            flat(q_c[1:, h]), flat(kv_c[: n - 1, h, :, :hd]), flat(kv_c[: n - 1, h, :, hd:]), bias_c
        )
        oc[h, 1:] = out.astype(bf16).reshape(n - 1, sub, hd)
        for k in (3, 2, 1):
            @pl.when(peer[k] > 0)
            def _():
                sp_copy(oc.at[h, peer[k]], ro.at[s, h], sent, rr.at[k - 1, h], peer[k]).start()
        lsend[h] = as_rows([None] + [lse[b * sub : (b + 1) * sub] for b in range(n - 1)])
        rl[s, h] = lsend[h]
        for k in (3, 2, 1):
            @pl.when(peer[k] > 0)
            def _():
                sp_copy(lsend.at[h], rl.at[s, h], sent, lr.at[k - 1, h], peer[k]).start()

    far_head(0)
    take(4)
    close(4, ((q_b, kv_b, mirror),), lambda: None)

    @pl.when((s < n - 1) & (s != 1))
    def _():
        send_halo(mirror)

    for h in range(1, heads):
        far_head(h)

    wf = []

    def pass_on(j):
        q = (xp, diag)[j]
        w_sends[j + 1].wait_recv()
        wf.append(go(copy_to("grp", wo.at[q, mine], wo.at[q, mine], sent, wfr.at[j], 1 - g)))

    pass_on(0)

    behind = row_of(iota(square, 0), sub) - row_of(iota(square, 1), sub)
    bias_b = log_count(*(strided(behind, step) for step in (1, n, WIDEST_DILATION)))
    gx = [same(tp_copy, at.at[p, h], gxr.at[h], xp) for h in range(heads)]
    gc = [same(tp_copy, at.at[p, h], gcr, core) for h in range(heads)]

    def share(h):
        gx[h].start()
        gc[h].start()

    for h in range(heads):
        out, lse = attend(flat(q_b[:, h]), flat(kv_b[:, h, :, :hd]), flat(kv_b[:, h, :, hd:]), bias_b)
        near_out[h] = out.reshape(n, sub, hd)
        near_row[h] = as_rows([lse[c * sub : (c + 1) * sub] for c in range(n)])

        @pl.when(s == 0)
        def _():
            at[p, h] = near_out[h].astype(bf16)
            share(h)
            all_log[h] = near_row[h]

    @pl.when(s > 0)
    def _():
        sp_copy(halo.at[pl.ds(0, n - 1)], halo.at[pl.ds(0, n - 1)], sent, hr, above).wait_recv()
        halo[s] = kv_c[s - 1, :, sub - halo_sub :, :]
        small = (halo_rows, halo_rows)
        behind = row_of(iota(small, 0), halo_sub) - row_of(iota(small, 1), halo_sub) + halo_rows
        bias_h = jnp.where(behind <= KEYS_BEHIND, 0.0, -jnp.inf).astype(f32)
        for h in range(heads):
            out, lse = attend(
                flat(q_b[:, h, :halo_sub]), flat(halo[:, h, :, :hd]), flat(halo[:, h, :, hd:]), bias_h
            )
            halo_out[h] = out.reshape(n, halo_sub, hd)
            pad = jnp.full((sub - halo_sub, 1), -jnp.inf, f32)
            halo_row[h] = as_rows([
                jnp.concatenate([lse[c * halo_sub : (c + 1) * halo_sub], pad], axis=0) for c in range(n)
            ])

    pass_on(1)

    @pl.when(s > 0)
    def _():
        for h in range(heads):
            for k in (1, 2, 3):
                same(sp_copy, ro.at[peer[k], h], rr.at[k - 1, h], peer[k]).wait_recv()
                same(sp_copy, rl.at[peer[k], h], lr.at[k - 1, h], peer[k]).wait_recv()
            ro[s, h] = oc[h, s]
            which = iota((8, LANES), 0)
            far_row = jnp.full((8, LANES), -jnp.inf, f32)
            for c in range(n):
                far_row = jnp.where(which == c, rl[c, h, pl.ds(s, 1), :], far_row)
            own, low = near_row[h], halo_row[h]
            live = (which < n) & (iota((8, LANES), 1) < sub)
            top = jnp.where(live, jnp.maximum(jnp.maximum(own, low), far_row), 0.0)
            exps = [jnp.where(live, jnp.exp(x - top), 0.0) for x in (own, low, far_row)]
            both = jnp.where(live, exps[0] + exps[1] + exps[2], 1.0)
            all_log[h] = top + jnp.log(both)
            shares = [x / both for x in exps]
            columns = jnp.transpose(jnp.concatenate(shares + [jnp.zeros((LANES - 24, LANES), f32)], axis=0))[:sub]
            for c in range(n):
                own_part = columns[:, c : c + 1] * near_out[h, c]
                far_part = columns[:, 16 + c : 17 + c] * ro[c, h].astype(f32)
                low_part = columns[:halo_sub, 8 + c : 9 + c] * halo_out[h, c]
                sums = own_part + far_part
                sums = jnp.concatenate([sums[:halo_sub] + low_part, sums[halo_sub:]], axis=0)
                at[p, h, c] = sums.astype(bf16)
            share(h)

    from_class = (iota(square, 0) == row_of(iota(square, 1), sub)).astype(f32).astype(bf16)
    def product(q):
        x = jnp.concatenate([flat(at[q, h]) for h in range(heads)], axis=1)
        return jnp.dot(x, wo[q], preferred_element_type=f32)

    def forward(h):
        gx[h].wait_recv()
        go(same(tp_copy, at.at[xp, h], gfr, core))

    by_head = iota((8, LANES), 0)
    logs = []
    for c in range(n):
        row = jnp.zeros((8, LANES), f32)
        for h in range(heads):
            row = jnp.where(by_head == h, all_log[h, c : c + 1, :], row)
        logs.append(row)
    logs = jnp.concatenate(logs, axis=1)
    placed = (n * LANES, rows)
    to_order = (
        (n * lax.rem(iota(placed, 0), LANES) + iota(placed, 0) // LANES == iota(placed, 1))
        & (lax.rem(iota(placed, 0), LANES) < sub)
    ).astype(f32).astype(bf16)
    high = logs.astype(bf16)
    rest = logs - high.astype(f32)
    middle = rest.astype(bf16)
    low = (rest - middle.astype(f32)).astype(bf16)
    total = sum(jnp.dot(x, to_order, preferred_element_type=f32) for x in (high, middle, low))
    total_ref[...] = total[:heads]

    result = product(p)
    forward(0)
    w_sends[0].wait_recv()
    same(tp_copy, at.at[core], gcr, core).wait_recv()
    result += product(core)
    for h in range(1, heads):
        forward(h)
    for copy in wf:
        copy.wait_recv()
    result += product(xp)
    same(tp_copy, at.at[diag], gfr, core).wait_recv()
    result += product(diag)
    mixed_ref[...] = jnp.dot(from_class, result.astype(bf16), preferred_element_type=f32).astype(bf16)
    back = heads * (sub * hd * 2 + 8 * LANES * 4)
    q_bytes, kv_bytes = 2 * heads * sub * hd * 2, 2 * heads * sub * 2 * hd * 2
    halo_bytes = (n - 1) * heads * halo_sub * 2 * hd * 2
    at_bytes = 2 * rows * lw * 2

    def all_sent(total):
        same(tp_copy, drain.at[pl.ds(0, total // (LANES * 4))], acr, core).wait_send()

    @pl.when(s == 0)
    def _():
        all_sent(sum(sends) + at_bytes + kv_bytes + halo_bytes + 3 * back)

    @pl.when((s > 0) & (s < n - 1))
    def _():
        all_sent(sum(sends) + at_bytes + q_bytes + kv_bytes + halo_bytes + 2 * back)

    @pl.when(s == n - 1)
    def _():
        all_sent(sum(sends) + at_bytes + q_bytes + 2 * back)


def local_by_class(hidden, norm_gain, w_query, w_key, w_value, query_gain, key_gain, w_out):
    n = MIDDLE_DILATION
    rows, width = hidden.shape
    heads, hd = query_gain.shape
    lw = heads * hd
    sub = rows // n
    halo_sub = KEYS_BEHIND // n
    bf16, f32 = jnp.bfloat16, jnp.float32
    table = jnp.asarray(rotary_table(n, sub, hd))
    most_bytes = 2 * (16 * sub * width + 3 * lw * width + 30 * sub * lw) + 3 * heads * 8 * LANES * 4
    vmem = pl.BlockSpec(memory_space=pltpu.VMEM)
    anyspace = pl.BlockSpec(memory_space=pl.ANY)
    dma = pltpu.SemaphoreType.DMA
    mixed, total = pl.pallas_call(
        class_kernel,
        out_shape=(
            pltpu.VMEM((rows, w_out.shape[1] // 4), bf16),
            pltpu.VMEM((heads, rows), f32),
        ),
        in_specs=[anyspace] * 9,
        out_specs=(vmem, vmem),
        scratch_shapes=[
            pltpu.VMEM((rows, width), bf16),
            pltpu.VMEM((4 * width // LANES, LANES), bf16),
            pltpu.VMEM((heads, hd), f32),
            pltpu.VMEM((heads, hd), f32),
            pltpu.VMEM((4, n, sub, width), bf16),
            pltpu.VMEM((4, 2, sub // 2, width), bf16),
            pltpu.VMEM((4 * width, 3 * lw), bf16),
            pltpu.VMEM((4, lw, width), bf16),
            pltpu.VMEM((n, sub, 2 * hd), f32),
            pltpu.VMEM((sub, 2 * hd), f32),
            pltpu.VMEM((n, sub, 3 * lw), f32),
            pltpu.VMEM((sub, 3 * lw), f32),
            pltpu.VMEM((n, sub, 1), f32),
            pltpu.VMEM((n, heads, sub, hd), bf16),
            pltpu.VMEM((n, heads, sub, 2 * hd), bf16),
            pltpu.VMEM((n, heads, sub, hd), bf16),
            pltpu.VMEM((n, heads, sub, 2 * hd), bf16),
            pltpu.VMEM((n, heads, halo_sub, 2 * hd), bf16),
            pltpu.VMEM((heads, n, sub, hd), bf16),
            pltpu.VMEM((heads, 8, LANES), f32),
            pltpu.VMEM((n, heads, sub, hd), bf16),
            pltpu.VMEM((n, heads, 8, LANES), f32),
            pltpu.VMEM((heads, n, sub, hd), f32),
            pltpu.VMEM((heads, 8, LANES), f32),
            pltpu.VMEM((heads, n, halo_sub, hd), f32),
            pltpu.VMEM((heads, 8, LANES), f32),
            pltpu.VMEM((heads, 8, LANES), f32),
            pltpu.VMEM((4, heads, n, sub, hd), bf16),
            pltpu.VMEM((4, 1, width), f32),
            pltpu.VMEM((most_bytes // (4 * LANES), LANES), f32),
            dma((10,)), dma, dma((2,)), dma((n + 1,)), dma, dma((n + 1,)), dma((2,)), dma, dma,
            dma((3,)), dma((2,)), dma((2, heads, 2)), dma((2, heads, 2)), dma, dma((3, heads)), dma((3, heads)),
            dma((heads,)), dma, dma,
        ],
        compiler_params=pltpu.CompilerParams(
            collective_id=0, has_side_effects=True, vmem_limit_bytes=60 * 1024 * 1024
        ),
    )(
        hidden, norm_gain.reshape(-1, LANES), query_gain, key_gain,
        w_query, w_key, w_value, w_out, table,
    )
    return mixed, total.T


def solution(mesh):
    split = (mesh.shape["grp"], mesh.shape["sp"], mesh.shape["tp"]) == (2, MIDDLE_DILATION, 4)
    chosen = local_by_class if split else local
    placed = (
        P(("grp", "sp"), "tp"),
        P(),
        P(None, "tp"),
        P(None, "tp"),
        P(None, "tp"),
        P("tp", None),
        P("tp", None),
        P("tp", None),
    )
    return jax.shard_map(
        chosen,
        mesh=mesh,
        in_specs=placed,
        out_specs=(P(("grp", "sp"), "tp"), P(("grp", "sp"), "tp")),
        check_vma=False,
    )
```

```python
import functools
import math

import jax
import jax.numpy as jnp
import numpy as np
from jax import lax
from jax.experimental import pallas as pl
from jax.experimental.pallas import tpu as pltpu
from jax.sharding import PartitionSpec as P

D = 2048
KEYS_BEHIND = 128
MIDDLE_DILATION = 4
WIDEST_DILATION = 16


EPSILON = 1e-06
ROTARY_BASE = 500000.0


def from_behind(value, axis, steps):
    count = lax.axis_size(axis)
    initial, last = (max(0, -steps), min(count, count - steps))
    return lax.ppermute(value, axis, [(source, source + steps) for source in range(initial, last)])


def rotate(values, positions):
    head_width = values.shape[-1]
    inverse = ROTARY_BASE ** (-jnp.arange(0, head_width, 2, dtype=jnp.float32) / head_width)
    angles = positions[:, None] * inverse[None, :]
    cosine = jnp.cos(angles)[:, None, :]
    sine = jnp.sin(angles)[:, None, :]
    half_width = head_width // 2
    first_half = values[..., :half_width]
    second_half = values[..., half_width:]
    return jnp.concatenate(
        [first_half * cosine - second_half * sine, second_half * cosine + first_half * sine],
        axis=-1,
    )


def head_norm(values, gains):
    normed = values * lax.rsqrt(jnp.mean(values * values, axis=-1, keepdims=True) + EPSILON)
    return normed * gains[None, :, :]


def earlier_pairs(own_pair, token_rows):
    distant_shards = (KEYS_BEHIND * WIDEST_DILATION + token_rows - 1) // token_rows
    pieces = [own_pair]
    for distance in range(1, distant_shards + 1):
        pieces.insert(0, from_behind(own_pair, "sp", distance))
    buffer = jnp.concatenate(pieces, axis=1)
    return buffer


def local_branch(query, key_rows, value_rows, dilation_step, first_pos):
    token_rows, head_count, head_width = query.shape
    reach_rows = KEYS_BEHIND * dilation_step
    buffer_rows = key_rows.shape[0]
    class_rows = token_rows // dilation_step
    class_keys = class_rows + KEYS_BEHIND
    window_start = buffer_rows - token_rows - reach_rows
    key_window = key_rows[window_start:]
    value_window = value_rows[window_start:]
    query_class = query.reshape(class_rows, dilation_step, head_count, head_width).transpose(
        1, 0, 2, 3
    )
    key_class = key_window.reshape(class_keys, dilation_step, head_count, head_width).transpose(
        1, 0, 2, 3
    )
    value_class = value_window.reshape(class_keys, dilation_step, head_count, head_width).transpose(
        1, 0, 2, 3
    )
    block_rows = math.gcd(class_rows, KEYS_BEHIND) if class_rows > KEYS_BEHIND else class_rows
    block_count = class_rows // block_rows
    query_blocks = query_class.reshape(
        dilation_step, block_count, block_rows, head_count, head_width
    )
    key_blocks = jnp.stack(
        [
            key_class[:, number * block_rows : number * block_rows + block_rows + KEYS_BEHIND]
            for number in range(block_count)
        ],
        axis=1,
    )
    value_blocks = jnp.stack(
        [
            value_class[:, number * block_rows : number * block_rows + block_rows + KEYS_BEHIND]
            for number in range(block_count)
        ],
        axis=1,
    )
    scores = jnp.einsum(
        "rnqhd,rnkhd->rnhqk", query_blocks, key_blocks, preferred_element_type=jnp.float32
    ) * head_width ** (-0.5)
    row_index = jnp.arange(block_rows, dtype=jnp.int32)[:, None]
    col_index = jnp.arange(block_rows + KEYS_BEHIND, dtype=jnp.int32)[None, :]
    distance = KEYS_BEHIND + row_index - col_index
    in_band = (distance >= 0) & (distance <= KEYS_BEHIND)
    class_index = jnp.arange(block_count, dtype=jnp.int32)[:, None] * block_rows + col_index
    residue = jnp.arange(dilation_step, dtype=jnp.int32)[:, None, None]
    key_position = first_pos - reach_rows + class_index[None] * dilation_step + residue
    allowed = in_band[None, None, None, :, :] & (key_position >= 0)[:, :, None, None, :]
    scores = jnp.where(allowed, scores, -jnp.inf)
    row_max = jnp.max(scores, axis=-1, keepdims=True)
    weights = jnp.exp(scores - row_max)
    weight_sum = jnp.sum(weights, axis=-1)
    weighted = jnp.einsum(
        "rnhqk,rnkhd->rnqhd",
        weights.astype(jnp.bfloat16),
        value_blocks,
        preferred_element_type=jnp.float32,
    )
    branch_out = weighted / jnp.transpose(weight_sum, (0, 1, 3, 2))[..., None]
    branch_out = branch_out.reshape(dilation_step, class_rows, head_count, head_width).transpose(
        1, 0, 2, 3
    )
    branch_out = branch_out.reshape(token_rows, head_count, head_width)
    log_sum = jnp.transpose(row_max[..., 0] + jnp.log(weight_sum), (0, 1, 3, 2))
    log_sum = (
        log_sum.reshape(dilation_step, class_rows, head_count)
        .transpose(1, 0, 2)
        .reshape(token_rows, head_count)
    )
    return (branch_out, log_sum)


def local(hidden, norm_gain, w_query, w_key, w_value, query_gain, key_gain, w_out):
    token_rows = hidden.shape[0]
    local_width = w_query.shape[1]
    head_count = query_gain.shape[0]
    head_width = query_gain.shape[1]
    gain_full = norm_gain.astype(jnp.float32)
    raw_piece = lax.all_gather(hidden, "tp", axis=1, tiled=True).astype(jnp.float32)
    scaled = (raw_piece * gain_full[None, :]).astype(jnp.bfloat16)

    def add_product(weight):
        return jnp.dot(scaled, weight, preferred_element_type=jnp.float32)

    query_raw = add_product(w_query)
    key_raw = add_product(w_key)
    value_raw = add_product(w_value)
    squares = jnp.sum(raw_piece * raw_piece, axis=1)
    row_scale = lax.rsqrt(squares / D + EPSILON)[:, None]
    first_pos = lax.axis_index("sp") * token_rows
    positions = (jnp.arange(token_rows, dtype=jnp.int32) + first_pos).astype(jnp.float32)
    query = rotate(
        head_norm((query_raw * row_scale).reshape(token_rows, head_count, head_width), query_gain),
        positions,
    ).astype(jnp.bfloat16)
    key_now = rotate(
        head_norm((key_raw * row_scale).reshape(token_rows, head_count, head_width), key_gain),
        positions,
    ).astype(jnp.bfloat16)
    value_now = (value_raw * row_scale).astype(jnp.bfloat16)
    own_pair = jnp.stack([key_now.reshape(token_rows, local_width), value_now], axis=0)
    buffer = earlier_pairs(own_pair, token_rows)
    key_rows = buffer[0].reshape(-1, head_count, head_width)
    value_rows = buffer[1].reshape(-1, head_count, head_width)
    branch_outs = []
    branch_logs = []
    for dilation_step in (1, MIDDLE_DILATION, WIDEST_DILATION):
        branch_out, log_sum = local_branch(query, key_rows, value_rows, dilation_step, first_pos)
        branch_outs.append(branch_out)
        branch_logs.append(log_sum)
    stacked_logs = jnp.stack(branch_logs, axis=0)
    peak = jnp.max(stacked_logs, axis=0)
    log_total = peak + jnp.log(jnp.sum(jnp.exp(stacked_logs - peak[None]), axis=0))
    shares = jnp.exp(stacked_logs - log_total[None])
    attended = jnp.sum(shares[..., None] * jnp.stack(branch_outs, axis=0), axis=0)
    attended = attended.astype(jnp.bfloat16).reshape(token_rows, local_width)
    column_block = lax.all_to_all(w_out, "tp", split_axis=1, concat_axis=0, tiled=True)
    mixed = jnp.dot(
        lax.all_gather(attended, "tp", axis=1, tiled=True),
        column_block,
        preferred_element_type=jnp.float32,
    )
    return (mixed.astype(jnp.bfloat16), log_total)


MESH = pl.DeviceIdType.MESH
LANES = 128


def rotary_table(classes, rows, head_width):
    inverse = (ROTARY_BASE ** (-np.arange(0, head_width, 2, dtype=np.float64) / head_width)).astype(np.float32)
    positions = np.arange(classes * classes * rows, dtype=np.float32)
    angles = (positions[:, None] * inverse[None, :]).astype(np.float64)
    cosine, sine = np.cos(angles), np.sin(angles)
    table = np.concatenate([cosine, cosine, -sine, sine], axis=1).astype(np.float32)
    return table.reshape(classes, rows, classes, 2 * head_width).transpose(0, 2, 1, 3)


def class_kernel(
    hid_ref, gain_ref, qgain_ref, kgain_ref, wq_ref, wk_ref, wv_ref, wo_ref, table_ref,
    mixed_ref, total_ref,
    hid, gain_in, qgain, kgain, hb, hm, wall, wo, tb, tm, acc, acc_m, sq, q_b, kv_b, q_c, kv_c,
    halo, oc, lsend, ro, rl, near_out, near_row, halo_out, halo_row, all_log, at, at_own, bias_far, bias_near, gain, drain,
    loc, sent, zr, axr, acr, afr, cxr, ccr, cfr, wor, wfr, qr, kr, hr, rr, lr, gxr, gcr, gfr, gor, gpr,
):
    f32, bf16 = jnp.float32, jnp.bfloat16
    g, s, p = lax.axis_index("grp"), lax.axis_index("sp"), lax.axis_index("tp")
    n = MIDDLE_DILATION
    rows, width = hid_ref.shape
    sub = rows // n
    heads, hd = qgain_ref.shape
    lw = heads * hd
    halo_sub = halo.shape[2]
    halo_rows = n * halo_sub
    core = p + 1 - 2 * lax.rem(p, 2)
    xp = lax.rem(p + 2, 4)
    diag = lax.rem(core + 2, 4)
    pair, two, mirror = s + 1 - 2 * lax.rem(s, 2), lax.rem(s + 2, n), n - 1 - s
    peer = (s, pair, two, mirror)
    part = sub // 2
    pieces = (
        (two, 0, part), (two, part, part), (pair, 0, sub), (s, 0, sub), (mirror, sub - halo_sub, halo_sub), (mirror, 0, sub - halo_sub)
    )

    def copy_to(axis, src, dst, ss, sr, q):
        return pltpu.make_async_remote_copy(
            src_ref=src, dst_ref=dst, send_sem=ss, recv_sem=sr, device_id={axis: q}, device_id_type=MESH
        )

    tp_copy = functools.partial(copy_to, "tp")
    sp_copy = functools.partial(copy_to, "sp")

    def same(copy, ref, sr, q):
        return copy(ref, ref, sent, sr, q)

    load_hid = pltpu.make_async_copy(hid_ref, hid, loc.at[1])
    load_hid.start()
    barrier = pltpu.get_barrier_semaphore()
    for k in (3, 2, 1):
        pl.semaphore_signal(barrier, inc=1, device_id={"sp": peer[k]}, device_id_type=MESH)
    for q in (xp, diag, core):
        pl.semaphore_signal(barrier, inc=1, device_id={"tp": q}, device_id_type=MESH)
    pl.semaphore_signal(barrier, inc=1, device_id={"grp": 1 - g}, device_id_type=MESH)
    loads = [
        pltpu.make_async_copy(gain_ref, gain_in, loc.at[0]),
        pltpu.make_async_copy(qgain_ref, qgain, loc.at[2]),
        pltpu.make_async_copy(kgain_ref, kgain, loc.at[3]),
        pltpu.make_async_copy(wq_ref, wall.at[:, pl.ds(0, lw)], loc.at[4]),
        pltpu.make_async_copy(wk_ref, wall.at[:, pl.ds(lw, lw)], loc.at[5]),
        pltpu.make_async_copy(wv_ref, wall.at[:, pl.ds(2 * lw, lw)], loc.at[6]),
        pltpu.make_async_copy(table_ref.at[s], tb, loc.at[7]),
        pltpu.make_async_copy(table_ref.at[mirror, s], tm, loc.at[8]),
        pltpu.make_async_copy(
            wo_ref.at[:, pl.ds(pl.multiple_of(p * width, LANES), width)], wo.at[p], loc.at[9]
        ),
    ]
    for load in loads:
        load.start()

    def iota(shape, dim):
        return lax.broadcasted_iota(jnp.int32, shape, dim)

    def row_of(r, part):
        return n * lax.rem(r, part) + r // part

    square = (rows, rows)
    to_class = (row_of(iota(square, 0), sub) == iota(square, 1)).astype(f32).astype(bf16)
    load_hid.wait()
    permuted = jnp.dot(to_class, hid[...], preferred_element_type=f32).astype(bf16)
    hb[p] = permuted.reshape(n, sub, width)
    pl.semaphore_wait(barrier, 3 + n)

    sends = []

    def go(copy):
        copy.start()
        sends.append(math.prod(copy.src_ref.shape) * copy.src_ref.dtype.itemsize)
        return copy

    zs = [
        go(sp_copy(hb.at[p, mirror, pl.ds(a * part, part), :], hm.at[p, a], sent, zr.at[a], mirror))
        for a in range(2)
    ]
    ax = [same(tp_copy, hb.at[p, c, pl.ds(i, m), :], axr.at[j], xp) for j, (c, i, m) in enumerate(pieces)]
    for copy in ax[:4]:
        go(copy)
    ac = go(same(tp_copy, hb.at[p], acr, core))
    w_sends = [
        go(tp_copy(wo_ref.at[:, pl.ds(pl.multiple_of(core * width, LANES), width)], wo.at[p], sent, wor.at[0], core))
    ]

    for load in loads:
        load.wait()
    flat_gain = gain_in[...].astype(f32)
    for j in range(flat_gain.shape[0]):
        each = width // LANES
        gain[j // each, :, (j % each) * LANES : (j % each + 1) * LANES] = flat_gain[j : j + 1]

    def chunk(raw, q):
        raw = raw.astype(f32)
        scaled = (raw * gain[q]).astype(bf16)
        w = wall[pl.ds(pl.multiple_of(q * width, LANES), width), :]
        return jnp.dot(scaled, w, preferred_element_type=f32), jnp.sum(raw * raw, axis=1, keepdims=True)

    def add_all(q, first):
        prod, more = chunk(hb[q].reshape(rows, width), q)
        prod, more = prod.reshape(n, sub, 3 * lw), more.reshape(n, sub, 1)
        acc[...] = prod if first else acc[...] + prod
        sq[...] = more if first else sq[...] + more

    add_all(p, True)
    ac.wait_recv()
    add_all(core, False)

    def finish(acc, sq, table, places, span):
        raw = acc * lax.rsqrt(sq / (width * 4) + EPSILON)
        cosine, sine = table[:, :hd], table[:, hd:]
        for h in range(heads):
            for j, gains in enumerate((qgain, kgain, None)):
                x = raw[:, j * lw + h * hd : j * lw + (h + 1) * hd]
                if gains is not None:
                    x = x * lax.rsqrt(jnp.mean(x * x, axis=-1, keepdims=True) + EPSILON)
                    x = x * gains[pl.ds(h, 1), :]
                    x = x * cosine + pltpu.roll(x, hd // 2, 1) * sine
                for q_ref, kv_ref, c in places:
                    if j == 0:
                        q_ref[c, h, span] = x.astype(bf16)
                    else:
                        kv_ref[c, h, span, (j - 1) * hd : j * hd] = x.astype(bf16)

    def take(j):
        c, i, m = pieces[j]
        ax[j].wait_recv()
        go(same(tp_copy, hb.at[xp, c, pl.ds(i, m), :], afr.at[j], core))

    def close(j, places, between):
        c, i, m = pieces[j]
        span = slice(i, i + m)
        prod, more = chunk(hb[xp, c, span], xp)
        between()
        same(tp_copy, hb.at[diag, c, pl.ds(i, m), :], afr.at[j], core).wait_recv()
        last, most = chunk(hb[diag, c, span], diag)
        finish(acc[c, span] + prod + last, sq[c, span] + more + most, tb[c, span], places, span)

    cx, cc = {}, {}

    def spread(a):
        zs[a].wait_recv()
        cx[a] = go(same(tp_copy, hm.at[p, a], cxr.at[a], xp))
        cc[a] = go(same(tp_copy, hm.at[p, a], ccr, core))

    def cross(a):
        cx[a].wait_recv()
        go(same(tp_copy, hm.at[xp, a], cfr, core))

    parts_of = {1: pieces[2:3], 2: pieces[:2]}

    def class_copy(own, other, sems, k, h, j, arriving):
        _, i, m = parts_of[k][j]
        q = peer[k]
        mine = other.at[q, h, pl.ds(i, m), :]
        if arriving:
            return same(sp_copy, mine, sems.at[k - 1, h, j], q)
        return sp_copy(own.at[q, h, pl.ds(i, m), :], other.at[s, h, pl.ds(i, m), :], sent, sems.at[k - 1, h, j], q)

    kv_copy = functools.partial(class_copy, kv_b, kv_c, kr)
    q_copy = functools.partial(class_copy, q_b, q_c, qr)

    def give(k, j):
        for h in range(heads):
            @pl.when(s < n - 1)
            def _():
                kv_copy(k, h, j, False).start()

            @pl.when(s > 0)
            def _():
                q_copy(k, h, j, False).start()

    def receive(k, h):
        @pl.when(peer[k] < n - 1)
        def _():
            for j in range(len(parts_of[k])):
                kv_copy(k, h, j, True).wait_recv()

        @pl.when(peer[k] > 0)
        def _():
            for j in range(len(parts_of[k])):
                q_copy(k, h, j, True).wait_recv()

    quarter = lw // 4

    def quarter_of(a):
        return pl.ds(pl.multiple_of((2 * g + a) * quarter, 8), quarter)

    def spread_first():
        spread(0)
        go(ax[4])

    def spread_last():
        spread(1)
        go(ax[5])
        for j, q in ((0, xp), (1, diag)):
            for a in range(2):
                block = quarter_of(a)
                w_sends.append(go(tp_copy(
                    wo_ref.at[block, pl.ds(pl.multiple_of(q * width, LANES), width)], wo.at[p, block],
                    sent, wor.at[1 + 2 * j + a], q,
                )))

    def add_mirror(q):
        prod, more = chunk(hm[q].reshape(sub, width), q)
        return prod, more

    squares = []

    def start_mirror():
        same(tp_copy, hm.at[core], ccr, core).wait_recv()
        first, one = add_mirror(p)
        prod, more = add_mirror(core)
        acc_m[...] = first + prod
        squares.append(one + more)
        cross(0)

    def log_count(*read):
        count = sum(each.astype(f32) for each in read)
        bias = jnp.where(count == 2, math.log(2.0), jnp.where(count == 3, math.log(3.0), 0.0))
        return jnp.where(count == 0, -jnp.inf, bias)

    def strided(behind, step):
        return (behind >= 0) & (behind <= KEYS_BEHIND * step) & ((behind + rows * step) % step == 0)

    later = (rows - sub, rows - sub)
    late, early = iota(later, 0) + sub, iota(later, 1)
    stride = WIDEST_DILATION // n
    crosses = late // sub > early // sub
    bias_far[...] = log_count(strided(late - early, 1) & crosses, strided(late - early, stride) & crosses)
    behind = row_of(iota(square, 0), sub) - row_of(iota(square, 1), sub)
    bias_near[...] = log_count(*(strided(behind, step) for step in (1, n, WIDEST_DILATION)))
    take(0)
    close(0, ((q_b, kv_b, two),), lambda: None)
    give(2, 0)
    take(1)
    close(1, ((q_b, kv_b, two),), spread_first)
    give(2, 1)
    take(2)
    close(2, ((q_b, kv_b, pair),), spread_last)
    give(1, 0)
    take(3)
    close(3, ((q_b, kv_b, s), (q_c, kv_c, s)), start_mirror)

    above = lax.rem(s + 1, n)

    def send_halo(c):
        sp_copy(kv_b.at[c, :, pl.ds(sub - halo_sub, halo_sub), :], halo.at[c], sent, hr, above).start()

    take(4)

    @pl.when(s < n - 1)
    def _():
        send_halo(two)
        send_halo(s)

    @pl.when(s == 1)
    def _():
        send_halo(pair)

    close(4, ((q_b, kv_b, mirror),), lambda: None)

    @pl.when((s < n - 1) & (s != 1))
    def _():
        send_halo(mirror)

    cross(1)
    prod, more = add_mirror(xp)
    take(5)
    same(tp_copy, hm.at[diag], cfr, core).wait_recv()
    last, most = add_mirror(diag)
    finish(acc_m[...] + prod + last, squares[0] + more + most, tm[...], ((q_c, kv_c, mirror),), slice(0, sub))

    def attend(q, k, v, bias):
        score = lax.dot_general(q, k, (((1,), (1,)), ((), ())), preferred_element_type=f32)
        score = score * hd ** (-0.5) + bias
        top = jnp.max(score, axis=-1, keepdims=True)
        weight = jnp.exp(score - top)
        total = jnp.sum(weight, axis=-1, keepdims=True)
        out = jnp.dot(weight.astype(bf16), v, preferred_element_type=f32) / total
        return out, top + jnp.log(total)

    lane = iota((rows, LANES), 1)

    def as_rows(columns):
        spread_out = jnp.full((sub, LANES), -jnp.inf, f32)
        for c, column in enumerate(columns):
            if column is not None:
                spread_out = jnp.where(lane[:sub] == c, column, spread_out)
        pad = jnp.zeros((LANES - sub, LANES), f32)
        return jnp.transpose(jnp.concatenate([spread_out, pad], axis=0))[:8]

    def flat(x):
        return x.reshape(x.shape[0] * x.shape[1], x.shape[2])

    def far_head(h):
        receive(2, h)
        receive(1, h)
        out, lse = attend(
            flat(q_c[1:, h]), flat(kv_c[: n - 1, h, :, :hd]), flat(kv_c[: n - 1, h, :, hd:]), bias_far[...]
        )
        lsend[h] = as_rows([None] + [lse[b * sub : (b + 1) * sub] for b in range(n - 1)])
        rl[s, h] = lsend[h]
        oc[h, 1:] = out.astype(bf16).reshape(n - 1, sub, hd)
        for k in (3, 2, 1):
            @pl.when(peer[k] > 0)
            def _():
                sp_copy(lsend.at[h], rl.at[s, h], sent, lr.at[k - 1, h], peer[k]).start()
                sp_copy(oc.at[h, peer[k]], ro.at[s, h], sent, rr.at[k - 1, h], peer[k]).start()

    wf = []

    def pass_on(j):
        piece = wo.at[(xp, diag)[j // 2], quarter_of(j % 2)]
        w_sends[j + 1].wait_recv()
        wf.append(go(copy_to("grp", piece, piece, sent, wfr.at[j], 1 - g)))

    far_head(0)
    for h in range(1, heads):
        far_head(h)
    pass_on(0)
    close(5, ((q_b, kv_b, mirror),), lambda: None)
    pass_on(1)

    others = pl.ds(0, n - 1)
    gx = [same(tp_copy, at.at[p, h, others], gxr.at[h], xp) for h in range(heads)]
    gc = [same(tp_copy, at.at[p, h, others], gcr, core) for h in range(heads)]
    gx.append(same(tp_copy, at_own.at[p], gxr.at[heads], xp))
    gc.append(same(tp_copy, at_own.at[p], gor, core))

    def share(j):
        gx[j].start()
        gc[j].start()

    def slot(c):
        return lax.rem(lax.rem(c + s, 2) + 2 * lax.rem(c // 2 + s // 2, 2) + n - 1, n)

    for h in range(heads):
        out, lse = attend(flat(q_b[:, h]), flat(kv_b[:, h, :, :hd]), flat(kv_b[:, h, :, hd:]), bias_near[...])
        near_out[h] = out.reshape(n, sub, hd)
        near_row[h] = as_rows([lse[c * sub : (c + 1) * sub] for c in range(n)])

        @pl.when(s == 0)
        def _():
            at_own[p, h] = near_out[h, 0].astype(bf16)
            for c in range(1, n):
                at[p, h, c - 1] = near_out[h, c].astype(bf16)
            if h == heads - 1:
                share(heads)
            share(h)
            all_log[h] = near_row[h]

        pass_on(2 + h)

    @pl.when(s > 0)
    def _():
        sp_copy(halo.at[pl.ds(0, n - 1)], halo.at[pl.ds(0, n - 1)], sent, hr, above).wait_recv()
        halo[s] = kv_c[s - 1, :, sub - halo_sub :, :]
        small = (halo_rows, halo_rows)
        behind = row_of(iota(small, 0), halo_sub) - row_of(iota(small, 1), halo_sub) + halo_rows
        bias_h = jnp.where(behind <= KEYS_BEHIND, 0.0, -jnp.inf).astype(f32)
        for h in range(heads):
            out, lse = attend(
                flat(q_b[:, h, :halo_sub]), flat(halo[:, h, :, :hd]), flat(halo[:, h, :, hd:]), bias_h
            )
            halo_out[h] = out.reshape(n, halo_sub, hd)
            pad = jnp.full((sub - halo_sub, 1), -jnp.inf, f32)
            halo_row[h] = as_rows([
                jnp.concatenate([lse[c * halo_sub : (c + 1) * halo_sub], pad], axis=0) for c in range(n)
            ])

    which = iota((8, LANES), 0)

    def weigh(own, low, far_row):
        top = jnp.maximum(jnp.maximum(own, low), far_row)
        exps = [jnp.exp(x - top) for x in (own, low, far_row)]
        both = exps[0] + exps[1] + exps[2]
        return [x / both for x in exps], top + jnp.log(both)

    def as_columns(shares):
        pad = jnp.zeros((LANES - 8 * len(shares), LANES), f32)
        return jnp.transpose(jnp.concatenate(shares + [pad], axis=0))[:sub]

    def blend(parts, own, far_out, low):
        sums = parts[0] * own + parts[2] * far_out.astype(f32)
        return jnp.concatenate([sums[:halo_sub] + parts[1][:halo_sub] * low, sums[halo_sub:]], axis=0).astype(bf16)

    @pl.when(s > 0)
    def _():
        mine = pl.ds(s, 1)
        rows_of = jnp.zeros((8, LANES), f32)
        for h in range(heads):
            shares, _ = weigh(near_row[h, mine], halo_row[h, mine], rl[s, h, mine])
            for j, x in enumerate(shares):
                rows_of = jnp.where(which == 3 * h + j, x, rows_of)
        columns = as_columns([rows_of])
        for h in range(heads):
            parts = [columns[:, 3 * h + j : 3 * h + j + 1] for j in range(3)]
            at_own[p, h] = blend(parts, near_out[h, s], oc[h, s], halo_out[h, s])
        share(heads)
        for h in range(heads):
            ro[s, h] = oc[h, s]
            for k in (1, 2, 3):
                same(sp_copy, rl.at[peer[k], h], lr.at[k - 1, h], peer[k]).wait_recv()
                same(sp_copy, ro.at[peer[k], h], rr.at[k - 1, h], peer[k]).wait_recv()
            far_row = jnp.zeros((8, LANES), f32)
            for c in range(n):
                far_row = jnp.where(which == c, rl[c, h, mine], far_row)
            live = which < n
            shares, all_log[h] = weigh(*(jnp.where(live, x, 0.0) for x in (near_row[h], halo_row[h], far_row)))
            columns = as_columns(shares)
            for c in range(n):
                parts = [columns[:, 8 * j + c : 8 * j + c + 1] for j in range(3)]
                at[p, h, slot(c)] = blend(parts, near_out[h, c], ro[c, h], halo_out[h, c])
            share(h)

    block = iota(square, 1) // sub
    class_of = jnp.where(block == 0, pair, jnp.where(block == 1, two, jnp.where(block == 2, mirror, s)))
    from_class = (iota(square, 0) == n * lax.rem(iota(square, 1), sub) + class_of).astype(f32).astype(bf16)

    def product(q):
        x = jnp.concatenate([
            jnp.concatenate([flat(at[q, h, : n - 1]), at_own[q, h]], axis=0) for h in range(heads)
        ], axis=1)
        return jnp.dot(x, wo[q], preferred_element_type=f32)

    def forward(j):
        gx[j].wait_recv()
        if j == heads:
            go(same(tp_copy, at_own.at[xp], gpr, core))
        else:
            go(same(tp_copy, at.at[xp, j, others], gfr, core))

    by_head = iota((8, LANES), 0)
    logs = []
    for c in range(n):
        row = jnp.zeros((8, LANES), f32)
        for h in range(heads):
            row = jnp.where(by_head == h, all_log[h, c : c + 1, :], row)
        logs.append(row)
    logs = jnp.concatenate(logs, axis=1)
    placed = (n * LANES, rows)
    to_order = (
        (n * lax.rem(iota(placed, 0), LANES) + iota(placed, 0) // LANES == iota(placed, 1))
        & (lax.rem(iota(placed, 0), LANES) < sub)
    ).astype(f32).astype(bf16)
    high = logs.astype(bf16)
    rest = logs - high.astype(f32)
    middle = rest.astype(bf16)
    low = (rest - middle.astype(f32)).astype(bf16)
    total = sum(jnp.dot(x, to_order, preferred_element_type=f32) for x in (high, middle, low))
    total_ref[...] = total[:heads]

    result = product(p)
    forward(heads)
    w_sends[0].wait_recv()
    same(tp_copy, at_own.at[core], gor, core).wait_recv()
    same(tp_copy, at.at[core, :, others], gcr, core).wait_recv()
    result += product(core)
    for h in range(heads):
        forward(h)
    for copy in wf:
        copy.wait_recv()
    result += product(xp)
    same(tp_copy, at_own.at[diag], gpr, core).wait_recv()
    same(tp_copy, at.at[diag, :, others], gfr, core).wait_recv()
    result += product(diag)
    mixed_ref[...] = jnp.dot(from_class, result.astype(bf16), preferred_element_type=f32).astype(bf16)
    back = heads * (sub * hd * 2 + 8 * LANES * 4)
    q_bytes, kv_bytes = 2 * heads * sub * hd * 2, 2 * heads * sub * 2 * hd * 2
    halo_bytes = (n - 1) * heads * halo_sub * 2 * hd * 2
    at_bytes = 2 * rows * lw * 2

    def all_sent(total):
        same(tp_copy, drain.at[pl.ds(0, total // (LANES * 4))], acr, core).wait_send()

    @pl.when(s == 0)
    def _():
        all_sent(sum(sends) + at_bytes + kv_bytes + halo_bytes + 3 * back)

    @pl.when((s > 0) & (s < n - 1))
    def _():
        all_sent(sum(sends) + at_bytes + q_bytes + kv_bytes + halo_bytes + 2 * back)

    @pl.when(s == n - 1)
    def _():
        all_sent(sum(sends) + at_bytes + q_bytes + 2 * back)


def write_kernel(mixed_ref, total_ref, out_ref, log_ref, sems):
    copies = [
        pltpu.make_async_copy(mixed_ref, out_ref, sems.at[0]),
        pltpu.make_async_copy(total_ref, log_ref, sems.at[1]),
    ]
    for copy in copies:
        copy.start()
    for copy in copies:
        copy.wait()


def local_by_class(hidden, norm_gain, w_query, w_key, w_value, query_gain, key_gain, w_out):
    n = MIDDLE_DILATION
    rows, width = hidden.shape
    heads, hd = query_gain.shape
    lw = heads * hd
    sub = rows // n
    halo_sub = KEYS_BEHIND // n
    bf16, f32 = jnp.bfloat16, jnp.float32
    table = jnp.asarray(rotary_table(n, sub, hd))
    most_bytes = 2 * (16 * sub * width + 3 * lw * width + 30 * sub * lw) + 3 * heads * 8 * LANES * 4
    vmem = pl.BlockSpec(memory_space=pltpu.VMEM)
    anyspace = pl.BlockSpec(memory_space=pl.ANY)
    dma = pltpu.SemaphoreType.DMA
    mixed, total = pl.pallas_call(
        class_kernel,
        out_shape=(
            pltpu.VMEM((rows, w_out.shape[1] // 4), bf16),
            pltpu.VMEM((heads, rows), f32),
        ),
        in_specs=[anyspace] * 9,
        out_specs=(vmem, vmem),
        scratch_shapes=[
            pltpu.VMEM((rows, width), bf16),
            pltpu.VMEM((4 * width // LANES, LANES), bf16),
            pltpu.VMEM((heads, hd), f32),
            pltpu.VMEM((heads, hd), f32),
            pltpu.VMEM((4, n, sub, width), bf16),
            pltpu.VMEM((4, 2, sub // 2, width), bf16),
            pltpu.VMEM((4 * width, 3 * lw), bf16),
            pltpu.VMEM((4, lw, width), bf16),
            pltpu.VMEM((n, sub, 2 * hd), f32),
            pltpu.VMEM((sub, 2 * hd), f32),
            pltpu.VMEM((n, sub, 3 * lw), f32),
            pltpu.VMEM((sub, 3 * lw), f32),
            pltpu.VMEM((n, sub, 1), f32),
            pltpu.VMEM((n, heads, sub, hd), bf16),
            pltpu.VMEM((n, heads, sub, 2 * hd), bf16),
            pltpu.VMEM((n, heads, sub, hd), bf16),
            pltpu.VMEM((n, heads, sub, 2 * hd), bf16),
            pltpu.VMEM((n, heads, halo_sub, 2 * hd), bf16),
            pltpu.VMEM((heads, n, sub, hd), bf16),
            pltpu.VMEM((heads, 8, LANES), f32),
            pltpu.VMEM((n, heads, sub, hd), bf16),
            pltpu.VMEM((n, heads, 8, LANES), f32),
            pltpu.VMEM((heads, n, sub, hd), f32),
            pltpu.VMEM((heads, 8, LANES), f32),
            pltpu.VMEM((heads, n, halo_sub, hd), f32),
            pltpu.VMEM((heads, 8, LANES), f32),
            pltpu.VMEM((heads, 8, LANES), f32),
            pltpu.VMEM((4, heads, n, sub, hd), bf16),
            pltpu.VMEM((4, heads, sub, hd), bf16),
            pltpu.VMEM((rows - sub, rows - sub), f32),
            pltpu.VMEM((rows, rows), f32),
            pltpu.VMEM((4, 1, width), f32),
            pltpu.VMEM((most_bytes // (4 * LANES), LANES), f32),
            dma((10,)), dma, dma((2,)), dma((n + 2,)), dma, dma((n + 2,)), dma((2,)), dma, dma,
            dma((5,)), dma((4,)), dma((2, heads, 2)), dma((2, heads, 2)), dma, dma((3, heads)), dma((3, heads)),
            dma((heads + 1,)), dma, dma, dma, dma,
        ],
        compiler_params=pltpu.CompilerParams(
            collective_id=0, has_side_effects=True, vmem_limit_bytes=60 * 1024 * 1024
        ),
    )(
        hidden, norm_gain.reshape(-1, LANES), query_gain, key_gain,
        w_query, w_key, w_value, w_out, table,
    )
    mixed, total = pl.pallas_call(
        write_kernel,
        out_shape=(
            jax.ShapeDtypeStruct(mixed.shape, bf16), jax.ShapeDtypeStruct(total.shape, f32)
        ),
        in_specs=[vmem, vmem],
        out_specs=(anyspace, anyspace),
        scratch_shapes=[dma((2,))],
    )(
        pltpu.with_memory_space_constraint(mixed, pltpu.VMEM),
        pltpu.with_memory_space_constraint(total, pltpu.VMEM),
    )
    return mixed, total.T


def solution(mesh):
    split = (mesh.shape["grp"], mesh.shape["sp"], mesh.shape["tp"]) == (2, MIDDLE_DILATION, 4)
    chosen = local_by_class if split else local
    placed = (
        P(("grp", "sp"), "tp"),
        P(),
        P(None, "tp"),
        P(None, "tp"),
        P(None, "tp"),
        P("tp", None),
        P("tp", None),
        P("tp", None),
    )
    return jax.shard_map(
        chosen,
        mesh=mesh,
        in_specs=placed,
        out_specs=(P(("grp", "sp"), "tp"), P(("grp", "sp"), "tp")),
        check_vma=False,
    )
```

```python
import functools
import math

import jax
import jax.numpy as jnp
import numpy as np
from jax import lax
from jax.experimental import pallas as pl
from jax.experimental.pallas import tpu as pltpu
from jax.sharding import PartitionSpec as P

D = 2048
KEYS_BEHIND = 128
MIDDLE_DILATION = 4
WIDEST_DILATION = 16


EPSILON = 1e-06
ROTARY_BASE = 500000.0


def from_behind(value, axis, steps):
    count = lax.axis_size(axis)
    initial, last = (max(0, -steps), min(count, count - steps))
    return lax.ppermute(value, axis, [(source, source + steps) for source in range(initial, last)])


def rotate(values, positions):
    head_width = values.shape[-1]
    inverse = ROTARY_BASE ** (-jnp.arange(0, head_width, 2, dtype=jnp.float32) / head_width)
    angles = positions[:, None] * inverse[None, :]
    cosine = jnp.cos(angles)[:, None, :]
    sine = jnp.sin(angles)[:, None, :]
    half_width = head_width // 2
    first_half = values[..., :half_width]
    second_half = values[..., half_width:]
    return jnp.concatenate(
        [first_half * cosine - second_half * sine, second_half * cosine + first_half * sine],
        axis=-1,
    )


def head_norm(values, gains):
    normed = values * lax.rsqrt(jnp.mean(values * values, axis=-1, keepdims=True) + EPSILON)
    return normed * gains[None, :, :]


def earlier_pairs(own_pair, token_rows):
    distant_shards = (KEYS_BEHIND * WIDEST_DILATION + token_rows - 1) // token_rows
    pieces = [own_pair]
    for distance in range(1, distant_shards + 1):
        pieces.insert(0, from_behind(own_pair, "sp", distance))
    buffer = jnp.concatenate(pieces, axis=1)
    return buffer


def local_branch(query, key_rows, value_rows, dilation_step, first_pos):
    token_rows, head_count, head_width = query.shape
    reach_rows = KEYS_BEHIND * dilation_step
    buffer_rows = key_rows.shape[0]
    class_rows = token_rows // dilation_step
    class_keys = class_rows + KEYS_BEHIND
    window_start = buffer_rows - token_rows - reach_rows
    key_window = key_rows[window_start:]
    value_window = value_rows[window_start:]
    query_class = query.reshape(class_rows, dilation_step, head_count, head_width).transpose(
        1, 0, 2, 3
    )
    key_class = key_window.reshape(class_keys, dilation_step, head_count, head_width).transpose(
        1, 0, 2, 3
    )
    value_class = value_window.reshape(class_keys, dilation_step, head_count, head_width).transpose(
        1, 0, 2, 3
    )
    block_rows = math.gcd(class_rows, KEYS_BEHIND) if class_rows > KEYS_BEHIND else class_rows
    block_count = class_rows // block_rows
    query_blocks = query_class.reshape(
        dilation_step, block_count, block_rows, head_count, head_width
    )
    key_blocks = jnp.stack(
        [
            key_class[:, number * block_rows : number * block_rows + block_rows + KEYS_BEHIND]
            for number in range(block_count)
        ],
        axis=1,
    )
    value_blocks = jnp.stack(
        [
            value_class[:, number * block_rows : number * block_rows + block_rows + KEYS_BEHIND]
            for number in range(block_count)
        ],
        axis=1,
    )
    scores = jnp.einsum(
        "rnqhd,rnkhd->rnhqk", query_blocks, key_blocks, preferred_element_type=jnp.float32
    ) * head_width ** (-0.5)
    row_index = jnp.arange(block_rows, dtype=jnp.int32)[:, None]
    col_index = jnp.arange(block_rows + KEYS_BEHIND, dtype=jnp.int32)[None, :]
    distance = KEYS_BEHIND + row_index - col_index
    in_band = (distance >= 0) & (distance <= KEYS_BEHIND)
    class_index = jnp.arange(block_count, dtype=jnp.int32)[:, None] * block_rows + col_index
    residue = jnp.arange(dilation_step, dtype=jnp.int32)[:, None, None]
    key_position = first_pos - reach_rows + class_index[None] * dilation_step + residue
    allowed = in_band[None, None, None, :, :] & (key_position >= 0)[:, :, None, None, :]
    scores = jnp.where(allowed, scores, -jnp.inf)
    row_max = jnp.max(scores, axis=-1, keepdims=True)
    weights = jnp.exp(scores - row_max)
    weight_sum = jnp.sum(weights, axis=-1)
    weighted = jnp.einsum(
        "rnhqk,rnkhd->rnqhd",
        weights.astype(jnp.bfloat16),
        value_blocks,
        preferred_element_type=jnp.float32,
    )
    branch_out = weighted / jnp.transpose(weight_sum, (0, 1, 3, 2))[..., None]
    branch_out = branch_out.reshape(dilation_step, class_rows, head_count, head_width).transpose(
        1, 0, 2, 3
    )
    branch_out = branch_out.reshape(token_rows, head_count, head_width)
    log_sum = jnp.transpose(row_max[..., 0] + jnp.log(weight_sum), (0, 1, 3, 2))
    log_sum = (
        log_sum.reshape(dilation_step, class_rows, head_count)
        .transpose(1, 0, 2)
        .reshape(token_rows, head_count)
    )
    return (branch_out, log_sum)


def local(hidden, norm_gain, w_query, w_key, w_value, query_gain, key_gain, w_out):
    token_rows = hidden.shape[0]
    local_width = w_query.shape[1]
    head_count = query_gain.shape[0]
    head_width = query_gain.shape[1]
    gain_full = norm_gain.astype(jnp.float32)
    raw_piece = lax.all_gather(hidden, "tp", axis=1, tiled=True).astype(jnp.float32)
    scaled = (raw_piece * gain_full[None, :]).astype(jnp.bfloat16)

    def add_product(weight):
        return jnp.dot(scaled, weight, preferred_element_type=jnp.float32)

    query_raw = add_product(w_query)
    key_raw = add_product(w_key)
    value_raw = add_product(w_value)
    squares = jnp.sum(raw_piece * raw_piece, axis=1)
    row_scale = lax.rsqrt(squares / D + EPSILON)[:, None]
    first_pos = lax.axis_index("sp") * token_rows
    positions = (jnp.arange(token_rows, dtype=jnp.int32) + first_pos).astype(jnp.float32)
    query = rotate(
        head_norm((query_raw * row_scale).reshape(token_rows, head_count, head_width), query_gain),
        positions,
    ).astype(jnp.bfloat16)
    key_now = rotate(
        head_norm((key_raw * row_scale).reshape(token_rows, head_count, head_width), key_gain),
        positions,
    ).astype(jnp.bfloat16)
    value_now = (value_raw * row_scale).astype(jnp.bfloat16)
    own_pair = jnp.stack([key_now.reshape(token_rows, local_width), value_now], axis=0)
    buffer = earlier_pairs(own_pair, token_rows)
    key_rows = buffer[0].reshape(-1, head_count, head_width)
    value_rows = buffer[1].reshape(-1, head_count, head_width)
    branch_outs = []
    branch_logs = []
    for dilation_step in (1, MIDDLE_DILATION, WIDEST_DILATION):
        branch_out, log_sum = local_branch(query, key_rows, value_rows, dilation_step, first_pos)
        branch_outs.append(branch_out)
        branch_logs.append(log_sum)
    stacked_logs = jnp.stack(branch_logs, axis=0)
    peak = jnp.max(stacked_logs, axis=0)
    log_total = peak + jnp.log(jnp.sum(jnp.exp(stacked_logs - peak[None]), axis=0))
    shares = jnp.exp(stacked_logs - log_total[None])
    attended = jnp.sum(shares[..., None] * jnp.stack(branch_outs, axis=0), axis=0)
    attended = attended.astype(jnp.bfloat16).reshape(token_rows, local_width)
    column_block = lax.all_to_all(w_out, "tp", split_axis=1, concat_axis=0, tiled=True)
    mixed = jnp.dot(
        lax.all_gather(attended, "tp", axis=1, tiled=True),
        column_block,
        preferred_element_type=jnp.float32,
    )
    return (mixed.astype(jnp.bfloat16), log_total)


MESH = pl.DeviceIdType.MESH
LANES = 128


def rotary_table(classes, rows, head_width):
    inverse = (ROTARY_BASE ** (-np.arange(0, head_width, 2, dtype=np.float64) / head_width)).astype(np.float32)
    positions = np.arange(classes * classes * rows, dtype=np.float32)
    angles = (positions[:, None] * inverse[None, :]).astype(np.float64)
    cosine, sine = np.cos(angles), np.sin(angles)
    table = np.concatenate([cosine, cosine, -sine, sine], axis=1).astype(np.float32)
    return table.reshape(classes, rows, classes, 2 * head_width).transpose(0, 2, 1, 3)


def class_kernel(
    hid_ref, gain_ref, qgain_ref, kgain_ref, wq_ref, wk_ref, wv_ref, wo_ref, table_ref,
    mixed_ref, total_ref,
    hid, gain_in, qgain, kgain, hb, hm, wall, wo, tb, tm, acc, acc_m, sq, q_b, kv_b, q_c, kv_c,
    halo, oc, lsend, ro, rl, near_out, near_row, halo_out, halo_row, all_log, at, at_own, bias_far, bias_near, gain, drain,
    loc, sent, zr, axr, acr, afr, cxr, ccr, cfr, wor, wfr, qr, kr, hr, rr, lr, gxr, gcr, gfr, gor, gpr,
):
    f32, bf16 = jnp.float32, jnp.bfloat16
    g, s, p = lax.axis_index("grp"), lax.axis_index("sp"), lax.axis_index("tp")
    n = MIDDLE_DILATION
    rows, width = hid_ref.shape
    sub = rows // n
    heads, hd = qgain_ref.shape
    lw = heads * hd
    halo_sub = halo.shape[2]
    halo_rows = n * halo_sub
    core = p + 1 - 2 * lax.rem(p, 2)
    xp = lax.rem(p + 2, 4)
    diag = lax.rem(core + 2, 4)
    pair, two, mirror = s + 1 - 2 * lax.rem(s, 2), lax.rem(s + 2, n), n - 1 - s
    peer = (s, pair, two, mirror)
    part = sub // 2
    pieces = (
        (two, 0, part), (two, part, part), (pair, 0, sub), (s, 0, sub), (mirror, sub - halo_sub, halo_sub), (mirror, 0, sub - halo_sub)
    )

    def copy_to(axis, src, dst, ss, sr, q):
        return pltpu.make_async_remote_copy(
            src_ref=src, dst_ref=dst, send_sem=ss, recv_sem=sr, device_id={axis: q}, device_id_type=MESH
        )

    tp_copy = functools.partial(copy_to, "tp")
    sp_copy = functools.partial(copy_to, "sp")

    def same(copy, ref, sr, q):
        return copy(ref, ref, sent, sr, q)

    load_hid = pltpu.make_async_copy(hid_ref, hid, loc.at[1])
    load_hid.start()
    barrier = pltpu.get_barrier_semaphore()
    for k in (3, 2, 1):
        pl.semaphore_signal(barrier, inc=1, device_id={"sp": peer[k]}, device_id_type=MESH)
    for q in (xp, diag, core):
        pl.semaphore_signal(barrier, inc=1, device_id={"tp": q}, device_id_type=MESH)
    pl.semaphore_signal(barrier, inc=1, device_id={"grp": 1 - g}, device_id_type=MESH)
    loads = [
        pltpu.make_async_copy(gain_ref, gain_in, loc.at[0]),
        pltpu.make_async_copy(qgain_ref, qgain, loc.at[2]),
        pltpu.make_async_copy(kgain_ref, kgain, loc.at[3]),
        pltpu.make_async_copy(wq_ref, wall.at[:, pl.ds(0, lw)], loc.at[4]),
        pltpu.make_async_copy(wk_ref, wall.at[:, pl.ds(lw, lw)], loc.at[5]),
        pltpu.make_async_copy(wv_ref, wall.at[:, pl.ds(2 * lw, lw)], loc.at[6]),
        pltpu.make_async_copy(table_ref.at[s], tb, loc.at[7]),
        pltpu.make_async_copy(table_ref.at[mirror, s], tm, loc.at[8]),
        pltpu.make_async_copy(
            wo_ref.at[:, pl.ds(pl.multiple_of(p * width, LANES), width)], wo.at[p], loc.at[9]
        ),
    ]
    for load in loads:
        load.start()

    def iota(shape, dim):
        return lax.broadcasted_iota(jnp.int32, shape, dim)

    def row_of(r, part):
        return n * lax.rem(r, part) + r // part

    square = (rows, rows)
    to_class = (row_of(iota(square, 0), sub) == iota(square, 1)).astype(f32).astype(bf16)
    load_hid.wait()
    permuted = jnp.dot(to_class, hid[...], preferred_element_type=f32).astype(bf16)
    hb[p] = permuted.reshape(n, sub, width)
    pl.semaphore_wait(barrier, 3 + n)

    sends = []

    def go(copy):
        copy.start()
        sends.append(math.prod(copy.src_ref.shape) * copy.src_ref.dtype.itemsize)
        return copy

    zs = [
        go(sp_copy(hb.at[p, mirror, pl.ds(a * part, part), :], hm.at[p, a], sent, zr.at[a], mirror))
        for a in range(2)
    ]
    ax = [same(tp_copy, hb.at[p, c, pl.ds(i, m), :], axr.at[j], xp) for j, (c, i, m) in enumerate(pieces)]
    for copy in ax[:4]:
        go(copy)
    ac = go(same(tp_copy, hb.at[p], acr, core))
    w_sends = [
        go(tp_copy(wo_ref.at[:, pl.ds(pl.multiple_of(core * width, LANES), width)], wo.at[p], sent, wor.at[0], core))
    ]

    for load in loads:
        load.wait()
    flat_gain = gain_in[...].astype(f32)
    for j in range(flat_gain.shape[0]):
        each = width // LANES
        gain[j // each, :, (j % each) * LANES : (j % each + 1) * LANES] = flat_gain[j : j + 1]

    def chunk(raw, q):
        raw = raw.astype(f32)
        scaled = (raw * gain[q]).astype(bf16)
        w = wall[pl.ds(pl.multiple_of(q * width, LANES), width), :]
        return jnp.dot(scaled, w, preferred_element_type=f32), jnp.sum(raw * raw, axis=1, keepdims=True)

    def add_all(q, first):
        prod, more = chunk(hb[q].reshape(rows, width), q)
        prod, more = prod.reshape(n, sub, 3 * lw), more.reshape(n, sub, 1)
        acc[...] = prod if first else acc[...] + prod
        sq[...] = more if first else sq[...] + more

    add_all(p, True)
    ac.wait_recv()
    add_all(core, False)

    def finish(acc, sq, table, places, span):
        raw = acc * lax.rsqrt(sq / (width * 4) + EPSILON)
        cosine, sine = table[:, :hd], table[:, hd:]
        for h in range(heads):
            for j, gains in enumerate((qgain, kgain, None)):
                x = raw[:, j * lw + h * hd : j * lw + (h + 1) * hd]
                if gains is not None:
                    x = x * lax.rsqrt(jnp.mean(x * x, axis=-1, keepdims=True) + EPSILON)
                    x = x * gains[pl.ds(h, 1), :]
                    x = x * cosine + pltpu.roll(x, hd // 2, 1) * sine
                for q_ref, kv_ref, c in places:
                    if j == 0:
                        q_ref[c, h, span] = x.astype(bf16)
                    else:
                        kv_ref[c, h, span, (j - 1) * hd : j * hd] = x.astype(bf16)

    def take(j):
        c, i, m = pieces[j]
        ax[j].wait_recv()
        go(same(tp_copy, hb.at[xp, c, pl.ds(i, m), :], afr.at[j], core))

    def close(j, places, between):
        c, i, m = pieces[j]
        span = slice(i, i + m)
        prod, more = chunk(hb[xp, c, span], xp)
        between()
        same(tp_copy, hb.at[diag, c, pl.ds(i, m), :], afr.at[j], core).wait_recv()
        last, most = chunk(hb[diag, c, span], diag)
        finish(acc[c, span] + prod + last, sq[c, span] + more + most, tb[c, span], places, span)

    cx, cc = {}, {}

    def spread(a):
        zs[a].wait_recv()
        cx[a] = go(same(tp_copy, hm.at[p, a], cxr.at[a], xp))
        cc[a] = go(same(tp_copy, hm.at[p, a], ccr, core))

    def cross(a):
        cx[a].wait_recv()
        go(same(tp_copy, hm.at[xp, a], cfr, core))

    parts_of = {1: pieces[2:3], 2: pieces[:2]}

    def class_copy(own, other, sems, k, h, j, arriving):
        _, i, m = parts_of[k][j]
        q = peer[k]
        mine = other.at[q, h, pl.ds(i, m), :]
        if arriving:
            return same(sp_copy, mine, sems.at[k - 1, h, j], q)
        return sp_copy(own.at[q, h, pl.ds(i, m), :], other.at[s, h, pl.ds(i, m), :], sent, sems.at[k - 1, h, j], q)

    kv_copy = functools.partial(class_copy, kv_b, kv_c, kr)
    q_copy = functools.partial(class_copy, q_b, q_c, qr)

    def give(k, j):
        for h in range(heads):
            @pl.when(s < n - 1)
            def _():
                kv_copy(k, h, j, False).start()

            @pl.when(s > 0)
            def _():
                q_copy(k, h, j, False).start()

    def receive(k, h):
        @pl.when(peer[k] < n - 1)
        def _():
            for j in range(len(parts_of[k])):
                kv_copy(k, h, j, True).wait_recv()

        @pl.when(peer[k] > 0)
        def _():
            for j in range(len(parts_of[k])):
                q_copy(k, h, j, True).wait_recv()

    quarter = lw // 4

    def quarter_of(a):
        return pl.ds(pl.multiple_of((2 * g + a) * quarter, 8), quarter)

    def spread_first():
        spread(0)
        go(ax[4])

    def spread_last():
        spread(1)
        go(ax[5])
        for j, q in ((0, xp), (1, diag)):
            for a in range(2):
                block = quarter_of(a)
                w_sends.append(go(tp_copy(
                    wo_ref.at[block, pl.ds(pl.multiple_of(q * width, LANES), width)], wo.at[p, block],
                    sent, wor.at[1 + 2 * j + a], q,
                )))

    def add_mirror(q):
        prod, more = chunk(hm[q].reshape(sub, width), q)
        return prod, more

    squares = []

    def start_mirror():
        same(tp_copy, hm.at[core], ccr, core).wait_recv()
        first, one = add_mirror(p)
        prod, more = add_mirror(core)
        acc_m[...] = first + prod
        squares.append(one + more)
        cross(0)

    def log_count(*read):
        count = sum(each.astype(f32) for each in read)
        bias = jnp.where(count == 2, math.log(2.0), jnp.where(count == 3, math.log(3.0), 0.0))
        return jnp.where(count == 0, -jnp.inf, bias)

    def strided(behind, step):
        return (behind >= 0) & (behind <= KEYS_BEHIND * step) & ((behind + rows * step) % step == 0)

    later = (rows - sub, rows - sub)
    late, early = iota(later, 0) + sub, iota(later, 1)
    stride = WIDEST_DILATION // n
    crosses = late // sub > early // sub
    bias_far[...] = log_count(strided(late - early, 1) & crosses, strided(late - early, stride) & crosses)
    behind = row_of(iota(square, 0), sub) - row_of(iota(square, 1), sub)
    bias_near[...] = log_count(*(strided(behind, step) for step in (1, n, WIDEST_DILATION)))
    take(0)
    close(0, ((q_b, kv_b, two),), lambda: None)
    give(2, 0)
    take(1)
    close(1, ((q_b, kv_b, two),), spread_first)
    give(2, 1)
    take(2)
    close(2, ((q_b, kv_b, pair),), spread_last)
    give(1, 0)
    take(3)
    close(3, ((q_b, kv_b, s), (q_c, kv_c, s)), start_mirror)

    above = lax.rem(s + 1, n)

    def send_halo(c):
        sp_copy(kv_b.at[c, :, pl.ds(sub - halo_sub, halo_sub), :], halo.at[c], sent, hr, above).start()

    take(4)

    @pl.when(s < n - 1)
    def _():
        send_halo(two)
        send_halo(s)

    @pl.when(s == 1)
    def _():
        send_halo(pair)

    close(4, ((q_b, kv_b, mirror),), lambda: None)

    @pl.when((s < n - 1) & (s != 1))
    def _():
        send_halo(mirror)

    cross(1)
    prod, more = add_mirror(xp)
    take(5)
    same(tp_copy, hm.at[diag], cfr, core).wait_recv()
    last, most = add_mirror(diag)
    finish(acc_m[...] + prod + last, squares[0] + more + most, tm[...], ((q_c, kv_c, mirror),), slice(0, sub))

    def attend(q, k, v, bias):
        score = lax.dot_general(q, k, (((1,), (1,)), ((), ())), preferred_element_type=f32)
        score = score * hd ** (-0.5) + bias
        top = jnp.max(score, axis=-1, keepdims=True)
        weight = jnp.exp(score - top)
        total = jnp.sum(weight, axis=-1, keepdims=True)
        out = jnp.dot(weight.astype(bf16), v, preferred_element_type=f32) / total
        return out, top + jnp.log(total)

    lane = iota((rows, LANES), 1)

    def as_rows(columns):
        spread_out = jnp.full((sub, LANES), -jnp.inf, f32)
        for c, column in enumerate(columns):
            if column is not None:
                spread_out = jnp.where(lane[:sub] == c, column, spread_out)
        pad = jnp.zeros((LANES - sub, LANES), f32)
        return jnp.transpose(jnp.concatenate([spread_out, pad], axis=0))[:8]

    def flat(x):
        return x.reshape(x.shape[0] * x.shape[1], x.shape[2])

    def far_head(h):
        receive(2, h)
        receive(1, h)
        out, lse = attend(
            flat(q_c[1:, h]), flat(kv_c[: n - 1, h, :, :hd]), flat(kv_c[: n - 1, h, :, hd:]), bias_far[...]
        )
        lsend[h] = as_rows([None] + [lse[b * sub : (b + 1) * sub] for b in range(n - 1)])
        rl[s, h] = lsend[h]
        oc[h, 1:] = out.astype(bf16).reshape(n - 1, sub, hd)
        for k in (3, 2, 1):
            @pl.when(peer[k] > 0)
            def _():
                sp_copy(lsend.at[h], rl.at[s, h], sent, lr.at[k - 1, h], peer[k]).start()
                sp_copy(oc.at[h, peer[k]], ro.at[s, h], sent, rr.at[k - 1, h], peer[k]).start()

    wf = []

    def pass_on(j):
        piece = wo.at[(xp, diag)[j // 2], quarter_of(j % 2)]
        w_sends[j + 1].wait_recv()
        wf.append(go(copy_to("grp", piece, piece, sent, wfr.at[j], 1 - g)))

    far_head(0)
    for h in range(1, heads):
        far_head(h)
    pass_on(0)
    close(5, ((q_b, kv_b, mirror),), lambda: None)
    pass_on(1)

    others = pl.ds(0, n - 1)

    def pair_of(piece, j, near_sem):
        return same(tp_copy, piece, gxr.at[j], xp), same(tp_copy, piece, near_sem, core)

    def index(k, h):
        return 1 + h * (n - 1) + k - 1

    shared = [pair_of(at_own.at[p], 0, gor)]
    for h in range(heads):
        for k in range(1, n):
            shared.append(pair_of(at.at[p, h, k - 1], index(k, h), gcr))

    def share(j):
        for copy in shared[j]:
            copy.start()

    for h in range(heads):
        out, lse = attend(flat(q_b[:, h]), flat(kv_b[:, h, :, :hd]), flat(kv_b[:, h, :, hd:]), bias_near[...])
        near_out[h] = out.reshape(n, sub, hd)
        near_row[h] = as_rows([lse[c * sub : (c + 1) * sub] for c in range(n)])

        @pl.when(s == 0)
        def _():
            at_own[p, h] = near_out[h, 0].astype(bf16)
            for c in range(1, n):
                at[p, h, c - 1] = near_out[h, c].astype(bf16)
            if h == heads - 1:
                share(0)
            for k in range(1, n):
                share(index(k, h))
            all_log[h] = near_row[h]

    pass_on(2)

    @pl.when(s > 0)
    def _():
        sp_copy(halo.at[pl.ds(0, n - 1)], halo.at[pl.ds(0, n - 1)], sent, hr, above).wait_recv()
        halo[s] = kv_c[s - 1, :, sub - halo_sub :, :]
        small = (halo_rows, halo_rows)
        behind = row_of(iota(small, 0), halo_sub) - row_of(iota(small, 1), halo_sub) + halo_rows
        bias_h = jnp.where(behind <= KEYS_BEHIND, 0.0, -jnp.inf).astype(f32)
        for h in range(heads):
            out, lse = attend(
                flat(q_b[:, h, :halo_sub]), flat(halo[:, h, :, :hd]), flat(halo[:, h, :, hd:]), bias_h
            )
            halo_out[h] = out.reshape(n, halo_sub, hd)
            pad = jnp.full((sub - halo_sub, 1), -jnp.inf, f32)
            halo_row[h] = as_rows([
                jnp.concatenate([lse[c * halo_sub : (c + 1) * halo_sub], pad], axis=0) for c in range(n)
            ])

    which = iota((8, LANES), 0)

    def weigh(own, low, far_row):
        top = jnp.maximum(jnp.maximum(own, low), far_row)
        exps = [jnp.exp(x - top) for x in (own, low, far_row)]
        both = exps[0] + exps[1] + exps[2]
        return [x / both for x in exps], top + jnp.log(both)

    def as_columns(shares):
        pad = jnp.zeros((LANES - 8 * len(shares), LANES), f32)
        return jnp.transpose(jnp.concatenate(shares + [pad], axis=0))[:sub]

    def blend(parts, own, far_out, low):
        sums = parts[0] * own + parts[2] * far_out.astype(f32)
        return jnp.concatenate([sums[:halo_sub] + parts[1][:halo_sub] * low, sums[halo_sub:]], axis=0).astype(bf16)

    mine = pl.ds(s, 1)

    def merge(c, hs):
        row = pl.ds(c, 1)
        rows_of = jnp.zeros((8, LANES), f32)
        for i, h in enumerate(hs):
            shares, all_log[h, row] = weigh(near_row[h, row], halo_row[h, row], rl[c, h, mine])
            for j, x in enumerate(shares):
                rows_of = jnp.where(which == 3 * i + j, x, rows_of)
        columns = as_columns([rows_of])
        return [[columns[:, 3 * i + j : 3 * i + j + 1] for j in range(3)] for i in range(len(hs))]

    @pl.when(s > 0)
    def _():
        for h, parts in enumerate(merge(s, range(heads))):
            at_own[p, h] = blend(parts, near_out[h, s], oc[h, s], halo_out[h, s])
        share(0)

    pass_on(3)

    @pl.when(s > 0)
    def _():
        for h in range(heads):
            for k in range(1, n):
                c = peer[k]
                same(sp_copy, rl.at[c, h], lr.at[k - 1, h], c).wait_recv()
                same(sp_copy, ro.at[c, h], rr.at[k - 1, h], c).wait_recv()
                at[p, h, k - 1] = blend(merge(c, (h,))[0], near_out[h, c], ro[c, h], halo_out[h, c])
                share(index(k, h))

    block = iota(square, 1) // sub
    class_of = jnp.where(block == 0, pair, jnp.where(block == 1, two, jnp.where(block == 2, mirror, s)))
    from_class = (iota(square, 0) == n * lax.rem(iota(square, 1), sub) + class_of).astype(f32).astype(bf16)

    def product(q):
        x = jnp.concatenate([
            jnp.concatenate([flat(at[q, h, : n - 1]), at_own[q, h]], axis=0) for h in range(heads)
        ], axis=1)
        return jnp.dot(x, wo[q], preferred_element_type=f32)

    def forward(j):
        shared[j][0].wait_recv()
        if j == 0:
            go(same(tp_copy, at_own.at[xp], gpr, core))
        else:
            go(same(tp_copy, at.at[xp, (j - 1) // (n - 1), (j - 1) % (n - 1)], gfr, core))

    by_head = iota((8, LANES), 0)
    logs = []
    for c in range(n):
        row = jnp.zeros((8, LANES), f32)
        for h in range(heads):
            row = jnp.where(by_head == h, all_log[h, c : c + 1, :], row)
        logs.append(row)
    logs = jnp.concatenate(logs, axis=1)
    placed = (n * LANES, rows)
    to_order = (
        (n * lax.rem(iota(placed, 0), LANES) + iota(placed, 0) // LANES == iota(placed, 1))
        & (lax.rem(iota(placed, 0), LANES) < sub)
    ).astype(f32).astype(bf16)
    high = logs.astype(bf16)
    rest = logs - high.astype(f32)
    middle = rest.astype(bf16)
    low = (rest - middle.astype(f32)).astype(bf16)
    total = sum(jnp.dot(x, to_order, preferred_element_type=f32) for x in (high, middle, low))
    total_ref[...] = total[:heads]

    result = product(p)
    for j in (*range(1, n), 0, *range(n, len(shared))):
        forward(j)
    w_sends[0].wait_recv()
    same(tp_copy, at_own.at[core], gor, core).wait_recv()
    same(tp_copy, at.at[core, :, others], gcr, core).wait_recv()
    result += product(core)
    for copy in wf:
        copy.wait_recv()
    result += product(xp)
    same(tp_copy, at_own.at[diag], gpr, core).wait_recv()
    same(tp_copy, at.at[diag, :, others], gfr, core).wait_recv()
    result += product(diag)
    mixed_ref[...] = jnp.dot(from_class, result.astype(bf16), preferred_element_type=f32).astype(bf16)
    back = heads * (sub * hd * 2 + 8 * LANES * 4)
    q_bytes, kv_bytes = 2 * heads * sub * hd * 2, 2 * heads * sub * 2 * hd * 2
    halo_bytes = (n - 1) * heads * halo_sub * 2 * hd * 2
    at_bytes = 2 * rows * lw * 2

    def all_sent(total):
        same(tp_copy, drain.at[pl.ds(0, total // (LANES * 4))], acr, core).wait_send()

    @pl.when(s == 0)
    def _():
        all_sent(sum(sends) + at_bytes + kv_bytes + halo_bytes + 3 * back)

    @pl.when((s > 0) & (s < n - 1))
    def _():
        all_sent(sum(sends) + at_bytes + q_bytes + kv_bytes + halo_bytes + 2 * back)

    @pl.when(s == n - 1)
    def _():
        all_sent(sum(sends) + at_bytes + q_bytes + 2 * back)


def write_kernel(mixed_ref, total_ref, out_ref, log_ref, sems):
    copies = [
        pltpu.make_async_copy(mixed_ref, out_ref, sems.at[0]),
        pltpu.make_async_copy(total_ref, log_ref, sems.at[1]),
    ]
    for copy in copies:
        copy.start()
    for copy in copies:
        copy.wait()


def local_by_class(hidden, norm_gain, w_query, w_key, w_value, query_gain, key_gain, w_out):
    n = MIDDLE_DILATION
    rows, width = hidden.shape
    heads, hd = query_gain.shape
    lw = heads * hd
    sub = rows // n
    halo_sub = KEYS_BEHIND // n
    bf16, f32 = jnp.bfloat16, jnp.float32
    table = jnp.asarray(rotary_table(n, sub, hd))
    most_bytes = 2 * (16 * sub * width + 3 * lw * width + 30 * sub * lw) + 3 * heads * 8 * LANES * 4
    vmem = pl.BlockSpec(memory_space=pltpu.VMEM)
    anyspace = pl.BlockSpec(memory_space=pl.ANY)
    dma = pltpu.SemaphoreType.DMA
    mixed, total = pl.pallas_call(
        class_kernel,
        out_shape=(
            pltpu.VMEM((rows, w_out.shape[1] // 4), bf16),
            pltpu.VMEM((heads, rows), f32),
        ),
        in_specs=[anyspace] * 9,
        out_specs=(vmem, vmem),
        scratch_shapes=[
            pltpu.VMEM((rows, width), bf16),
            pltpu.VMEM((4 * width // LANES, LANES), bf16),
            pltpu.VMEM((heads, hd), f32),
            pltpu.VMEM((heads, hd), f32),
            pltpu.VMEM((4, n, sub, width), bf16),
            pltpu.VMEM((4, 2, sub // 2, width), bf16),
            pltpu.VMEM((4 * width, 3 * lw), bf16),
            pltpu.VMEM((4, lw, width), bf16),
            pltpu.VMEM((n, sub, 2 * hd), f32),
            pltpu.VMEM((sub, 2 * hd), f32),
            pltpu.VMEM((n, sub, 3 * lw), f32),
            pltpu.VMEM((sub, 3 * lw), f32),
            pltpu.VMEM((n, sub, 1), f32),
            pltpu.VMEM((n, heads, sub, hd), bf16),
            pltpu.VMEM((n, heads, sub, 2 * hd), bf16),
            pltpu.VMEM((n, heads, sub, hd), bf16),
            pltpu.VMEM((n, heads, sub, 2 * hd), bf16),
            pltpu.VMEM((n, heads, halo_sub, 2 * hd), bf16),
            pltpu.VMEM((heads, n, sub, hd), bf16),
            pltpu.VMEM((heads, 8, LANES), f32),
            pltpu.VMEM((n, heads, sub, hd), bf16),
            pltpu.VMEM((n, heads, 8, LANES), f32),
            pltpu.VMEM((heads, n, sub, hd), f32),
            pltpu.VMEM((heads, 8, LANES), f32),
            pltpu.VMEM((heads, n, halo_sub, hd), f32),
            pltpu.VMEM((heads, 8, LANES), f32),
            pltpu.VMEM((heads, 8, LANES), f32),
            pltpu.VMEM((4, heads, n, sub, hd), bf16),
            pltpu.VMEM((4, heads, sub, hd), bf16),
            pltpu.VMEM((rows - sub, rows - sub), f32),
            pltpu.VMEM((rows, rows), f32),
            pltpu.VMEM((4, 1, width), f32),
            pltpu.VMEM((most_bytes // (4 * LANES), LANES), f32),
            dma((10,)), dma, dma((2,)), dma((n + 2,)), dma, dma((n + 2,)), dma((2,)), dma, dma,
            dma((5,)), dma((4,)), dma((2, heads, 2)), dma((2, heads, 2)), dma, dma((3, heads)), dma((3, heads)),
            dma((1 + 3 * heads,)), dma, dma, dma, dma,
        ],
        compiler_params=pltpu.CompilerParams(
            collective_id=0, has_side_effects=True, vmem_limit_bytes=60 * 1024 * 1024
        ),
    )(
        hidden, norm_gain.reshape(-1, LANES), query_gain, key_gain,
        w_query, w_key, w_value, w_out, table,
    )
    mixed, total = pl.pallas_call(
        write_kernel,
        out_shape=(
            jax.ShapeDtypeStruct(mixed.shape, bf16), jax.ShapeDtypeStruct(total.shape, f32)
        ),
        in_specs=[vmem, vmem],
        out_specs=(anyspace, anyspace),
        scratch_shapes=[dma((2,))],
    )(
        pltpu.with_memory_space_constraint(mixed, pltpu.VMEM),
        pltpu.with_memory_space_constraint(total, pltpu.VMEM),
    )
    return mixed, total.T


def solution(mesh):
    split = (mesh.shape["grp"], mesh.shape["sp"], mesh.shape["tp"]) == (2, MIDDLE_DILATION, 4)
    chosen = local_by_class if split else local
    placed = (
        P(("grp", "sp"), "tp"),
        P(),
        P(None, "tp"),
        P(None, "tp"),
        P(None, "tp"),
        P("tp", None),
        P("tp", None),
        P("tp", None),
    )
    return jax.shard_map(
        chosen,
        mesh=mesh,
        in_specs=placed,
        out_specs=(P(("grp", "sp"), "tp"), P(("grp", "sp"), "tp")),
        check_vma=False,
    )
```

```python
import functools
import math

import jax
import jax.numpy as jnp
import numpy as np
from jax import lax
from jax.experimental import pallas as pl
from jax.experimental.pallas import tpu as pltpu
from jax.sharding import PartitionSpec as P

D = 2048
KEYS_BEHIND = 128
MIDDLE_DILATION = 4
WIDEST_DILATION = 16


EPSILON = 1e-06
ROTARY_BASE = 500000.0


def from_behind(value, axis, steps):
    count = lax.axis_size(axis)
    initial, last = (max(0, -steps), min(count, count - steps))
    return lax.ppermute(value, axis, [(source, source + steps) for source in range(initial, last)])


def rotate(values, positions):
    head_width = values.shape[-1]
    inverse = ROTARY_BASE ** (-jnp.arange(0, head_width, 2, dtype=jnp.float32) / head_width)
    angles = positions[:, None] * inverse[None, :]
    cosine = jnp.cos(angles)[:, None, :]
    sine = jnp.sin(angles)[:, None, :]
    half_width = head_width // 2
    first_half = values[..., :half_width]
    second_half = values[..., half_width:]
    return jnp.concatenate(
        [first_half * cosine - second_half * sine, second_half * cosine + first_half * sine],
        axis=-1,
    )


def head_norm(values, gains):
    normed = values * lax.rsqrt(jnp.mean(values * values, axis=-1, keepdims=True) + EPSILON)
    return normed * gains[None, :, :]


def earlier_pairs(own_pair, token_rows):
    distant_shards = (KEYS_BEHIND * WIDEST_DILATION + token_rows - 1) // token_rows
    pieces = [own_pair]
    for distance in range(1, distant_shards + 1):
        pieces.insert(0, from_behind(own_pair, "sp", distance))
    buffer = jnp.concatenate(pieces, axis=1)
    return buffer


def local_branch(query, key_rows, value_rows, dilation_step, first_pos):
    token_rows, head_count, head_width = query.shape
    reach_rows = KEYS_BEHIND * dilation_step
    buffer_rows = key_rows.shape[0]
    class_rows = token_rows // dilation_step
    class_keys = class_rows + KEYS_BEHIND
    window_start = buffer_rows - token_rows - reach_rows
    key_window = key_rows[window_start:]
    value_window = value_rows[window_start:]
    query_class = query.reshape(class_rows, dilation_step, head_count, head_width).transpose(
        1, 0, 2, 3
    )
    key_class = key_window.reshape(class_keys, dilation_step, head_count, head_width).transpose(
        1, 0, 2, 3
    )
    value_class = value_window.reshape(class_keys, dilation_step, head_count, head_width).transpose(
        1, 0, 2, 3
    )
    block_rows = math.gcd(class_rows, KEYS_BEHIND) if class_rows > KEYS_BEHIND else class_rows
    block_count = class_rows // block_rows
    query_blocks = query_class.reshape(
        dilation_step, block_count, block_rows, head_count, head_width
    )
    key_blocks = jnp.stack(
        [
            key_class[:, number * block_rows : number * block_rows + block_rows + KEYS_BEHIND]
            for number in range(block_count)
        ],
        axis=1,
    )
    value_blocks = jnp.stack(
        [
            value_class[:, number * block_rows : number * block_rows + block_rows + KEYS_BEHIND]
            for number in range(block_count)
        ],
        axis=1,
    )
    scores = jnp.einsum(
        "rnqhd,rnkhd->rnhqk", query_blocks, key_blocks, preferred_element_type=jnp.float32
    ) * head_width ** (-0.5)
    row_index = jnp.arange(block_rows, dtype=jnp.int32)[:, None]
    col_index = jnp.arange(block_rows + KEYS_BEHIND, dtype=jnp.int32)[None, :]
    distance = KEYS_BEHIND + row_index - col_index
    in_band = (distance >= 0) & (distance <= KEYS_BEHIND)
    class_index = jnp.arange(block_count, dtype=jnp.int32)[:, None] * block_rows + col_index
    residue = jnp.arange(dilation_step, dtype=jnp.int32)[:, None, None]
    key_position = first_pos - reach_rows + class_index[None] * dilation_step + residue
    allowed = in_band[None, None, None, :, :] & (key_position >= 0)[:, :, None, None, :]
    scores = jnp.where(allowed, scores, -jnp.inf)
    row_max = jnp.max(scores, axis=-1, keepdims=True)
    weights = jnp.exp(scores - row_max)
    weight_sum = jnp.sum(weights, axis=-1)
    weighted = jnp.einsum(
        "rnhqk,rnkhd->rnqhd",
        weights.astype(jnp.bfloat16),
        value_blocks,
        preferred_element_type=jnp.float32,
    )
    branch_out = weighted / jnp.transpose(weight_sum, (0, 1, 3, 2))[..., None]
    branch_out = branch_out.reshape(dilation_step, class_rows, head_count, head_width).transpose(
        1, 0, 2, 3
    )
    branch_out = branch_out.reshape(token_rows, head_count, head_width)
    log_sum = jnp.transpose(row_max[..., 0] + jnp.log(weight_sum), (0, 1, 3, 2))
    log_sum = (
        log_sum.reshape(dilation_step, class_rows, head_count)
        .transpose(1, 0, 2)
        .reshape(token_rows, head_count)
    )
    return (branch_out, log_sum)


def local(hidden, norm_gain, w_query, w_key, w_value, query_gain, key_gain, w_out):
    token_rows = hidden.shape[0]
    local_width = w_query.shape[1]
    head_count = query_gain.shape[0]
    head_width = query_gain.shape[1]
    gain_full = norm_gain.astype(jnp.float32)
    raw_piece = lax.all_gather(hidden, "tp", axis=1, tiled=True).astype(jnp.float32)
    scaled = (raw_piece * gain_full[None, :]).astype(jnp.bfloat16)

    def add_product(weight):
        return jnp.dot(scaled, weight, preferred_element_type=jnp.float32)

    query_raw = add_product(w_query)
    key_raw = add_product(w_key)
    value_raw = add_product(w_value)
    squares = jnp.sum(raw_piece * raw_piece, axis=1)
    row_scale = lax.rsqrt(squares / D + EPSILON)[:, None]
    first_pos = lax.axis_index("sp") * token_rows
    positions = (jnp.arange(token_rows, dtype=jnp.int32) + first_pos).astype(jnp.float32)
    query = rotate(
        head_norm((query_raw * row_scale).reshape(token_rows, head_count, head_width), query_gain),
        positions,
    ).astype(jnp.bfloat16)
    key_now = rotate(
        head_norm((key_raw * row_scale).reshape(token_rows, head_count, head_width), key_gain),
        positions,
    ).astype(jnp.bfloat16)
    value_now = (value_raw * row_scale).astype(jnp.bfloat16)
    own_pair = jnp.stack([key_now.reshape(token_rows, local_width), value_now], axis=0)
    buffer = earlier_pairs(own_pair, token_rows)
    key_rows = buffer[0].reshape(-1, head_count, head_width)
    value_rows = buffer[1].reshape(-1, head_count, head_width)
    branch_outs = []
    branch_logs = []
    for dilation_step in (1, MIDDLE_DILATION, WIDEST_DILATION):
        branch_out, log_sum = local_branch(query, key_rows, value_rows, dilation_step, first_pos)
        branch_outs.append(branch_out)
        branch_logs.append(log_sum)
    stacked_logs = jnp.stack(branch_logs, axis=0)
    peak = jnp.max(stacked_logs, axis=0)
    log_total = peak + jnp.log(jnp.sum(jnp.exp(stacked_logs - peak[None]), axis=0))
    shares = jnp.exp(stacked_logs - log_total[None])
    attended = jnp.sum(shares[..., None] * jnp.stack(branch_outs, axis=0), axis=0)
    attended = attended.astype(jnp.bfloat16).reshape(token_rows, local_width)
    column_block = lax.all_to_all(w_out, "tp", split_axis=1, concat_axis=0, tiled=True)
    mixed = jnp.dot(
        lax.all_gather(attended, "tp", axis=1, tiled=True),
        column_block,
        preferred_element_type=jnp.float32,
    )
    return (mixed.astype(jnp.bfloat16), log_total)


MESH = pl.DeviceIdType.MESH
LANES = 128


def rotary_table(classes, rows, head_width):
    inverse = (ROTARY_BASE ** (-np.arange(0, head_width, 2, dtype=np.float64) / head_width)).astype(np.float32)
    positions = np.arange(classes * classes * rows, dtype=np.float32)
    angles = (positions[:, None] * inverse[None, :]).astype(np.float64)
    cosine, sine = np.cos(angles), np.sin(angles)
    table = np.concatenate([cosine, cosine, -sine, sine], axis=1).astype(np.float32)
    return table.reshape(classes, rows, classes, 2 * head_width).transpose(0, 2, 1, 3)


def class_kernel(
    hid_ref, gain_ref, qgain_ref, kgain_ref, wq_ref, wk_ref, wv_ref, wo_ref, table_ref,
    mixed_ref, total_ref,
    hid, gain_in, qgain, kgain, hb, hm, wall, wo, tb, tm, acc, acc_m, sq, q_b, kv_b, q_c, kv_c,
    halo, oc, lsend, ro, rl, near_out, near_row, halo_out, halo_row, all_log, at, at_own, bias_far, bias_near, gain, drain,
    loc, sent, zr, axr, acr, afr, cxr, ccr, cfr, wor, wfr, wzr, qr, kr, hr, rr, lr, gxr, gcr, gfr, gor, gpr,
):
    f32, bf16 = jnp.float32, jnp.bfloat16
    g, s, p = lax.axis_index("grp"), lax.axis_index("sp"), lax.axis_index("tp")
    n = MIDDLE_DILATION
    rows, width = hid_ref.shape
    sub = rows // n
    heads, hd = qgain_ref.shape
    lw = heads * hd
    halo_sub = halo.shape[2]
    halo_rows = n * halo_sub
    core = p + 1 - 2 * lax.rem(p, 2)
    xp = lax.rem(p + 2, 4)
    diag = lax.rem(core + 2, 4)
    pair, two, mirror = s + 1 - 2 * lax.rem(s, 2), lax.rem(s + 2, n), n - 1 - s
    peer = (s, pair, two, mirror)
    part = sub // 2
    pieces = (
        (two, 0, part), (two, part, part), (pair, 0, sub), (s, 0, sub), (mirror, sub - halo_sub, halo_sub), (mirror, 0, sub - halo_sub)
    )

    def copy_to(axis, src, dst, ss, sr, q):
        return pltpu.make_async_remote_copy(
            src_ref=src, dst_ref=dst, send_sem=ss, recv_sem=sr, device_id={axis: q}, device_id_type=MESH
        )

    tp_copy = functools.partial(copy_to, "tp")
    sp_copy = functools.partial(copy_to, "sp")

    def same(copy, ref, sr, q):
        return copy(ref, ref, sent, sr, q)

    load_hid = pltpu.make_async_copy(hid_ref, hid, loc.at[1])
    load_hid.start()
    barrier = pltpu.get_barrier_semaphore()
    for k in (3, 2, 1):
        pl.semaphore_signal(barrier, inc=1, device_id={"sp": peer[k]}, device_id_type=MESH)
    for q in (xp, diag, core):
        pl.semaphore_signal(barrier, inc=1, device_id={"tp": q}, device_id_type=MESH)
    pl.semaphore_signal(barrier, inc=1, device_id={"grp": 1 - g}, device_id_type=MESH)
    loads = [
        pltpu.make_async_copy(gain_ref, gain_in, loc.at[0]),
        pltpu.make_async_copy(qgain_ref, qgain, loc.at[2]),
        pltpu.make_async_copy(kgain_ref, kgain, loc.at[3]),
        pltpu.make_async_copy(wq_ref, wall.at[:, pl.ds(0, lw)], loc.at[4]),
        pltpu.make_async_copy(wk_ref, wall.at[:, pl.ds(lw, lw)], loc.at[5]),
        pltpu.make_async_copy(wv_ref, wall.at[:, pl.ds(2 * lw, lw)], loc.at[6]),
        pltpu.make_async_copy(table_ref.at[s], tb, loc.at[7]),
        pltpu.make_async_copy(table_ref.at[mirror, s], tm, loc.at[8]),
        pltpu.make_async_copy(
            wo_ref.at[:, pl.ds(pl.multiple_of(p * width, LANES), width)], wo.at[p], loc.at[9]
        ),
    ]
    for load in loads:
        load.start()

    def iota(shape, dim):
        return lax.broadcasted_iota(jnp.int32, shape, dim)

    def row_of(r, part):
        return n * lax.rem(r, part) + r // part

    square = (rows, rows)
    to_class = (row_of(iota(square, 0), sub) == iota(square, 1)).astype(f32).astype(bf16)
    load_hid.wait()
    permuted = jnp.dot(to_class, hid[...], preferred_element_type=f32).astype(bf16)
    hb[p] = permuted.reshape(n, sub, width)
    pl.semaphore_wait(barrier, 3 + n)

    sends = []

    def go(copy):
        copy.start()
        sends.append(math.prod(copy.src_ref.shape) * copy.src_ref.dtype.itemsize)
        return copy

    zs = [
        go(sp_copy(hb.at[p, mirror, pl.ds(a * part, part), :], hm.at[p, a], sent, zr.at[a], mirror))
        for a in range(2)
    ]
    ax = [same(tp_copy, hb.at[p, c, pl.ds(i, m), :], axr.at[j], xp) for j, (c, i, m) in enumerate(pieces)]
    for copy in ax[:4]:
        go(copy)
    ac = go(same(tp_copy, hb.at[p], acr, core))
    w_core = go(tp_copy(
        wo_ref.at[:, pl.ds(pl.multiple_of(core * width, LANES), width)],
        wo.at[p], sent, wor.at[0], core,
    ))

    for load in loads:
        load.wait()
    flat_gain = gain_in[...].astype(f32)
    for j in range(flat_gain.shape[0]):
        each = width // LANES
        gain[j // each, :, (j % each) * LANES : (j % each + 1) * LANES] = flat_gain[j : j + 1]

    def chunk(raw, q):
        raw = raw.astype(f32)
        scaled = (raw * gain[q]).astype(bf16)
        w = wall[pl.ds(pl.multiple_of(q * width, LANES), width), :]
        return jnp.dot(scaled, w, preferred_element_type=f32), jnp.sum(raw * raw, axis=1, keepdims=True)

    def add_all(q, first):
        prod, more = chunk(hb[q].reshape(rows, width), q)
        prod, more = prod.reshape(n, sub, 3 * lw), more.reshape(n, sub, 1)
        acc[...] = prod if first else acc[...] + prod
        sq[...] = more if first else sq[...] + more

    add_all(p, True)
    ac.wait_recv()
    add_all(core, False)

    def finish(acc, sq, table, places, span):
        raw = acc * lax.rsqrt(sq / (width * 4) + EPSILON)
        cosine, sine = table[:, :hd], table[:, hd:]
        for h in range(heads):
            for j, gains in enumerate((qgain, kgain, None)):
                x = raw[:, j * lw + h * hd : j * lw + (h + 1) * hd]
                if gains is not None:
                    x = x * lax.rsqrt(jnp.mean(x * x, axis=-1, keepdims=True) + EPSILON)
                    x = x * gains[pl.ds(h, 1), :]
                    x = x * cosine + pltpu.roll(x, hd // 2, 1) * sine
                for q_ref, kv_ref, c in places:
                    if j == 0:
                        q_ref[c, h, span] = x.astype(bf16)
                    else:
                        kv_ref[c, h, span, (j - 1) * hd : j * hd] = x.astype(bf16)

    def take(j):
        c, i, m = pieces[j]
        ax[j].wait_recv()
        go(same(tp_copy, hb.at[xp, c, pl.ds(i, m), :], afr.at[j], core))

    def close(j, places, between):
        c, i, m = pieces[j]
        span = slice(i, i + m)
        prod, more = chunk(hb[xp, c, span], xp)
        between()
        same(tp_copy, hb.at[diag, c, pl.ds(i, m), :], afr.at[j], core).wait_recv()
        last, most = chunk(hb[diag, c, span], diag)
        finish(acc[c, span] + prod + last, sq[c, span] + more + most, tb[c, span], places, span)

    cx, cc = {}, {}

    def spread(a):
        zs[a].wait_recv()
        cx[a] = go(same(tp_copy, hm.at[p, a], cxr.at[a], xp))
        cc[a] = go(same(tp_copy, hm.at[p, a], ccr, core))

    def cross(a):
        cx[a].wait_recv()
        go(same(tp_copy, hm.at[xp, a], cfr, core))

    parts_of = {1: pieces[2:3], 2: pieces[:2]}

    def class_copy(own, other, sems, k, h, j, arriving):
        _, i, m = parts_of[k][j]
        q = peer[k]
        mine = other.at[q, h, pl.ds(i, m), :]
        if arriving:
            return same(sp_copy, mine, sems.at[k - 1, h, j], q)
        return sp_copy(own.at[q, h, pl.ds(i, m), :], other.at[s, h, pl.ds(i, m), :], sent, sems.at[k - 1, h, j], q)

    kv_copy = functools.partial(class_copy, kv_b, kv_c, kr)
    q_copy = functools.partial(class_copy, q_b, q_c, qr)

    def give(k, j):
        for h in range(heads):
            @pl.when(s < n - 1)
            def _():
                kv_copy(k, h, j, False).start()

            @pl.when(s > 0)
            def _():
                q_copy(k, h, j, False).start()

    def receive(k, h):
        @pl.when(peer[k] < n - 1)
        def _():
            for j in range(len(parts_of[k])):
                kv_copy(k, h, j, True).wait_recv()

        @pl.when(peer[k] > 0)
        def _():
            for j in range(len(parts_of[k])):
                q_copy(k, h, j, True).wait_recv()

    quarter = lw // 4

    def quarter_of(a):
        return pl.ds(pl.multiple_of((2 * g + a) * quarter, 8), quarter)

    def w_copy(i):
        q, block = (xp, diag)[i // 2], quarter_of(i % 2)
        source = wo_ref.at[block, pl.ds(pl.multiple_of(q * width, LANES), width)]
        return tp_copy(source, wo.at[p, block], sent, wor.at[1 + i], q)

    w_copies = [w_copy(i) for i in range(4)]

    def spread_first():
        spread(0)
        go(ax[4])

    def spread_last():
        spread(1)
        go(ax[5])
        @pl.when(s > 0)
        def _():
            w_copies[3].start()

        for copy in w_copies[:3]:
            go(copy)

    def add_mirror(q):
        prod, more = chunk(hm[q].reshape(sub, width), q)
        return prod, more

    squares = []

    def start_mirror():
        same(tp_copy, hm.at[core], ccr, core).wait_recv()
        first, one = add_mirror(p)
        prod, more = add_mirror(core)
        acc_m[...] = first + prod
        squares.append(one + more)
        cross(0)

    def log_count(*read):
        count = sum(each.astype(f32) for each in read)
        bias = jnp.where(count == 2, math.log(2.0), jnp.where(count == 3, math.log(3.0), 0.0))
        return jnp.where(count == 0, -jnp.inf, bias)

    def strided(behind, step):
        return (behind >= 0) & (behind <= KEYS_BEHIND * step) & ((behind + rows * step) % step == 0)

    later = (rows - sub, rows - sub)
    late, early = iota(later, 0) + sub, iota(later, 1)
    stride = WIDEST_DILATION // n
    crosses = late // sub > early // sub
    bias_far[...] = log_count(strided(late - early, 1) & crosses, strided(late - early, stride) & crosses)
    behind = row_of(iota(square, 0), sub) - row_of(iota(square, 1), sub)
    bias_near[...] = log_count(*(strided(behind, step) for step in (1, n, WIDEST_DILATION)))
    take(0)
    close(0, ((q_b, kv_b, two),), lambda: None)
    give(2, 0)
    take(1)
    close(1, ((q_b, kv_b, two),), spread_first)
    give(2, 1)
    take(2)
    close(2, ((q_b, kv_b, pair),), spread_last)
    give(1, 0)
    take(3)
    close(3, ((q_b, kv_b, s), (q_c, kv_c, s)), start_mirror)

    above = lax.rem(s + 1, n)

    def send_halo(c):
        sp_copy(kv_b.at[c, :, pl.ds(sub - halo_sub, halo_sub), :], halo.at[c], sent, hr, above).start()

    take(4)

    @pl.when(s < n - 1)
    def _():
        send_halo(two)
        send_halo(s)

    @pl.when(s == 1)
    def _():
        send_halo(pair)

    close(4, ((q_b, kv_b, mirror),), lambda: None)

    @pl.when((s < n - 1) & (s != 1))
    def _():
        send_halo(mirror)

    cross(1)
    prod, more = add_mirror(xp)
    take(5)
    same(tp_copy, hm.at[diag], cfr, core).wait_recv()
    last, most = add_mirror(diag)
    finish(acc_m[...] + prod + last, squares[0] + more + most, tm[...], ((q_c, kv_c, mirror),), slice(0, sub))

    def attend(q, k, v, bias):
        score = lax.dot_general(q, k, (((1,), (1,)), ((), ())), preferred_element_type=f32)
        score = score * hd ** (-0.5) + bias
        top = jnp.max(score, axis=-1, keepdims=True)
        weight = jnp.exp(score - top)
        total = jnp.sum(weight, axis=-1, keepdims=True)
        out = jnp.dot(weight.astype(bf16), v, preferred_element_type=f32) / total
        return out, top + jnp.log(total)

    lane = iota((rows, LANES), 1)

    def as_rows(columns):
        spread_out = jnp.full((sub, LANES), -jnp.inf, f32)
        for c, column in enumerate(columns):
            if column is not None:
                spread_out = jnp.where(lane[:sub] == c, column, spread_out)
        pad = jnp.zeros((LANES - sub, LANES), f32)
        return jnp.transpose(jnp.concatenate([spread_out, pad], axis=0))[:8]

    def flat(x):
        return x.reshape(x.shape[0] * x.shape[1], x.shape[2])

    def far_head(h):
        receive(2, h)
        receive(1, h)
        out, lse = attend(
            flat(q_c[1:, h]), flat(kv_c[: n - 1, h, :, :hd]), flat(kv_c[: n - 1, h, :, hd:]), bias_far[...]
        )
        lsend[h] = as_rows([None] + [lse[b * sub : (b + 1) * sub] for b in range(n - 1)])
        rl[s, h] = lsend[h]
        oc[h, 1:] = out.astype(bf16).reshape(n - 1, sub, hd)
        for k in (3, 2, 1):
            @pl.when(peer[k] > 0)
            def _():
                sp_copy(lsend.at[h], rl.at[s, h], sent, lr.at[k - 1, h], peer[k]).start()
                sp_copy(oc.at[h, peer[k]], ro.at[s, h], sent, rr.at[k - 1, h], peer[k]).start()


    def y_copy(i):
        piece = wo.at[(xp, diag)[i // 2], quarter_of(i % 2)]
        return copy_to("grp", piece, piece, sent, wfr.at[i], 1 - g)

    def pass_step(i):
        later = (i + 3) % 4

        @pl.when(s > 0)
        def _():
            w_copies[later].wait_recv()
            y_copy(later).start()

        if i == 0:
            @pl.when(s == 1)
            def _():
                same(sp_copy, wo.at[diag, quarter_of(1)], wzr, s - 1).start()

        @pl.when(s == 0)
        def _():
            if i < 3:
                w_copies[i].wait_recv()
            else:
                same(sp_copy, wo.at[diag, quarter_of(1)], wzr, s + 1).wait_recv()
            y_copy(i).start()

    far_head(0)
    pass_step(0)
    for h in range(1, heads):
        far_head(h)
    pass_step(1)
    close(5, ((q_b, kv_b, mirror),), lambda: None)

    others = pl.ds(0, n - 1)

    def pair_of(piece, j, near_sem):
        return same(tp_copy, piece, gxr.at[j], xp), same(tp_copy, piece, near_sem, core)

    def index(k, h):
        return 1 + h * (n - 1) + k - 1

    shared = [pair_of(at_own.at[p], 0, gor)]
    for h in range(heads):
        for k in range(1, n):
            shared.append(pair_of(at.at[p, h, k - 1], index(k, h), gcr))

    def share(j):
        for copy in shared[j]:
            copy.start()

    for h in range(heads):
        out, lse = attend(flat(q_b[:, h]), flat(kv_b[:, h, :, :hd]), flat(kv_b[:, h, :, hd:]), bias_near[...])
        near_out[h] = out.reshape(n, sub, hd)
        near_row[h] = as_rows([lse[c * sub : (c + 1) * sub] for c in range(n)])

        @pl.when(s == 0)
        def _():
            at_own[p, h] = near_out[h, 0].astype(bf16)
            for c in range(1, n):
                at[p, h, c - 1] = near_out[h, c].astype(bf16)
            if h == heads - 1:
                share(0)
            for k in range(1, n):
                share(index(k, h))
            all_log[h] = near_row[h]

    pass_step(2)

    @pl.when(s > 0)
    def _():
        sp_copy(halo.at[pl.ds(0, n - 1)], halo.at[pl.ds(0, n - 1)], sent, hr, above).wait_recv()
        halo[s] = kv_c[s - 1, :, sub - halo_sub :, :]
        small = (halo_rows, halo_rows)
        behind = row_of(iota(small, 0), halo_sub) - row_of(iota(small, 1), halo_sub) + halo_rows
        bias_h = jnp.where(behind <= KEYS_BEHIND, 0.0, -jnp.inf).astype(f32)
        low = []
        pad = jnp.full((sub - halo_sub, 1), -jnp.inf, f32)
        for h in range(heads):
            out, lse = attend(
                flat(q_b[:, h, :halo_sub]), flat(halo[:, h, :, :hd]), flat(halo[:, h, :, hd:]), bias_h
            )
            halo_out[h] = out.reshape(n, halo_sub, hd)
            for c in range(n):
                low.append(jnp.concatenate([lse[c * halo_sub : (c + 1) * halo_sub], pad], axis=0))
        halo_row[...] = as_rows(low)

    which = iota((16, LANES), 0)

    def weigh(own, low, far_row):
        top = jnp.maximum(jnp.maximum(own, low), far_row)
        exps = [jnp.exp(x - top) for x in (own, low, far_row)]
        both = exps[0] + exps[1] + exps[2]
        return [x / both for x in exps], top + jnp.log(both)

    def as_columns(shares):
        pad = jnp.zeros((LANES - 16 * len(shares), LANES), f32)
        return jnp.transpose(jnp.concatenate(shares + [pad], axis=0))[:sub]

    def blend(parts, own, far_out, low):
        sums = parts[0] * own + parts[2] * far_out.astype(f32)
        return jnp.concatenate([sums[:halo_sub] + parts[1][:halo_sub] * low, sums[halo_sub:]], axis=0).astype(bf16)

    mine = pl.ds(s, 1)

    def merge(places):
        rows_of = jnp.zeros((16, LANES), f32)
        for i, (c, h) in enumerate(places):
            row = pl.ds(c, 1)
            shares, all_log[h, row] = weigh(near_row[h, row], halo_row[pl.ds(h * n + c, 1)], rl[c, h, mine])
            for j, x in enumerate(shares):
                rows_of = jnp.where(which == 3 * i + j, x, rows_of)
        columns = as_columns([rows_of])
        for i, (c, h) in enumerate(places):
            parts = [columns[:, 3 * i + j : 3 * i + j + 1] for j in range(3)]
            yield lambda far, c=c, h=h, parts=parts: blend(parts, near_out[h, c], far[...], halo_out[h, c])

    @pl.when(s > 0)
    def _():
        for h, mixed in enumerate(merge([(s, h) for h in range(heads)])):
            at_own[p, h] = mixed(oc.at[h, s])
        share(0)

    pass_step(3)

    @pl.when(s > 0)
    def _():
        for h in range(heads):
            for ks in ((1,), (2, 3)) if h < heads - 1 else ((1,), (2, 3)):
                for k in ks:
                    same(sp_copy, rl.at[peer[k], h], lr.at[k - 1, h], peer[k]).wait_recv()
                    same(sp_copy, ro.at[peer[k], h], rr.at[k - 1, h], peer[k]).wait_recv()
                for k, mixed in zip(ks, merge([(peer[k], h) for k in ks])):
                    at[p, h, k - 1] = mixed(ro.at[peer[k], h])
                for k in ks:
                    share(index(k, h))

    block = iota(square, 1) // sub
    class_of = jnp.where(block == 0, pair, jnp.where(block == 1, two, jnp.where(block == 2, mirror, s)))
    from_class = (iota(square, 0) == n * lax.rem(iota(square, 1), sub) + class_of).astype(f32).astype(bf16)

    def product(q):
        x = jnp.concatenate([
            jnp.concatenate([flat(at[q, h, : n - 1]), at_own[q, h]], axis=0) for h in range(heads)
        ], axis=1)
        return jnp.dot(x, wo[q], preferred_element_type=f32)

    def forward(j):
        shared[j][0].wait_recv()
        if j == 0:
            go(same(tp_copy, at_own.at[xp], gpr, core))
        else:
            go(same(tp_copy, at.at[xp, (j - 1) // (n - 1), (j - 1) % (n - 1)], gfr, core))

    by_head = iota((8, LANES), 0)
    logs = []
    for c in range(n):
        row = jnp.zeros((8, LANES), f32)
        for h in range(heads):
            row = jnp.where(by_head == h, all_log[h, c : c + 1, :], row)
        logs.append(row)
    logs = jnp.concatenate(logs, axis=1)
    placed = (n * LANES, rows)
    to_order = (
        (n * lax.rem(iota(placed, 0), LANES) + iota(placed, 0) // LANES == iota(placed, 1))
        & (lax.rem(iota(placed, 0), LANES) < sub)
    ).astype(f32).astype(bf16)
    high = logs.astype(bf16)
    rest = logs - high.astype(f32)
    middle = rest.astype(bf16)
    low = (rest - middle.astype(f32)).astype(bf16)
    total = sum(jnp.dot(x, to_order, preferred_element_type=f32) for x in (high, middle, low))
    total_ref[...] = total[:heads]

    result = product(p)
    for j in (*range(1, n), 0, *range(n, len(shared))):
        forward(j)
    w_core.wait_recv()
    same(tp_copy, at_own.at[core], gor, core).wait_recv()
    same(tp_copy, at.at[core, :, others], gcr, core).wait_recv()
    result += product(core)
    for i in range(4):
        y_copy(i).wait_recv()
    result += product(xp)
    same(tp_copy, at_own.at[diag], gpr, core).wait_recv()
    same(tp_copy, at.at[diag, :, others], gfr, core).wait_recv()
    result += product(diag)
    mixed_ref[...] = jnp.dot(from_class, result.astype(bf16), preferred_element_type=f32).astype(bf16)
    back = heads * (sub * hd * 2 + 8 * LANES * 4)
    q_bytes, kv_bytes = 2 * heads * sub * hd * 2, 2 * heads * sub * 2 * hd * 2
    halo_bytes = (n - 1) * heads * halo_sub * 2 * hd * 2
    at_bytes = 2 * rows * lw * 2
    w_bytes = quarter * width * 2

    def all_sent(total):
        same(tp_copy, drain.at[pl.ds(0, total // (LANES * 4))], acr, core).wait_send()

    always = sum(sends) + at_bytes + 4 * w_bytes + 2 * back

    @pl.when(s == 0)
    def _():
        all_sent(always + kv_bytes + halo_bytes + back)

    @pl.when(s == 1)
    def _():
        all_sent(always + q_bytes + kv_bytes + halo_bytes + 2 * w_bytes)

    @pl.when((s > 1) & (s < n - 1))
    def _():
        all_sent(always + q_bytes + kv_bytes + halo_bytes + w_bytes)

    @pl.when(s == n - 1)
    def _():
        all_sent(always + q_bytes + w_bytes)


def write_kernel(mixed_ref, total_ref, out_ref, log_ref, sems):
    copies = [
        pltpu.make_async_copy(mixed_ref, out_ref, sems.at[0]),
        pltpu.make_async_copy(total_ref, log_ref, sems.at[1]),
    ]
    for copy in copies:
        copy.start()
    for copy in copies:
        copy.wait()


def local_by_class(hidden, norm_gain, w_query, w_key, w_value, query_gain, key_gain, w_out):
    n = MIDDLE_DILATION
    rows, width = hidden.shape
    heads, hd = query_gain.shape
    lw = heads * hd
    sub = rows // n
    halo_sub = KEYS_BEHIND // n
    bf16, f32 = jnp.bfloat16, jnp.float32
    table = jnp.asarray(rotary_table(n, sub, hd))
    most_bytes = 2 * (16 * sub * width + 3 * lw * width + 30 * sub * lw) + 3 * heads * 8 * LANES * 4
    vmem = pl.BlockSpec(memory_space=pltpu.VMEM)
    anyspace = pl.BlockSpec(memory_space=pl.ANY)
    dma = pltpu.SemaphoreType.DMA
    mixed, total = pl.pallas_call(
        class_kernel,
        out_shape=(
            pltpu.VMEM((rows, w_out.shape[1] // 4), bf16),
            pltpu.VMEM((heads, rows), f32),
        ),
        in_specs=[anyspace] * 9,
        out_specs=(vmem, vmem),
        scratch_shapes=[
            pltpu.VMEM((rows, width), bf16),
            pltpu.VMEM((4 * width // LANES, LANES), bf16),
            pltpu.VMEM((heads, hd), f32),
            pltpu.VMEM((heads, hd), f32),
            pltpu.VMEM((4, n, sub, width), bf16),
            pltpu.VMEM((4, 2, sub // 2, width), bf16),
            pltpu.VMEM((4 * width, 3 * lw), bf16),
            pltpu.VMEM((4, lw, width), bf16),
            pltpu.VMEM((n, sub, 2 * hd), f32),
            pltpu.VMEM((sub, 2 * hd), f32),
            pltpu.VMEM((n, sub, 3 * lw), f32),
            pltpu.VMEM((sub, 3 * lw), f32),
            pltpu.VMEM((n, sub, 1), f32),
            pltpu.VMEM((n, heads, sub, hd), bf16),
            pltpu.VMEM((n, heads, sub, 2 * hd), bf16),
            pltpu.VMEM((n, heads, sub, hd), bf16),
            pltpu.VMEM((n, heads, sub, 2 * hd), bf16),
            pltpu.VMEM((n, heads, halo_sub, 2 * hd), bf16),
            pltpu.VMEM((heads, n, sub, hd), bf16),
            pltpu.VMEM((heads, 8, LANES), f32),
            pltpu.VMEM((n, heads, sub, hd), bf16),
            pltpu.VMEM((n, heads, 8, LANES), f32),
            pltpu.VMEM((heads, n, sub, hd), f32),
            pltpu.VMEM((heads, 8, LANES), f32),
            pltpu.VMEM((heads, n, halo_sub, hd), f32),
            pltpu.VMEM((8, LANES), f32),
            pltpu.VMEM((heads, 8, LANES), f32),
            pltpu.VMEM((4, heads, n, sub, hd), bf16),
            pltpu.VMEM((4, heads, sub, hd), bf16),
            pltpu.VMEM((rows - sub, rows - sub), f32),
            pltpu.VMEM((rows, rows), f32),
            pltpu.VMEM((4, 1, width), f32),
            pltpu.VMEM((most_bytes // (4 * LANES), LANES), f32),
            dma((10,)), dma, dma((2,)), dma((n + 2,)), dma, dma((n + 2,)), dma((2,)), dma, dma,
            dma((5,)), dma((4,)), dma, dma((2, heads, 2)), dma((2, heads, 2)), dma, dma((3, heads)), dma((3, heads)),
            dma((1 + 3 * heads,)), dma, dma, dma, dma,
        ],
        compiler_params=pltpu.CompilerParams(
            collective_id=0, has_side_effects=True, vmem_limit_bytes=60 * 1024 * 1024
        ),
    )(
        hidden, norm_gain.reshape(-1, LANES), query_gain, key_gain,
        w_query, w_key, w_value, w_out, table,
    )
    mixed, total = pl.pallas_call(
        write_kernel,
        out_shape=(
            jax.ShapeDtypeStruct(mixed.shape, bf16), jax.ShapeDtypeStruct(total.shape, f32)
        ),
        in_specs=[vmem, vmem],
        out_specs=(anyspace, anyspace),
        scratch_shapes=[dma((2,))],
    )(
        pltpu.with_memory_space_constraint(mixed, pltpu.VMEM),
        pltpu.with_memory_space_constraint(total, pltpu.VMEM),
    )
    return mixed, total.T


def solution(mesh):
    split = (mesh.shape["grp"], mesh.shape["sp"], mesh.shape["tp"]) == (2, MIDDLE_DILATION, 4)
    chosen = local_by_class if split else local
    placed = (
        P(("grp", "sp"), "tp"),
        P(),
        P(None, "tp"),
        P(None, "tp"),
        P(None, "tp"),
        P("tp", None),
        P("tp", None),
        P("tp", None),
    )
    return jax.shard_map(
        chosen,
        mesh=mesh,
        in_specs=placed,
        out_specs=(P(("grp", "sp"), "tp"), P(("grp", "sp"), "tp")),
        check_vma=False,
    )
```

```python
import functools
import math

import jax
import jax.numpy as jnp
import numpy as np
from jax import lax
from jax.experimental import pallas as pl
from jax.experimental.pallas import tpu as pltpu
from jax.sharding import PartitionSpec as P

D = 2048
KEYS_BEHIND = 128
MIDDLE_DILATION = 4
WIDEST_DILATION = 16


EPSILON = 1e-06
ROTARY_BASE = 500000.0


def from_behind(value, axis, steps):
    count = lax.axis_size(axis)
    initial, last = (max(0, -steps), min(count, count - steps))
    return lax.ppermute(value, axis, [(source, source + steps) for source in range(initial, last)])


def rotate(values, positions):
    head_width = values.shape[-1]
    inverse = ROTARY_BASE ** (-jnp.arange(0, head_width, 2, dtype=jnp.float32) / head_width)
    angles = positions[:, None] * inverse[None, :]
    cosine = jnp.cos(angles)[:, None, :]
    sine = jnp.sin(angles)[:, None, :]
    half_width = head_width // 2
    first_half = values[..., :half_width]
    second_half = values[..., half_width:]
    return jnp.concatenate(
        [first_half * cosine - second_half * sine, second_half * cosine + first_half * sine],
        axis=-1,
    )


def head_norm(values, gains):
    normed = values * lax.rsqrt(jnp.mean(values * values, axis=-1, keepdims=True) + EPSILON)
    return normed * gains[None, :, :]


def earlier_pairs(own_pair, token_rows):
    distant_shards = (KEYS_BEHIND * WIDEST_DILATION + token_rows - 1) // token_rows
    pieces = [own_pair]
    for distance in range(1, distant_shards + 1):
        pieces.insert(0, from_behind(own_pair, "sp", distance))
    buffer = jnp.concatenate(pieces, axis=1)
    return buffer


def local_branch(query, key_rows, value_rows, dilation_step, first_pos):
    token_rows, head_count, head_width = query.shape
    reach_rows = KEYS_BEHIND * dilation_step
    buffer_rows = key_rows.shape[0]
    class_rows = token_rows // dilation_step
    class_keys = class_rows + KEYS_BEHIND
    window_start = buffer_rows - token_rows - reach_rows
    key_window = key_rows[window_start:]
    value_window = value_rows[window_start:]
    query_class = query.reshape(class_rows, dilation_step, head_count, head_width).transpose(
        1, 0, 2, 3
    )
    key_class = key_window.reshape(class_keys, dilation_step, head_count, head_width).transpose(
        1, 0, 2, 3
    )
    value_class = value_window.reshape(class_keys, dilation_step, head_count, head_width).transpose(
        1, 0, 2, 3
    )
    block_rows = math.gcd(class_rows, KEYS_BEHIND) if class_rows > KEYS_BEHIND else class_rows
    block_count = class_rows // block_rows
    query_blocks = query_class.reshape(
        dilation_step, block_count, block_rows, head_count, head_width
    )
    key_blocks = jnp.stack(
        [
            key_class[:, number * block_rows : number * block_rows + block_rows + KEYS_BEHIND]
            for number in range(block_count)
        ],
        axis=1,
    )
    value_blocks = jnp.stack(
        [
            value_class[:, number * block_rows : number * block_rows + block_rows + KEYS_BEHIND]
            for number in range(block_count)
        ],
        axis=1,
    )
    scores = jnp.einsum(
        "rnqhd,rnkhd->rnhqk", query_blocks, key_blocks, preferred_element_type=jnp.float32
    ) * head_width ** (-0.5)
    row_index = jnp.arange(block_rows, dtype=jnp.int32)[:, None]
    col_index = jnp.arange(block_rows + KEYS_BEHIND, dtype=jnp.int32)[None, :]
    distance = KEYS_BEHIND + row_index - col_index
    in_band = (distance >= 0) & (distance <= KEYS_BEHIND)
    class_index = jnp.arange(block_count, dtype=jnp.int32)[:, None] * block_rows + col_index
    residue = jnp.arange(dilation_step, dtype=jnp.int32)[:, None, None]
    key_position = first_pos - reach_rows + class_index[None] * dilation_step + residue
    allowed = in_band[None, None, None, :, :] & (key_position >= 0)[:, :, None, None, :]
    scores = jnp.where(allowed, scores, -jnp.inf)
    row_max = jnp.max(scores, axis=-1, keepdims=True)
    weights = jnp.exp(scores - row_max)
    weight_sum = jnp.sum(weights, axis=-1)
    weighted = jnp.einsum(
        "rnhqk,rnkhd->rnqhd",
        weights.astype(jnp.bfloat16),
        value_blocks,
        preferred_element_type=jnp.float32,
    )
    branch_out = weighted / jnp.transpose(weight_sum, (0, 1, 3, 2))[..., None]
    branch_out = branch_out.reshape(dilation_step, class_rows, head_count, head_width).transpose(
        1, 0, 2, 3
    )
    branch_out = branch_out.reshape(token_rows, head_count, head_width)
    log_sum = jnp.transpose(row_max[..., 0] + jnp.log(weight_sum), (0, 1, 3, 2))
    log_sum = (
        log_sum.reshape(dilation_step, class_rows, head_count)
        .transpose(1, 0, 2)
        .reshape(token_rows, head_count)
    )
    return (branch_out, log_sum)


def local(hidden, norm_gain, w_query, w_key, w_value, query_gain, key_gain, w_out):
    token_rows = hidden.shape[0]
    local_width = w_query.shape[1]
    head_count = query_gain.shape[0]
    head_width = query_gain.shape[1]
    gain_full = norm_gain.astype(jnp.float32)
    raw_piece = lax.all_gather(hidden, "tp", axis=1, tiled=True).astype(jnp.float32)
    scaled = (raw_piece * gain_full[None, :]).astype(jnp.bfloat16)

    def add_product(weight):
        return jnp.dot(scaled, weight, preferred_element_type=jnp.float32)

    query_raw = add_product(w_query)
    key_raw = add_product(w_key)
    value_raw = add_product(w_value)
    squares = jnp.sum(raw_piece * raw_piece, axis=1)
    row_scale = lax.rsqrt(squares / D + EPSILON)[:, None]
    first_pos = lax.axis_index("sp") * token_rows
    positions = (jnp.arange(token_rows, dtype=jnp.int32) + first_pos).astype(jnp.float32)
    query = rotate(
        head_norm((query_raw * row_scale).reshape(token_rows, head_count, head_width), query_gain),
        positions,
    ).astype(jnp.bfloat16)
    key_now = rotate(
        head_norm((key_raw * row_scale).reshape(token_rows, head_count, head_width), key_gain),
        positions,
    ).astype(jnp.bfloat16)
    value_now = (value_raw * row_scale).astype(jnp.bfloat16)
    own_pair = jnp.stack([key_now.reshape(token_rows, local_width), value_now], axis=0)
    buffer = earlier_pairs(own_pair, token_rows)
    key_rows = buffer[0].reshape(-1, head_count, head_width)
    value_rows = buffer[1].reshape(-1, head_count, head_width)
    branch_outs = []
    branch_logs = []
    for dilation_step in (1, MIDDLE_DILATION, WIDEST_DILATION):
        branch_out, log_sum = local_branch(query, key_rows, value_rows, dilation_step, first_pos)
        branch_outs.append(branch_out)
        branch_logs.append(log_sum)
    stacked_logs = jnp.stack(branch_logs, axis=0)
    peak = jnp.max(stacked_logs, axis=0)
    log_total = peak + jnp.log(jnp.sum(jnp.exp(stacked_logs - peak[None]), axis=0))
    shares = jnp.exp(stacked_logs - log_total[None])
    attended = jnp.sum(shares[..., None] * jnp.stack(branch_outs, axis=0), axis=0)
    attended = attended.astype(jnp.bfloat16).reshape(token_rows, local_width)
    column_block = lax.all_to_all(w_out, "tp", split_axis=1, concat_axis=0, tiled=True)
    mixed = jnp.dot(
        lax.all_gather(attended, "tp", axis=1, tiled=True),
        column_block,
        preferred_element_type=jnp.float32,
    )
    return (mixed.astype(jnp.bfloat16), log_total)


MESH = pl.DeviceIdType.MESH
LANES = 128


def rotary_table(classes, rows, head_width):
    inverse = (ROTARY_BASE ** (-np.arange(0, head_width, 2, dtype=np.float64) / head_width)).astype(np.float32)
    positions = np.arange(classes * classes * rows, dtype=np.float32)
    angles = (positions[:, None] * inverse[None, :]).astype(np.float64)
    cosine, sine = np.cos(angles), np.sin(angles)
    table = np.concatenate([cosine, cosine, -sine, sine], axis=1).astype(np.float32)
    return table.reshape(classes, rows, classes, 2 * head_width).transpose(0, 2, 1, 3)


def class_kernel(
    hid_ref, gain_ref, qgain_ref, kgain_ref, wq_ref, wk_ref, wv_ref, wo_ref, table_ref,
    mixed_ref, total_ref,
    hid, gain_in, qgain, kgain, hb, hm, wall, wo, tb, tm, acc, acc_m, sq, q_b, kv_b, q_c, kv_c,
    halo, oc, lsend, ro, rl, near_out, near_row, halo_out, halo_row, all_log, at, at_own, bias_far, bias_near, gain, drain,
    loc, sent, zr, axr, acr, afr, cxr, ccr, cfr, wor, wfr, wzr, qr, kr, hr, rr, lr, gxr, gcr, gfr, gor, gpr,
):
    f32, bf16 = jnp.float32, jnp.bfloat16
    g, s, p = lax.axis_index("grp"), lax.axis_index("sp"), lax.axis_index("tp")
    n = MIDDLE_DILATION
    rows, width = hid_ref.shape
    sub = rows // n
    heads, hd = qgain_ref.shape
    lw = heads * hd
    halo_sub = halo.shape[2]
    halo_rows = n * halo_sub
    core = p + 1 - 2 * lax.rem(p, 2)
    xp = lax.rem(p + 2, 4)
    diag = lax.rem(core + 2, 4)
    pair, two, mirror = s + 1 - 2 * lax.rem(s, 2), lax.rem(s + 2, n), n - 1 - s
    peer = (s, pair, two, mirror)
    part = sub // 2
    pieces = (
        (two, 0, part), (two, part, part), (pair, 0, sub), (s, 0, sub), (mirror, sub - halo_sub, halo_sub), (mirror, 0, sub - halo_sub)
    )

    def copy_to(axis, src, dst, ss, sr, q):
        return pltpu.make_async_remote_copy(
            src_ref=src, dst_ref=dst, send_sem=ss, recv_sem=sr, device_id={axis: q}, device_id_type=MESH
        )

    tp_copy = functools.partial(copy_to, "tp")
    sp_copy = functools.partial(copy_to, "sp")

    def same(copy, ref, sr, q):
        return copy(ref, ref, sent, sr, q)

    load_hid = pltpu.make_async_copy(hid_ref, hid, loc.at[1])
    load_hid.start()
    barrier = pltpu.get_barrier_semaphore()
    for k in (3, 2, 1):
        pl.semaphore_signal(barrier, inc=1, device_id={"sp": peer[k]}, device_id_type=MESH)
    for q in (xp, diag, core):
        pl.semaphore_signal(barrier, inc=1, device_id={"tp": q}, device_id_type=MESH)
    pl.semaphore_signal(barrier, inc=1, device_id={"grp": 1 - g}, device_id_type=MESH)
    loads = [
        pltpu.make_async_copy(gain_ref, gain_in, loc.at[0]),
        pltpu.make_async_copy(qgain_ref, qgain, loc.at[2]),
        pltpu.make_async_copy(kgain_ref, kgain, loc.at[3]),
        pltpu.make_async_copy(wq_ref, wall.at[:, pl.ds(0, lw)], loc.at[4]),
        pltpu.make_async_copy(wk_ref, wall.at[:, pl.ds(lw, lw)], loc.at[5]),
        pltpu.make_async_copy(wv_ref, wall.at[:, pl.ds(2 * lw, lw)], loc.at[6]),
        pltpu.make_async_copy(table_ref.at[s], tb, loc.at[7]),
        pltpu.make_async_copy(table_ref.at[mirror, s], tm, loc.at[8]),
        pltpu.make_async_copy(
            wo_ref.at[:, pl.ds(pl.multiple_of(p * width, LANES), width)], wo.at[p], loc.at[9]
        ),
    ]
    for load in loads:
        load.start()

    def iota(shape, dim):
        return lax.broadcasted_iota(jnp.int32, shape, dim)

    def row_of(r, part):
        return n * lax.rem(r, part) + r // part

    square = (rows, rows)
    to_class = (row_of(iota(square, 0), sub) == iota(square, 1)).astype(f32).astype(bf16)
    load_hid.wait()
    permuted = jnp.dot(to_class, hid[...], preferred_element_type=f32).astype(bf16)
    hb[p] = permuted.reshape(n, sub, width)
    pl.semaphore_wait(barrier, 3 + n)

    sends = []

    def go(copy):
        copy.start()
        sends.append(math.prod(copy.src_ref.shape) * copy.src_ref.dtype.itemsize)
        return copy

    zs = [
        go(sp_copy(hb.at[p, mirror, pl.ds(a * part, part), :], hm.at[p, a], sent, zr.at[a], mirror))
        for a in range(2)
    ]
    ax = [same(tp_copy, hb.at[p, c, pl.ds(i, m), :], axr.at[j], xp) for j, (c, i, m) in enumerate(pieces)]
    for copy in ax[:5]:
        go(copy)
    ac = go(same(tp_copy, hb.at[p], acr, core))
    w_core = go(tp_copy(
        wo_ref.at[:, pl.ds(pl.multiple_of(core * width, LANES), width)],
        wo.at[p], sent, wor.at[0], core,
    ))

    for load in loads:
        load.wait()
    flat_gain = gain_in[...].astype(f32)
    for j in range(flat_gain.shape[0]):
        each = width // LANES
        gain[j // each, :, (j % each) * LANES : (j % each + 1) * LANES] = flat_gain[j : j + 1]

    def chunk(raw, q):
        raw = raw.astype(f32)
        scaled = (raw * gain[q]).astype(bf16)
        w = wall[pl.ds(pl.multiple_of(q * width, LANES), width), :]
        return jnp.dot(scaled, w, preferred_element_type=f32), jnp.sum(raw * raw, axis=1, keepdims=True)

    def add_all(q, first):
        prod, more = chunk(hb[q].reshape(rows, width), q)
        prod, more = prod.reshape(n, sub, 3 * lw), more.reshape(n, sub, 1)
        acc[...] = prod if first else acc[...] + prod
        sq[...] = more if first else sq[...] + more

    add_all(p, True)
    ac.wait_recv()
    add_all(core, False)

    def finish(acc, sq, table, places, span):
        raw = acc * lax.rsqrt(sq / (width * 4) + EPSILON)
        cosine, sine = table[:, :hd], table[:, hd:]
        for h in range(heads):
            for j, gains in enumerate((qgain, kgain, None)):
                x = raw[:, j * lw + h * hd : j * lw + (h + 1) * hd]
                if gains is not None:
                    x = x * lax.rsqrt(jnp.mean(x * x, axis=-1, keepdims=True) + EPSILON)
                    x = x * gains[pl.ds(h, 1), :]
                    x = x * cosine + pltpu.roll(x, hd // 2, 1) * sine
                for q_ref, kv_ref, c in places:
                    if j == 0:
                        q_ref[c, h, span] = x.astype(bf16)
                    else:
                        kv_ref[c, h, span, (j - 1) * hd : j * hd] = x.astype(bf16)

    def take(j):
        c, i, m = pieces[j]
        ax[j].wait_recv()
        go(same(tp_copy, hb.at[xp, c, pl.ds(i, m), :], afr.at[j], core))

    def close(j, places, between):
        c, i, m = pieces[j]
        span = slice(i, i + m)
        prod, more = chunk(hb[xp, c, span], xp)
        between()
        same(tp_copy, hb.at[diag, c, pl.ds(i, m), :], afr.at[j], core).wait_recv()
        last, most = chunk(hb[diag, c, span], diag)
        finish(acc[c, span] + prod + last, sq[c, span] + more + most, tb[c, span], places, span)

    cx, cc = {}, {}

    def spread(a):
        zs[a].wait_recv()
        cx[a] = go(same(tp_copy, hm.at[p, a], cxr.at[a], xp))
        cc[a] = go(same(tp_copy, hm.at[p, a], ccr, core))

    def cross(a):
        cx[a].wait_recv()
        go(same(tp_copy, hm.at[xp, a], cfr, core))

    parts_of = {1: pieces[2:3], 2: pieces[:2]}

    def class_copy(own, other, sems, k, h, j, arriving):
        _, i, m = parts_of[k][j]
        q = peer[k]
        mine = other.at[q, h, pl.ds(i, m), :]
        if arriving:
            return same(sp_copy, mine, sems.at[k - 1, h, j], q)
        return sp_copy(own.at[q, h, pl.ds(i, m), :], other.at[s, h, pl.ds(i, m), :], sent, sems.at[k - 1, h, j], q)

    kv_copy = functools.partial(class_copy, kv_b, kv_c, kr)
    q_copy = functools.partial(class_copy, q_b, q_c, qr)

    def give(k, j):
        for h in range(heads):
            @pl.when(s < n - 1)
            def _():
                kv_copy(k, h, j, False).start()

            @pl.when(s > 0)
            def _():
                q_copy(k, h, j, False).start()

    def receive(k, h):
        @pl.when(peer[k] < n - 1)
        def _():
            for j in range(len(parts_of[k])):
                kv_copy(k, h, j, True).wait_recv()

        @pl.when(peer[k] > 0)
        def _():
            for j in range(len(parts_of[k])):
                q_copy(k, h, j, True).wait_recv()

    quarter = lw // 4

    def quarter_of(a):
        return pl.ds(pl.multiple_of((2 * g + a) * quarter, 8), quarter)

    def w_copy(i):
        q, block = (xp, diag)[i // 2], quarter_of(i % 2)
        source = wo_ref.at[block, pl.ds(pl.multiple_of(q * width, LANES), width)]
        return tp_copy(source, wo.at[p, block], sent, wor.at[1 + i], q)

    w_copies = [w_copy(i) for i in range(4)]

    def spread_first():
        spread(0)

    def spread_last():
        spread(1)
        go(ax[5])
        @pl.when(s > 0)
        def _():
            w_copies[3].start()

        for copy in w_copies[:3]:
            go(copy)

    def add_mirror(q):
        prod, more = chunk(hm[q].reshape(sub, width), q)
        return prod, more

    squares = []

    def start_mirror():
        same(tp_copy, hm.at[core], ccr, core).wait_recv()
        first, one = add_mirror(p)
        prod, more = add_mirror(core)
        acc_m[...] = first + prod
        squares.append(one + more)
        cross(0)

    def log_count(*read):
        count = sum(each.astype(f32) for each in read)
        bias = jnp.where(count == 2, math.log(2.0), jnp.where(count == 3, math.log(3.0), 0.0))
        return jnp.where(count == 0, -jnp.inf, bias)

    def strided(behind, step):
        return (behind >= 0) & (behind <= KEYS_BEHIND * step) & ((behind + rows * step) % step == 0)

    later = (rows - sub, rows - sub)
    late, early = iota(later, 0) + sub, iota(later, 1)
    stride = WIDEST_DILATION // n
    crosses = late // sub > early // sub
    bias_far[...] = log_count(strided(late - early, 1) & crosses, strided(late - early, stride) & crosses)
    behind = row_of(iota(square, 0), sub) - row_of(iota(square, 1), sub)
    bias_near[...] = log_count(*(strided(behind, step) for step in (1, n, WIDEST_DILATION)))
    take(0)
    close(0, ((q_b, kv_b, two),), lambda: None)
    give(2, 0)
    take(1)
    close(1, ((q_b, kv_b, two),), spread_first)
    give(2, 1)
    above = lax.rem(s + 1, n)

    def send_halo(c):
        sp_copy(kv_b.at[c, :, pl.ds(sub - halo_sub, halo_sub), :], halo.at[c], sent, hr, above).start()

    @pl.when(s < n - 1)
    def _():
        send_halo(two)

    take(2)
    close(2, ((q_b, kv_b, pair),), spread_last)
    give(1, 0)
    @pl.when(s == 1)
    def _():
        send_halo(pair)

    take(3)
    close(3, ((q_b, kv_b, s), (q_c, kv_c, s)), start_mirror)

    take(4)

    @pl.when(s < n - 1)
    def _():
        send_halo(s)

    close(4, ((q_b, kv_b, mirror),), lambda: None)

    @pl.when((s < n - 1) & (s != 1))
    def _():
        send_halo(mirror)

    cross(1)
    prod, more = add_mirror(xp)
    take(5)
    same(tp_copy, hm.at[diag], cfr, core).wait_recv()
    last, most = add_mirror(diag)
    finish(acc_m[...] + prod + last, squares[0] + more + most, tm[...], ((q_c, kv_c, mirror),), slice(0, sub))

    def attend(q, k, v, bias):
        score = lax.dot_general(q, k, (((1,), (1,)), ((), ())), preferred_element_type=f32)
        score = score * hd ** (-0.5) + bias
        top = jnp.max(score, axis=-1, keepdims=True)
        weight = jnp.exp(score - top)
        total = jnp.sum(weight, axis=-1, keepdims=True)
        out = jnp.dot(weight.astype(bf16), v, preferred_element_type=f32) / total
        return out, top + jnp.log(total)

    lane = iota((rows, LANES), 1)

    def as_rows(columns):
        spread_out = jnp.full((sub, LANES), -jnp.inf, f32)
        for c, column in enumerate(columns):
            if column is not None:
                spread_out = jnp.where(lane[:sub] == c, column, spread_out)
        pad = jnp.zeros((LANES - sub, LANES), f32)
        return jnp.transpose(jnp.concatenate([spread_out, pad], axis=0))[:8]

    def flat(x):
        return x.reshape(x.shape[0] * x.shape[1], x.shape[2])

    def far_head(h):
        receive(2, h)
        receive(1, h)
        out, lse = attend(
            flat(q_c[1:, h]), flat(kv_c[: n - 1, h, :, :hd]), flat(kv_c[: n - 1, h, :, hd:]), bias_far[...]
        )
        lsend[h] = as_rows([None] + [lse[b * sub : (b + 1) * sub] for b in range(n - 1)])
        rl[s, h] = lsend[h]
        oc[h, 1:] = out.astype(bf16).reshape(n - 1, sub, hd)
        for k in (3, 2, 1):
            @pl.when(peer[k] > 0)
            def _():
                sp_copy(lsend.at[h], rl.at[s, h], sent, lr.at[k - 1, h], peer[k]).start()
                sp_copy(oc.at[h, peer[k]], ro.at[s, h], sent, rr.at[k - 1, h], peer[k]).start()


    def y_copy(i):
        piece = wo.at[(xp, diag)[i // 2], quarter_of(i % 2)]
        return copy_to("grp", piece, piece, sent, wfr.at[i], 1 - g)

    def pass_step(i):
        later = (i + 3) % 4

        @pl.when(s > 0)
        def _():
            w_copies[later].wait_recv()
            y_copy(later).start()

        if i == 0:
            @pl.when(s == 1)
            def _():
                same(sp_copy, wo.at[diag, quarter_of(1)], wzr, s - 1).start()

        @pl.when(s == 0)
        def _():
            if i < 3:
                w_copies[i].wait_recv()
            else:
                same(sp_copy, wo.at[diag, quarter_of(1)], wzr, s + 1).wait_recv()
            y_copy(i).start()

    far_head(0)
    pass_step(0)
    for h in range(1, heads):
        far_head(h)
    pass_step(1)
    close(5, ((q_b, kv_b, mirror),), lambda: None)

    others = pl.ds(0, n - 1)

    def pair_of(piece, j, near_sem):
        return same(tp_copy, piece, gxr.at[j], xp), same(tp_copy, piece, near_sem, core)

    def index(k, h):
        return 1 + h * (n - 1) + k - 1

    shared = [pair_of(at_own.at[p], 0, gor)]
    for h in range(heads):
        for k in range(1, n):
            shared.append(pair_of(at.at[p, h, k - 1], index(k, h), gcr))

    def share(j):
        for copy in shared[j]:
            copy.start()

    for h in range(heads):
        out, lse = attend(flat(q_b[:, h]), flat(kv_b[:, h, :, :hd]), flat(kv_b[:, h, :, hd:]), bias_near[...])
        near_out[h] = out.reshape(n, sub, hd)
        near_row[h] = as_rows([lse[c * sub : (c + 1) * sub] for c in range(n)])

        @pl.when(s == 0)
        def _():
            at_own[p, h] = near_out[h, 0].astype(bf16)
            for c in range(1, n):
                at[p, h, c - 1] = near_out[h, c].astype(bf16)
            if h == heads - 1:
                share(0)
            for k in range(1, n):
                share(index(k, h))
            all_log[h] = near_row[h]

    pass_step(2)

    @pl.when(s > 0)
    def _():
        sp_copy(halo.at[pl.ds(0, n - 1)], halo.at[pl.ds(0, n - 1)], sent, hr, above).wait_recv()
        halo[s] = kv_c[s - 1, :, sub - halo_sub :, :]
        small = (halo_rows, halo_rows)
        behind = row_of(iota(small, 0), halo_sub) - row_of(iota(small, 1), halo_sub) + halo_rows
        bias_h = jnp.where(behind <= KEYS_BEHIND, 0.0, -jnp.inf).astype(f32)
        low = []
        pad = jnp.full((sub - halo_sub, 1), -jnp.inf, f32)
        for h in range(heads):
            out, lse = attend(
                flat(q_b[:, h, :halo_sub]), flat(halo[:, h, :, :hd]), flat(halo[:, h, :, hd:]), bias_h
            )
            halo_out[h] = out.reshape(n, halo_sub, hd)
            for c in range(n):
                low.append(jnp.concatenate([lse[c * halo_sub : (c + 1) * halo_sub], pad], axis=0))
        halo_row[...] = as_rows(low)

    which = iota((16, LANES), 0)

    def weigh(own, low, far_row):
        top = jnp.maximum(jnp.maximum(own, low), far_row)
        exps = [jnp.exp(x - top) for x in (own, low, far_row)]
        both = exps[0] + exps[1] + exps[2]
        return [x / both for x in exps], top + jnp.log(both)

    def as_columns(shares):
        pad = jnp.zeros((LANES - 16 * len(shares), LANES), f32)
        return jnp.transpose(jnp.concatenate(shares + [pad], axis=0))[:sub]

    def blend(parts, own, far_out, low):
        sums = parts[0] * own + parts[2] * far_out.astype(f32)
        return jnp.concatenate([sums[:halo_sub] + parts[1][:halo_sub] * low, sums[halo_sub:]], axis=0).astype(bf16)

    mine = pl.ds(s, 1)

    def merge(places):
        rows_of = jnp.zeros((16, LANES), f32)
        for i, (c, h) in enumerate(places):
            row = pl.ds(c, 1)
            shares, all_log[h, row] = weigh(near_row[h, row], halo_row[pl.ds(h * n + c, 1)], rl[c, h, mine])
            for j, x in enumerate(shares):
                rows_of = jnp.where(which == 3 * i + j, x, rows_of)
        columns = as_columns([rows_of])
        for i, (c, h) in enumerate(places):
            parts = [columns[:, 3 * i + j : 3 * i + j + 1] for j in range(3)]
            yield lambda far, c=c, h=h, parts=parts: blend(parts, near_out[h, c], far[...], halo_out[h, c])

    @pl.when(s > 0)
    def _():
        for h, mixed in enumerate(merge([(s, h) for h in range(heads)])):
            at_own[p, h] = mixed(oc.at[h, s])
        share(0)

    pass_step(3)

    @pl.when(s > 0)
    def _():
        for h in range(heads):
            for ks in ((1,), (2, 3)) if h < heads - 1 else ((1,), (2, 3)):
                for k in ks:
                    same(sp_copy, rl.at[peer[k], h], lr.at[k - 1, h], peer[k]).wait_recv()
                    same(sp_copy, ro.at[peer[k], h], rr.at[k - 1, h], peer[k]).wait_recv()
                for k, mixed in zip(ks, merge([(peer[k], h) for k in ks])):
                    at[p, h, k - 1] = mixed(ro.at[peer[k], h])
                for k in ks:
                    share(index(k, h))

    block = iota(square, 1) // sub
    class_of = jnp.where(block == 0, pair, jnp.where(block == 1, two, jnp.where(block == 2, mirror, s)))
    from_class = (iota(square, 0) == n * lax.rem(iota(square, 1), sub) + class_of).astype(f32).astype(bf16)

    def product(q):
        x = jnp.concatenate([
            jnp.concatenate([flat(at[q, h, : n - 1]), at_own[q, h]], axis=0) for h in range(heads)
        ], axis=1)
        return jnp.dot(x, wo[q], preferred_element_type=f32)

    def forward(j):
        shared[j][0].wait_recv()
        if j == 0:
            go(same(tp_copy, at_own.at[xp], gpr, core))
        else:
            go(same(tp_copy, at.at[xp, (j - 1) // (n - 1), (j - 1) % (n - 1)], gfr, core))

    by_head = iota((8, LANES), 0)
    logs = []
    for c in range(n):
        row = jnp.zeros((8, LANES), f32)
        for h in range(heads):
            row = jnp.where(by_head == h, all_log[h, c : c + 1, :], row)
        logs.append(row)
    logs = jnp.concatenate(logs, axis=1)
    placed = (n * LANES, rows)
    to_order = (
        (n * lax.rem(iota(placed, 0), LANES) + iota(placed, 0) // LANES == iota(placed, 1))
        & (lax.rem(iota(placed, 0), LANES) < sub)
    ).astype(f32).astype(bf16)
    high = logs.astype(bf16)
    rest = logs - high.astype(f32)
    middle = rest.astype(bf16)
    low = (rest - middle.astype(f32)).astype(bf16)
    total = sum(jnp.dot(x, to_order, preferred_element_type=f32) for x in (high, middle, low))
    total_ref[...] = total[:heads]

    result = product(p)
    for j in (*range(1, n), 0, *range(n, len(shared))):
        forward(j)
    w_core.wait_recv()
    same(tp_copy, at_own.at[core], gor, core).wait_recv()
    same(tp_copy, at.at[core, :, others], gcr, core).wait_recv()
    result += product(core)
    for i in range(4):
        y_copy(i).wait_recv()
    result += product(xp)
    same(tp_copy, at_own.at[diag], gpr, core).wait_recv()
    same(tp_copy, at.at[diag, :, others], gfr, core).wait_recv()
    result += product(diag)
    mixed_ref[...] = jnp.dot(from_class, result.astype(bf16), preferred_element_type=f32).astype(bf16)
    back = heads * (sub * hd * 2 + 8 * LANES * 4)
    q_bytes, kv_bytes = 2 * heads * sub * hd * 2, 2 * heads * sub * 2 * hd * 2
    halo_bytes = (n - 1) * heads * halo_sub * 2 * hd * 2
    at_bytes = 2 * rows * lw * 2
    w_bytes = quarter * width * 2

    def all_sent(total):
        same(tp_copy, drain.at[pl.ds(0, total // (LANES * 4))], acr, core).wait_send()

    always = sum(sends) + at_bytes + 4 * w_bytes + 2 * back

    @pl.when(s == 0)
    def _():
        all_sent(always + kv_bytes + halo_bytes + back)

    @pl.when(s == 1)
    def _():
        all_sent(always + q_bytes + kv_bytes + halo_bytes + 2 * w_bytes)

    @pl.when((s > 1) & (s < n - 1))
    def _():
        all_sent(always + q_bytes + kv_bytes + halo_bytes + w_bytes)

    @pl.when(s == n - 1)
    def _():
        all_sent(always + q_bytes + w_bytes)


def write_kernel(mixed_ref, total_ref, out_ref, log_ref, sems):
    copies = [
        pltpu.make_async_copy(mixed_ref, out_ref, sems.at[0]),
        pltpu.make_async_copy(total_ref, log_ref, sems.at[1]),
    ]
    for copy in copies:
        copy.start()
    for copy in copies:
        copy.wait()


def local_by_class(hidden, norm_gain, w_query, w_key, w_value, query_gain, key_gain, w_out):
    n = MIDDLE_DILATION
    rows, width = hidden.shape
    heads, hd = query_gain.shape
    lw = heads * hd
    sub = rows // n
    halo_sub = KEYS_BEHIND // n
    bf16, f32 = jnp.bfloat16, jnp.float32
    table = jnp.asarray(rotary_table(n, sub, hd))
    most_bytes = 2 * (16 * sub * width + 3 * lw * width + 30 * sub * lw) + 3 * heads * 8 * LANES * 4
    vmem = pl.BlockSpec(memory_space=pltpu.VMEM)
    anyspace = pl.BlockSpec(memory_space=pl.ANY)
    dma = pltpu.SemaphoreType.DMA
    mixed, total = pl.pallas_call(
        class_kernel,
        out_shape=(
            pltpu.VMEM((rows, w_out.shape[1] // 4), bf16),
            pltpu.VMEM((heads, rows), f32),
        ),
        in_specs=[anyspace] * 9,
        out_specs=(vmem, vmem),
        scratch_shapes=[
            pltpu.VMEM((rows, width), bf16),
            pltpu.VMEM((4 * width // LANES, LANES), bf16),
            pltpu.VMEM((heads, hd), f32),
            pltpu.VMEM((heads, hd), f32),
            pltpu.VMEM((4, n, sub, width), bf16),
            pltpu.VMEM((4, 2, sub // 2, width), bf16),
            pltpu.VMEM((4 * width, 3 * lw), bf16),
            pltpu.VMEM((4, lw, width), bf16),
            pltpu.VMEM((n, sub, 2 * hd), f32),
            pltpu.VMEM((sub, 2 * hd), f32),
            pltpu.VMEM((n, sub, 3 * lw), f32),
            pltpu.VMEM((sub, 3 * lw), f32),
            pltpu.VMEM((n, sub, 1), f32),
            pltpu.VMEM((n, heads, sub, hd), bf16),
            pltpu.VMEM((n, heads, sub, 2 * hd), bf16),
            pltpu.VMEM((n, heads, sub, hd), bf16),
            pltpu.VMEM((n, heads, sub, 2 * hd), bf16),
            pltpu.VMEM((n, heads, halo_sub, 2 * hd), bf16),
            pltpu.VMEM((heads, n, sub, hd), bf16),
            pltpu.VMEM((heads, 8, LANES), f32),
            pltpu.VMEM((n, heads, sub, hd), bf16),
            pltpu.VMEM((n, heads, 8, LANES), f32),
            pltpu.VMEM((heads, n, sub, hd), f32),
            pltpu.VMEM((heads, 8, LANES), f32),
            pltpu.VMEM((heads, n, halo_sub, hd), f32),
            pltpu.VMEM((8, LANES), f32),
            pltpu.VMEM((heads, 8, LANES), f32),
            pltpu.VMEM((4, heads, n, sub, hd), bf16),
            pltpu.VMEM((4, heads, sub, hd), bf16),
            pltpu.VMEM((rows - sub, rows - sub), f32),
            pltpu.VMEM((rows, rows), f32),
            pltpu.VMEM((4, 1, width), f32),
            pltpu.VMEM((most_bytes // (4 * LANES), LANES), f32),
            dma((10,)), dma, dma((2,)), dma((n + 2,)), dma, dma((n + 2,)), dma((2,)), dma, dma,
            dma((5,)), dma((4,)), dma, dma((2, heads, 2)), dma((2, heads, 2)), dma, dma((3, heads)), dma((3, heads)),
            dma((1 + 3 * heads,)), dma, dma, dma, dma,
        ],
        compiler_params=pltpu.CompilerParams(
            collective_id=0, has_side_effects=True, vmem_limit_bytes=60 * 1024 * 1024
        ),
    )(
        hidden, norm_gain.reshape(-1, LANES), query_gain, key_gain,
        w_query, w_key, w_value, w_out, table,
    )
    mixed, total = pl.pallas_call(
        write_kernel,
        out_shape=(
            jax.ShapeDtypeStruct(mixed.shape, bf16), jax.ShapeDtypeStruct(total.shape, f32)
        ),
        in_specs=[vmem, vmem],
        out_specs=(anyspace, anyspace),
        scratch_shapes=[dma((2,))],
    )(
        pltpu.with_memory_space_constraint(mixed, pltpu.VMEM),
        pltpu.with_memory_space_constraint(total, pltpu.VMEM),
    )
    return mixed, total.T


def solution(mesh):
    split = (mesh.shape["grp"], mesh.shape["sp"], mesh.shape["tp"]) == (2, MIDDLE_DILATION, 4)
    chosen = local_by_class if split else local
    placed = (
        P(("grp", "sp"), "tp"),
        P(),
        P(None, "tp"),
        P(None, "tp"),
        P(None, "tp"),
        P("tp", None),
        P("tp", None),
        P("tp", None),
    )
    return jax.shard_map(
        chosen,
        mesh=mesh,
        in_specs=placed,
        out_specs=(P(("grp", "sp"), "tp"), P(("grp", "sp"), "tp")),
        check_vma=False,
    )
```

```python
import functools
import math

import jax
import jax.numpy as jnp
import numpy as np
from jax import lax
from jax.experimental import pallas as pl
from jax.experimental.pallas import tpu as pltpu
from jax.sharding import PartitionSpec as P

D = 2048
KEYS_BEHIND = 128
MIDDLE_DILATION = 4
WIDEST_DILATION = 16


EPSILON = 1e-06
ROTARY_BASE = 500000.0


def from_behind(value, axis, steps):
    count = lax.axis_size(axis)
    initial, last = (max(0, -steps), min(count, count - steps))
    return lax.ppermute(value, axis, [(source, source + steps) for source in range(initial, last)])


def rotate(values, positions):
    head_width = values.shape[-1]
    inverse = ROTARY_BASE ** (-jnp.arange(0, head_width, 2, dtype=jnp.float32) / head_width)
    angles = positions[:, None] * inverse[None, :]
    cosine = jnp.cos(angles)[:, None, :]
    sine = jnp.sin(angles)[:, None, :]
    half_width = head_width // 2
    first_half = values[..., :half_width]
    second_half = values[..., half_width:]
    return jnp.concatenate(
        [first_half * cosine - second_half * sine, second_half * cosine + first_half * sine],
        axis=-1,
    )


def head_norm(values, gains):
    normed = values * lax.rsqrt(jnp.mean(values * values, axis=-1, keepdims=True) + EPSILON)
    return normed * gains[None, :, :]


def earlier_pairs(own_pair, token_rows):
    distant_shards = (KEYS_BEHIND * WIDEST_DILATION + token_rows - 1) // token_rows
    pieces = [own_pair]
    for distance in range(1, distant_shards + 1):
        pieces.insert(0, from_behind(own_pair, "sp", distance))
    buffer = jnp.concatenate(pieces, axis=1)
    return buffer


def local_branch(query, key_rows, value_rows, dilation_step, first_pos):
    token_rows, head_count, head_width = query.shape
    reach_rows = KEYS_BEHIND * dilation_step
    buffer_rows = key_rows.shape[0]
    class_rows = token_rows // dilation_step
    class_keys = class_rows + KEYS_BEHIND
    window_start = buffer_rows - token_rows - reach_rows
    key_window = key_rows[window_start:]
    value_window = value_rows[window_start:]
    query_class = query.reshape(class_rows, dilation_step, head_count, head_width).transpose(
        1, 0, 2, 3
    )
    key_class = key_window.reshape(class_keys, dilation_step, head_count, head_width).transpose(
        1, 0, 2, 3
    )
    value_class = value_window.reshape(class_keys, dilation_step, head_count, head_width).transpose(
        1, 0, 2, 3
    )
    block_rows = math.gcd(class_rows, KEYS_BEHIND) if class_rows > KEYS_BEHIND else class_rows
    block_count = class_rows // block_rows
    query_blocks = query_class.reshape(
        dilation_step, block_count, block_rows, head_count, head_width
    )
    key_blocks = jnp.stack(
        [
            key_class[:, number * block_rows : number * block_rows + block_rows + KEYS_BEHIND]
            for number in range(block_count)
        ],
        axis=1,
    )
    value_blocks = jnp.stack(
        [
            value_class[:, number * block_rows : number * block_rows + block_rows + KEYS_BEHIND]
            for number in range(block_count)
        ],
        axis=1,
    )
    scores = jnp.einsum(
        "rnqhd,rnkhd->rnhqk", query_blocks, key_blocks, preferred_element_type=jnp.float32
    ) * head_width ** (-0.5)
    row_index = jnp.arange(block_rows, dtype=jnp.int32)[:, None]
    col_index = jnp.arange(block_rows + KEYS_BEHIND, dtype=jnp.int32)[None, :]
    distance = KEYS_BEHIND + row_index - col_index
    in_band = (distance >= 0) & (distance <= KEYS_BEHIND)
    class_index = jnp.arange(block_count, dtype=jnp.int32)[:, None] * block_rows + col_index
    residue = jnp.arange(dilation_step, dtype=jnp.int32)[:, None, None]
    key_position = first_pos - reach_rows + class_index[None] * dilation_step + residue
    allowed = in_band[None, None, None, :, :] & (key_position >= 0)[:, :, None, None, :]
    scores = jnp.where(allowed, scores, -jnp.inf)
    row_max = jnp.max(scores, axis=-1, keepdims=True)
    weights = jnp.exp(scores - row_max)
    weight_sum = jnp.sum(weights, axis=-1)
    weighted = jnp.einsum(
        "rnhqk,rnkhd->rnqhd",
        weights.astype(jnp.bfloat16),
        value_blocks,
        preferred_element_type=jnp.float32,
    )
    branch_out = weighted / jnp.transpose(weight_sum, (0, 1, 3, 2))[..., None]
    branch_out = branch_out.reshape(dilation_step, class_rows, head_count, head_width).transpose(
        1, 0, 2, 3
    )
    branch_out = branch_out.reshape(token_rows, head_count, head_width)
    log_sum = jnp.transpose(row_max[..., 0] + jnp.log(weight_sum), (0, 1, 3, 2))
    log_sum = (
        log_sum.reshape(dilation_step, class_rows, head_count)
        .transpose(1, 0, 2)
        .reshape(token_rows, head_count)
    )
    return (branch_out, log_sum)


def local(hidden, norm_gain, w_query, w_key, w_value, query_gain, key_gain, w_out):
    token_rows = hidden.shape[0]
    local_width = w_query.shape[1]
    head_count = query_gain.shape[0]
    head_width = query_gain.shape[1]
    gain_full = norm_gain.astype(jnp.float32)
    raw_piece = lax.all_gather(hidden, "tp", axis=1, tiled=True).astype(jnp.float32)
    scaled = (raw_piece * gain_full[None, :]).astype(jnp.bfloat16)

    def add_product(weight):
        return jnp.dot(scaled, weight, preferred_element_type=jnp.float32)

    query_raw = add_product(w_query)
    key_raw = add_product(w_key)
    value_raw = add_product(w_value)
    squares = jnp.sum(raw_piece * raw_piece, axis=1)
    row_scale = lax.rsqrt(squares / D + EPSILON)[:, None]
    first_pos = lax.axis_index("sp") * token_rows
    positions = (jnp.arange(token_rows, dtype=jnp.int32) + first_pos).astype(jnp.float32)
    query = rotate(
        head_norm((query_raw * row_scale).reshape(token_rows, head_count, head_width), query_gain),
        positions,
    ).astype(jnp.bfloat16)
    key_now = rotate(
        head_norm((key_raw * row_scale).reshape(token_rows, head_count, head_width), key_gain),
        positions,
    ).astype(jnp.bfloat16)
    value_now = (value_raw * row_scale).astype(jnp.bfloat16)
    own_pair = jnp.stack([key_now.reshape(token_rows, local_width), value_now], axis=0)
    buffer = earlier_pairs(own_pair, token_rows)
    key_rows = buffer[0].reshape(-1, head_count, head_width)
    value_rows = buffer[1].reshape(-1, head_count, head_width)
    branch_outs = []
    branch_logs = []
    for dilation_step in (1, MIDDLE_DILATION, WIDEST_DILATION):
        branch_out, log_sum = local_branch(query, key_rows, value_rows, dilation_step, first_pos)
        branch_outs.append(branch_out)
        branch_logs.append(log_sum)
    stacked_logs = jnp.stack(branch_logs, axis=0)
    peak = jnp.max(stacked_logs, axis=0)
    log_total = peak + jnp.log(jnp.sum(jnp.exp(stacked_logs - peak[None]), axis=0))
    shares = jnp.exp(stacked_logs - log_total[None])
    attended = jnp.sum(shares[..., None] * jnp.stack(branch_outs, axis=0), axis=0)
    attended = attended.astype(jnp.bfloat16).reshape(token_rows, local_width)
    column_block = lax.all_to_all(w_out, "tp", split_axis=1, concat_axis=0, tiled=True)
    mixed = jnp.dot(
        lax.all_gather(attended, "tp", axis=1, tiled=True),
        column_block,
        preferred_element_type=jnp.float32,
    )
    return (mixed.astype(jnp.bfloat16), log_total)


MESH = pl.DeviceIdType.MESH
LANES = 128


def rotary_table(classes, rows, head_width):
    inverse = (ROTARY_BASE ** (-np.arange(0, head_width, 2, dtype=np.float64) / head_width)).astype(np.float32)
    positions = np.arange(classes * classes * rows, dtype=np.float32)
    angles = (positions[:, None] * inverse[None, :]).astype(np.float64)
    cosine, sine = np.cos(angles), np.sin(angles)
    table = np.concatenate([cosine, cosine, -sine, sine], axis=1).astype(np.float32)
    return table.reshape(classes, rows, classes, 2 * head_width).transpose(0, 2, 1, 3)


def class_kernel(
    hid_ref, gain_ref, qgain_ref, kgain_ref, wq_ref, wk_ref, wv_ref, wo_ref, table_ref,
    mixed_ref, total_ref,
    hid, gain_in, qgain, kgain, hb, hm, wall, wo, tb, tm, acc, acc_m, sq, q_b, kv_b, q_c, kv_c,
    halo, oc, lsend, ro, rl, near_out, near_row, halo_out, halo_row, all_log, at, at_own, bias_far, bias_near, gain, drain,
    loc, sent, zr, axr, acr, afr, cxr, ccr, cfr, wor, wfr, wzr, qr, kr, hr, rr, lr, gxr, gcr, gfr, gor, gpr,
):
    f32, bf16 = jnp.float32, jnp.bfloat16
    g, s, p = lax.axis_index("grp"), lax.axis_index("sp"), lax.axis_index("tp")
    n = MIDDLE_DILATION
    rows, width = hid_ref.shape
    sub = rows // n
    heads, hd = qgain_ref.shape
    lw = heads * hd
    halo_sub = halo.shape[2]
    halo_rows = n * halo_sub
    core = p + 1 - 2 * lax.rem(p, 2)
    xp = lax.rem(p + 2, 4)
    diag = lax.rem(core + 2, 4)
    pair, two, mirror = s + 1 - 2 * lax.rem(s, 2), lax.rem(s + 2, n), n - 1 - s
    peer = (s, pair, two, mirror)
    part = sub // 2
    pieces = (
        (two, 0, part), (two, part, part), (pair, 0, sub), (s, 0, sub), (mirror, sub - halo_sub, halo_sub), (mirror, 0, sub - halo_sub)
    )

    def copy_to(axis, src, dst, ss, sr, q):
        return pltpu.make_async_remote_copy(
            src_ref=src, dst_ref=dst, send_sem=ss, recv_sem=sr, device_id={axis: q}, device_id_type=MESH
        )

    tp_copy = functools.partial(copy_to, "tp")
    sp_copy = functools.partial(copy_to, "sp")

    def same(copy, ref, sr, q):
        return copy(ref, ref, sent, sr, q)

    load_hid = pltpu.make_async_copy(hid_ref, hid, loc.at[1])
    load_hid.start()
    barrier = pltpu.get_barrier_semaphore()
    for k in (3, 2, 1):
        pl.semaphore_signal(barrier, inc=1, device_id={"sp": peer[k]}, device_id_type=MESH)
    for q in (xp, diag, core):
        pl.semaphore_signal(barrier, inc=1, device_id={"tp": q}, device_id_type=MESH)
    pl.semaphore_signal(barrier, inc=1, device_id={"grp": 1 - g}, device_id_type=MESH)
    loads = [
        pltpu.make_async_copy(gain_ref, gain_in, loc.at[0]),
        pltpu.make_async_copy(qgain_ref, qgain, loc.at[2]),
        pltpu.make_async_copy(kgain_ref, kgain, loc.at[3]),
        pltpu.make_async_copy(wq_ref, wall.at[:, pl.ds(0, lw)], loc.at[4]),
        pltpu.make_async_copy(wk_ref, wall.at[:, pl.ds(lw, lw)], loc.at[5]),
        pltpu.make_async_copy(wv_ref, wall.at[:, pl.ds(2 * lw, lw)], loc.at[6]),
        pltpu.make_async_copy(table_ref.at[s], tb, loc.at[7]),
        pltpu.make_async_copy(table_ref.at[mirror, s], tm, loc.at[8]),
        pltpu.make_async_copy(
            wo_ref.at[:, pl.ds(pl.multiple_of(p * width, LANES), width)], wo.at[p], loc.at[9]
        ),
    ]
    for load in loads:
        load.start()

    def iota(shape, dim):
        return lax.broadcasted_iota(jnp.int32, shape, dim)

    def row_of(r, part):
        return n * lax.rem(r, part) + r // part

    square = (rows, rows)
    to_class = (row_of(iota(square, 0), sub) == iota(square, 1)).astype(f32).astype(bf16)
    load_hid.wait()
    permuted = jnp.dot(to_class, hid[...], preferred_element_type=f32).astype(bf16)
    hb[p] = permuted.reshape(n, sub, width)
    pl.semaphore_wait(barrier, 3 + n)

    sends = []

    def go(copy):
        copy.start()
        sends.append(math.prod(copy.src_ref.shape) * copy.src_ref.dtype.itemsize)
        return copy

    zs = [
        go(sp_copy(hb.at[p, mirror, pl.ds(a * part, part), :], hm.at[p, a], sent, zr.at[a], mirror))
        for a in range(2)
    ]
    ax = [same(tp_copy, hb.at[p, c, pl.ds(i, m), :], axr.at[j], xp) for j, (c, i, m) in enumerate(pieces)]
    for copy in ax[:5]:
        go(copy)
    ac = go(same(tp_copy, hb.at[p], acr, core))
    w_core = go(tp_copy(
        wo_ref.at[:, pl.ds(pl.multiple_of(core * width, LANES), width)],
        wo.at[p], sent, wor.at[0], core,
    ))

    for load in loads:
        load.wait()
    flat_gain = gain_in[...].astype(f32)
    for j in range(flat_gain.shape[0]):
        each = width // LANES
        gain[j // each, :, (j % each) * LANES : (j % each + 1) * LANES] = flat_gain[j : j + 1]

    def chunk(raw, q):
        raw = raw.astype(f32)
        scaled = (raw * gain[q]).astype(bf16)
        w = wall[pl.ds(pl.multiple_of(q * width, LANES), width), :]
        return jnp.dot(scaled, w, preferred_element_type=f32), jnp.sum(raw * raw, axis=1, keepdims=True)

    def add_all(q, first):
        prod, more = chunk(hb[q].reshape(rows, width), q)
        prod, more = prod.reshape(n, sub, 3 * lw), more.reshape(n, sub, 1)
        acc[...] = prod if first else acc[...] + prod
        sq[...] = more if first else sq[...] + more

    add_all(p, True)
    ac.wait_recv()
    add_all(core, False)

    def finish(acc, sq, table, places, span):
        raw = acc * lax.rsqrt(sq / (width * 4) + EPSILON)
        cosine, sine = table[:, :hd], table[:, hd:]
        for h in range(heads):
            for j, gains in enumerate((qgain, kgain, None)):
                x = raw[:, j * lw + h * hd : j * lw + (h + 1) * hd]
                if gains is not None:
                    x = x * lax.rsqrt(jnp.mean(x * x, axis=-1, keepdims=True) + EPSILON)
                    x = x * gains[pl.ds(h, 1), :]
                    x = x * cosine + pltpu.roll(x, hd // 2, 1) * sine
                for q_ref, kv_ref, c in places:
                    if j == 0:
                        q_ref[c, h, span] = x.astype(bf16)
                    else:
                        kv_ref[c, h, span, (j - 1) * hd : j * hd] = x.astype(bf16)

    def take(j):
        c, i, m = pieces[j]
        ax[j].wait_recv()
        go(same(tp_copy, hb.at[xp, c, pl.ds(i, m), :], afr.at[j], core))

    def close(j, places, between):
        c, i, m = pieces[j]
        span = slice(i, i + m)
        prod, more = chunk(hb[xp, c, span], xp)
        between()
        same(tp_copy, hb.at[diag, c, pl.ds(i, m), :], afr.at[j], core).wait_recv()
        last, most = chunk(hb[diag, c, span], diag)
        finish(acc[c, span] + prod + last, sq[c, span] + more + most, tb[c, span], places, span)

    cx, cc = {}, {}

    def spread(a):
        zs[a].wait_recv()
        cx[a] = go(same(tp_copy, hm.at[p, a], cxr.at[a], xp))
        cc[a] = go(same(tp_copy, hm.at[p, a], ccr, core))

    def cross(a):
        cx[a].wait_recv()
        go(same(tp_copy, hm.at[xp, a], cfr, core))

    parts_of = {1: pieces[2:3], 2: pieces[:2]}

    def class_copy(own, other, sems, k, h, j, arriving):
        _, i, m = parts_of[k][j]
        q = peer[k]
        mine = other.at[q, h, pl.ds(i, m), :]
        if arriving:
            return same(sp_copy, mine, sems.at[k - 1, h, j], q)
        return sp_copy(own.at[q, h, pl.ds(i, m), :], other.at[s, h, pl.ds(i, m), :], sent, sems.at[k - 1, h, j], q)

    kv_copy = functools.partial(class_copy, kv_b, kv_c, kr)
    q_copy = functools.partial(class_copy, q_b, q_c, qr)

    def give(k, j):
        for h in range(heads):
            @pl.when(s < n - 1)
            def _():
                kv_copy(k, h, j, False).start()

            @pl.when(s > 0)
            def _():
                q_copy(k, h, j, False).start()

    def receive(k, h):
        @pl.when(peer[k] < n - 1)
        def _():
            for j in range(len(parts_of[k])):
                kv_copy(k, h, j, True).wait_recv()

        @pl.when(peer[k] > 0)
        def _():
            for j in range(len(parts_of[k])):
                q_copy(k, h, j, True).wait_recv()

    quarter = lw // 4

    def quarter_of(a):
        return pl.ds(pl.multiple_of((2 * g + a) * quarter, 8), quarter)

    def w_copy(i):
        q, block = (xp, diag)[i // 2], quarter_of(i % 2)
        source = wo_ref.at[block, pl.ds(pl.multiple_of(q * width, LANES), width)]
        return tp_copy(source, wo.at[p, block], sent, wor.at[1 + i], q)

    w_copies = [w_copy(i) for i in range(4)]

    def spread_first():
        spread(0)

    def spread_last():
        spread(1)
        go(ax[5])
        @pl.when(s > 0)
        def _():
            w_copies[3].start()

        for copy in w_copies[:3]:
            go(copy)

    def add_mirror(q):
        prod, more = chunk(hm[q].reshape(sub, width), q)
        return prod, more

    squares = []

    def start_mirror():
        same(tp_copy, hm.at[core], ccr, core).wait_recv()
        first, one = add_mirror(p)
        prod, more = add_mirror(core)
        acc_m[...] = first + prod
        squares.append(one + more)
        cross(0)

    def log_count(*read):
        count = sum(each.astype(f32) for each in read)
        bias = jnp.where(count == 2, 1.0, jnp.where(count == 3, math.log2(3.0), 0.0))
        return jnp.where(count == 0, -jnp.inf, bias)

    def strided(behind, step):
        return (behind >= 0) & (behind <= KEYS_BEHIND * step) & ((behind + rows * step) % step == 0)

    later = (rows - sub, rows - sub)
    late, early = iota(later, 0) + sub, iota(later, 1)
    stride = WIDEST_DILATION // n
    crosses = late // sub > early // sub
    bias_far[...] = log_count(strided(late - early, 1) & crosses, strided(late - early, stride) & crosses)
    behind = row_of(iota(square, 0), sub) - row_of(iota(square, 1), sub)
    bias_near[...] = log_count(*(strided(behind, step) for step in (1, n, WIDEST_DILATION)))
    take(0)
    close(0, ((q_b, kv_b, two),), lambda: None)
    give(2, 0)
    take(1)
    close(1, ((q_b, kv_b, two),), spread_first)
    give(2, 1)
    above = lax.rem(s + 1, n)

    def send_halo(c):
        sp_copy(kv_b.at[c, :, pl.ds(sub - halo_sub, halo_sub), :], halo.at[c], sent, hr, above).start()

    @pl.when(s < n - 1)
    def _():
        send_halo(two)

    take(2)
    close(2, ((q_b, kv_b, pair),), spread_last)
    give(1, 0)
    @pl.when(s == 1)
    def _():
        send_halo(pair)

    take(3)
    close(3, ((q_b, kv_b, s), (q_c, kv_c, s)), start_mirror)

    take(4)

    @pl.when(s < n - 1)
    def _():
        send_halo(s)

    close(4, ((q_b, kv_b, mirror),), functools.partial(cross, 1))

    @pl.when((s < n - 1) & (s != 1))
    def _():
        send_halo(mirror)

    prod, more = add_mirror(xp)
    take(5)
    same(tp_copy, hm.at[diag], cfr, core).wait_recv()
    last, most = add_mirror(diag)
    finish(acc_m[...] + prod + last, squares[0] + more + most, tm[...], ((q_c, kv_c, mirror),), slice(0, sub))

    def attend(q, k, v, bias):
        score = lax.dot_general(q, k, (((1,), (1,)), ((), ())), preferred_element_type=f32)
        score = score * (hd ** (-0.5) / math.log(2.0)) + bias
        top = jnp.max(score, axis=-1, keepdims=True)
        weight = jnp.exp2(score - top)
        total = jnp.sum(weight, axis=-1, keepdims=True)
        out = jnp.dot(weight.astype(bf16), v, preferred_element_type=f32) / total
        return out, top * math.log(2.0) + jnp.log(total)

    lane = iota((rows, LANES), 1)

    def as_rows(columns):
        spread_out = jnp.full((sub, LANES), -jnp.inf, f32)
        for c, column in enumerate(columns):
            if column is not None:
                spread_out = jnp.where(lane[:sub] == c, column, spread_out)
        pad = jnp.zeros((LANES - sub, LANES), f32)
        return jnp.transpose(jnp.concatenate([spread_out, pad], axis=0))[:8]

    def flat(x):
        return x.reshape(x.shape[0] * x.shape[1], x.shape[2])

    def far_head(h):
        receive(2, h)
        receive(1, h)
        out, lse = attend(
            flat(q_c[1:, h]), flat(kv_c[: n - 1, h, :, :hd]), flat(kv_c[: n - 1, h, :, hd:]), bias_far[...]
        )
        lsend[h] = as_rows([None] + [lse[b * sub : (b + 1) * sub] for b in range(n - 1)])
        rl[s, h] = lsend[h]
        oc[h, 1:] = out.astype(bf16).reshape(n - 1, sub, hd)
        for k in (3, 2, 1):
            @pl.when(peer[k] > 0)
            def _():
                sp_copy(lsend.at[h], rl.at[s, h], sent, lr.at[k - 1, h], peer[k]).start()
                sp_copy(oc.at[h, peer[k]], ro.at[s, h], sent, rr.at[k - 1, h], peer[k]).start()


    def y_copy(i):
        piece = wo.at[(xp, diag)[i // 2], quarter_of(i % 2)]
        return copy_to("grp", piece, piece, sent, wfr.at[i], 1 - g)

    def pass_step(i):
        later = (i + 3) % 4

        @pl.when(s > 0)
        def _():
            w_copies[later].wait_recv()
            y_copy(later).start()

        if i == 0:
            @pl.when(s == 1)
            def _():
                same(sp_copy, wo.at[diag, quarter_of(1)], wzr, s - 1).start()

        @pl.when(s == 0)
        def _():
            if i < 3:
                w_copies[i].wait_recv()
            else:
                same(sp_copy, wo.at[diag, quarter_of(1)], wzr, s + 1).wait_recv()
            y_copy(i).start()

    far_head(0)
    pass_step(0)
    for h in range(1, heads):
        far_head(h)
    pass_step(1)
    close(5, ((q_b, kv_b, mirror),), lambda: None)

    others = pl.ds(0, n - 1)

    def pair_of(piece, j, near_sem):
        return same(tp_copy, piece, gxr.at[j], xp), same(tp_copy, piece, near_sem, core)

    def index(k, h):
        return 1 + h * (n - 1) + k - 1

    shared = [pair_of(at_own.at[p], 0, gor)]
    for h in range(heads):
        for k in range(1, n):
            shared.append(pair_of(at.at[p, h, k - 1], index(k, h), gcr))

    def share(j):
        for copy in shared[j]:
            copy.start()

    for h in range(heads):
        out, lse = attend(flat(q_b[:, h]), flat(kv_b[:, h, :, :hd]), flat(kv_b[:, h, :, hd:]), bias_near[...])
        near_out[h] = out.reshape(n, sub, hd)
        near_row[h] = as_rows([lse[c * sub : (c + 1) * sub] for c in range(n)])

        @pl.when(s == 0)
        def _():
            at_own[p, h] = near_out[h, 0].astype(bf16)
            for c in range(1, n):
                at[p, h, c - 1] = near_out[h, c].astype(bf16)
            if h == heads - 1:
                share(0)
            for k in range(1, n):
                share(index(k, h))
            all_log[h] = near_row[h]

    pass_step(2)

    @pl.when(s > 0)
    def _():
        sp_copy(halo.at[pl.ds(0, n - 1)], halo.at[pl.ds(0, n - 1)], sent, hr, above).wait_recv()
        halo[s] = kv_c[s - 1, :, sub - halo_sub :, :]
        small = (halo_rows, halo_rows)
        behind = row_of(iota(small, 0), halo_sub) - row_of(iota(small, 1), halo_sub) + halo_rows
        bias_h = jnp.where(behind <= KEYS_BEHIND, 0.0, -jnp.inf).astype(f32)
        low = []
        pad = jnp.full((sub - halo_sub, 1), -jnp.inf, f32)
        for h in range(heads):
            out, lse = attend(
                flat(q_b[:, h, :halo_sub]), flat(halo[:, h, :, :hd]), flat(halo[:, h, :, hd:]), bias_h
            )
            halo_out[h] = out.reshape(n, halo_sub, hd)
            for c in range(n):
                low.append(jnp.concatenate([lse[c * halo_sub : (c + 1) * halo_sub], pad], axis=0))
        halo_row[...] = as_rows(low)

    which = iota((16, LANES), 0)

    def weigh(own, low, far_row):
        top = jnp.maximum(jnp.maximum(own, low), far_row)
        exps = [jnp.exp(x - top) for x in (own, low, far_row)]
        both = exps[0] + exps[1] + exps[2]
        return [x / both for x in exps], top + jnp.log(both)

    def as_columns(shares):
        pad = jnp.zeros((LANES - 16 * len(shares), LANES), f32)
        return jnp.transpose(jnp.concatenate(shares + [pad], axis=0))[:sub]

    def blend(parts, own, far_out, low):
        sums = parts[0] * own + parts[2] * far_out.astype(f32)
        return jnp.concatenate([sums[:halo_sub] + parts[1][:halo_sub] * low, sums[halo_sub:]], axis=0).astype(bf16)

    mine = pl.ds(s, 1)

    def merge(places):
        rows_of = jnp.zeros((16, LANES), f32)
        for i, (c, h) in enumerate(places):
            row = pl.ds(c, 1)
            shares, all_log[h, row] = weigh(near_row[h, row], halo_row[pl.ds(h * n + c, 1)], rl[c, h, mine])
            for j, x in enumerate(shares):
                rows_of = jnp.where(which == 3 * i + j, x, rows_of)
        columns = as_columns([rows_of])
        for i, (c, h) in enumerate(places):
            parts = [columns[:, 3 * i + j : 3 * i + j + 1] for j in range(3)]
            yield lambda far, c=c, h=h, parts=parts: blend(parts, near_out[h, c], far[...], halo_out[h, c])

    @pl.when(s > 0)
    def _():
        for h, mixed in enumerate(merge([(s, h) for h in range(heads)])):
            at_own[p, h] = mixed(oc.at[h, s])
        share(0)

    pass_step(3)

    @pl.when(s > 0)
    def _():
        for h in range(heads):
            for ks in ((1,), (2, 3)) if h < heads - 1 else ((1,), (2, 3)):
                for k in ks:
                    same(sp_copy, rl.at[peer[k], h], lr.at[k - 1, h], peer[k]).wait_recv()
                    same(sp_copy, ro.at[peer[k], h], rr.at[k - 1, h], peer[k]).wait_recv()
                for k, mixed in zip(ks, merge([(peer[k], h) for k in ks])):
                    at[p, h, k - 1] = mixed(ro.at[peer[k], h])
                for k in ks:
                    share(index(k, h))

    block = iota(square, 1) // sub
    class_of = jnp.where(block == 0, pair, jnp.where(block == 1, two, jnp.where(block == 2, mirror, s)))
    from_class = (iota(square, 0) == n * lax.rem(iota(square, 1), sub) + class_of).astype(f32).astype(bf16)

    def product(q):
        x = jnp.concatenate([
            jnp.concatenate([flat(at[q, h, : n - 1]), at_own[q, h]], axis=0) for h in range(heads)
        ], axis=1)
        return jnp.dot(x, wo[q], preferred_element_type=f32)

    def forward(j):
        shared[j][0].wait_recv()
        if j == 0:
            go(same(tp_copy, at_own.at[xp], gpr, core))
        else:
            go(same(tp_copy, at.at[xp, (j - 1) // (n - 1), (j - 1) % (n - 1)], gfr, core))

    by_head = iota((8, LANES), 0)
    logs = []
    for c in range(n):
        row = jnp.zeros((8, LANES), f32)
        for h in range(heads):
            row = jnp.where(by_head == h, all_log[h, c : c + 1, :], row)
        logs.append(row)
    logs = jnp.concatenate(logs, axis=1)
    placed = (n * LANES, rows)
    to_order = (
        (n * lax.rem(iota(placed, 0), LANES) + iota(placed, 0) // LANES == iota(placed, 1))
        & (lax.rem(iota(placed, 0), LANES) < sub)
    ).astype(f32).astype(bf16)
    high = logs.astype(bf16)
    rest = logs - high.astype(f32)
    middle = rest.astype(bf16)
    low = (rest - middle.astype(f32)).astype(bf16)
    total = sum(jnp.dot(x, to_order, preferred_element_type=f32) for x in (high, middle, low))
    total_ref[...] = total[:heads]

    result = product(p)
    for j in (*range(1, n), 0, *range(n, len(shared))):
        forward(j)
    w_core.wait_recv()
    same(tp_copy, at_own.at[core], gor, core).wait_recv()
    same(tp_copy, at.at[core, :, others], gcr, core).wait_recv()
    result += product(core)
    for i in range(4):
        y_copy(i).wait_recv()
    result += product(xp)
    same(tp_copy, at_own.at[diag], gpr, core).wait_recv()
    same(tp_copy, at.at[diag, :, others], gfr, core).wait_recv()
    result += product(diag)
    mixed_ref[...] = jnp.dot(from_class, result.astype(bf16), preferred_element_type=f32).astype(bf16)
    back = heads * (sub * hd * 2 + 8 * LANES * 4)
    q_bytes, kv_bytes = 2 * heads * sub * hd * 2, 2 * heads * sub * 2 * hd * 2
    halo_bytes = (n - 1) * heads * halo_sub * 2 * hd * 2
    at_bytes = 2 * rows * lw * 2
    w_bytes = quarter * width * 2

    def all_sent(total):
        same(tp_copy, drain.at[pl.ds(0, total // (LANES * 4))], acr, core).wait_send()

    always = sum(sends) + at_bytes + 4 * w_bytes + 2 * back

    @pl.when(s == 0)
    def _():
        all_sent(always + kv_bytes + halo_bytes + back)

    @pl.when(s == 1)
    def _():
        all_sent(always + q_bytes + kv_bytes + halo_bytes + 2 * w_bytes)

    @pl.when((s > 1) & (s < n - 1))
    def _():
        all_sent(always + q_bytes + kv_bytes + halo_bytes + w_bytes)

    @pl.when(s == n - 1)
    def _():
        all_sent(always + q_bytes + w_bytes)


def write_kernel(mixed_ref, total_ref, out_ref, log_ref, sems):
    copies = [
        pltpu.make_async_copy(mixed_ref, out_ref, sems.at[0]),
        pltpu.make_async_copy(total_ref, log_ref, sems.at[1]),
    ]
    for copy in copies:
        copy.start()
    for copy in copies:
        copy.wait()


def local_by_class(hidden, norm_gain, w_query, w_key, w_value, query_gain, key_gain, w_out):
    n = MIDDLE_DILATION
    rows, width = hidden.shape
    heads, hd = query_gain.shape
    lw = heads * hd
    sub = rows // n
    halo_sub = KEYS_BEHIND // n
    bf16, f32 = jnp.bfloat16, jnp.float32
    table = jnp.asarray(rotary_table(n, sub, hd))
    most_bytes = 2 * (16 * sub * width + 3 * lw * width + 30 * sub * lw) + 3 * heads * 8 * LANES * 4
    vmem = pl.BlockSpec(memory_space=pltpu.VMEM)
    anyspace = pl.BlockSpec(memory_space=pl.ANY)
    dma = pltpu.SemaphoreType.DMA
    mixed, total = pl.pallas_call(
        class_kernel,
        out_shape=(
            pltpu.VMEM((rows, w_out.shape[1] // 4), bf16),
            pltpu.VMEM((heads, rows), f32),
        ),
        in_specs=[anyspace] * 9,
        out_specs=(vmem, vmem),
        scratch_shapes=[
            pltpu.VMEM((rows, width), bf16),
            pltpu.VMEM((4 * width // LANES, LANES), bf16),
            pltpu.VMEM((heads, hd), f32),
            pltpu.VMEM((heads, hd), f32),
            pltpu.VMEM((4, n, sub, width), bf16),
            pltpu.VMEM((4, 2, sub // 2, width), bf16),
            pltpu.VMEM((4 * width, 3 * lw), bf16),
            pltpu.VMEM((4, lw, width), bf16),
            pltpu.VMEM((n, sub, 2 * hd), f32),
            pltpu.VMEM((sub, 2 * hd), f32),
            pltpu.VMEM((n, sub, 3 * lw), f32),
            pltpu.VMEM((sub, 3 * lw), f32),
            pltpu.VMEM((n, sub, 1), f32),
            pltpu.VMEM((n, heads, sub, hd), bf16),
            pltpu.VMEM((n, heads, sub, 2 * hd), bf16),
            pltpu.VMEM((n, heads, sub, hd), bf16),
            pltpu.VMEM((n, heads, sub, 2 * hd), bf16),
            pltpu.VMEM((n, heads, halo_sub, 2 * hd), bf16),
            pltpu.VMEM((heads, n, sub, hd), bf16),
            pltpu.VMEM((heads, 8, LANES), f32),
            pltpu.VMEM((n, heads, sub, hd), bf16),
            pltpu.VMEM((n, heads, 8, LANES), f32),
            pltpu.VMEM((heads, n, sub, hd), f32),
            pltpu.VMEM((heads, 8, LANES), f32),
            pltpu.VMEM((heads, n, halo_sub, hd), f32),
            pltpu.VMEM((8, LANES), f32),
            pltpu.VMEM((heads, 8, LANES), f32),
            pltpu.VMEM((4, heads, n, sub, hd), bf16),
            pltpu.VMEM((4, heads, sub, hd), bf16),
            pltpu.VMEM((rows - sub, rows - sub), f32),
            pltpu.VMEM((rows, rows), f32),
            pltpu.VMEM((4, 1, width), f32),
            pltpu.VMEM((most_bytes // (4 * LANES), LANES), f32),
            dma((10,)), dma, dma((2,)), dma((n + 2,)), dma, dma((n + 2,)), dma((2,)), dma, dma,
            dma((5,)), dma((4,)), dma, dma((2, heads, 2)), dma((2, heads, 2)), dma, dma((3, heads)), dma((3, heads)),
            dma((1 + 3 * heads,)), dma, dma, dma, dma,
        ],
        compiler_params=pltpu.CompilerParams(
            collective_id=0, has_side_effects=True, vmem_limit_bytes=60 * 1024 * 1024
        ),
    )(
        hidden, norm_gain.reshape(-1, LANES), query_gain, key_gain,
        w_query, w_key, w_value, w_out, table,
    )
    mixed, total = pl.pallas_call(
        write_kernel,
        out_shape=(
            jax.ShapeDtypeStruct(mixed.shape, bf16), jax.ShapeDtypeStruct(total.shape, f32)
        ),
        in_specs=[vmem, vmem],
        out_specs=(anyspace, anyspace),
        scratch_shapes=[dma((2,))],
    )(
        pltpu.with_memory_space_constraint(mixed, pltpu.VMEM),
        pltpu.with_memory_space_constraint(total, pltpu.VMEM),
    )
    return mixed, total.T


def solution(mesh):
    split = (mesh.shape["grp"], mesh.shape["sp"], mesh.shape["tp"]) == (2, MIDDLE_DILATION, 4)
    chosen = local_by_class if split else local
    placed = (
        P(("grp", "sp"), "tp"),
        P(),
        P(None, "tp"),
        P(None, "tp"),
        P(None, "tp"),
        P("tp", None),
        P("tp", None),
        P("tp", None),
    )
    return jax.shard_map(
        chosen,
        mesh=mesh,
        in_specs=placed,
        out_specs=(P(("grp", "sp"), "tp"), P(("grp", "sp"), "tp")),
        check_vma=False,
    )
```
